32 devices in a mesh: grp: 2 (over y), sp: 4 (over z), tp: 4 (over x, core).
Axes of the slice: x: 2, y: 2, z: 4, core: 2. Of those that a mesh axis runs over, the one named last changes fastest.
Arguments:
- latent: bfloat16 [4096, 4096], P(('grp', 'sp', 'tp')), parts along dimension 0, may hold values from -260 to 260
- context: bfloat16 [1536, 4096], P(('grp', 'sp')), parts along dimension 0, may hold values from -6 to 6
- conditioning: bfloat16 [8192], P(('grp', 'sp')), parts along dimension 0, may hold values from -6 to 6
- norm_gain: float32 [4096], replicated, may hold values from 0.1 to 1.9
- shift_weight: bfloat16 [4096, 4096], P('sp', 'tp'), may hold values from -0.09375 to 0.09375
- scale_weight: bfloat16 [4096, 4096], P('sp', 'tp'), may hold values from -0.09375 to 0.09375
- gate_weight: bfloat16 [4096, 4096], P('sp', 'tp'), may hold values from -0.09375 to 0.09375
- query_weight: bfloat16 [4096, 1024], P(None, 'tp'), may hold values from -3 to 3
- key_weight: bfloat16 [4096, 512], P(None, 'tp'), may hold values from -3 to 3
- value_weight: bfloat16 [4096, 512], P(None, 'tp'), may hold values from -0.09375 to 0.09375
- out_weight: bfloat16 [1024, 4096], P(None, 'tp'), may hold values from -1.5 to 1.5
- sink_logit: float32 [16], P('tp'), may hold values from 3 to 7
Outputs:
- mixed: bfloat16 [4096, 4096], P(('grp', 'sp', 'tp')), parts along dimension 0
The draws below stay inside these ranges and needn't reach their ends.
There are 2 independent parts, one for each index of `grp`. The reference program is written for one: setup_inputs(seed, part) draws one part's arguments, and reference() takes and returns one part's arrays. A program takes and returns all parts, laid end to end along the dimension named above; an argument that names none is the same for every part. Nothing has to cross between parts.
All inputs are finite; a program needn't handle non-finite values.
Results may differ from the reference program's by a relative error of at most 0.012.
The reference program's roundings to bfloat16 on the way count: a program that leaves them out, or rounds other values in their place, can miss the bound.
Values may be sent and summed in bfloat16 or wider, within the bound.
A program may use at most 64 MiB of HBM per device.

```python
import math
import jax
import jax.numpy as jnp
from jax import lax

D = 4096
HEADS = 16
KV_HEADS = 8
HD = 64
GRID_W = 64
WIN = 128
CTX = 768
SEQ = 2048


def paired_projections(seed_key):
    query_rows = jax.random.truncated_normal(jax.random.fold_in(seed_key, 11), -4.0, 4.0, (D, HEADS * HD), jnp.float32) / math.sqrt(D)
    key_rows = jax.random.truncated_normal(jax.random.fold_in(seed_key, 12), -4.0, 4.0, (D, KV_HEADS * HD), jnp.float32) / math.sqrt(D)
    return (query_rows, key_rows)


def draw_query_weight(key, part):
    return paired_projections(key)[0].astype(jnp.bfloat16)


def draw_key_weight(key, part):
    return paired_projections(key)[1].astype(jnp.bfloat16)


def draw_latent(key, part):
    values_drawn = jax.random.truncated_normal(jax.random.fold_in(key, 1), -6.0, 6.0, (SEQ, D), jnp.float32)
    return values_drawn.astype(jnp.bfloat16)


def block_scale(rng, extent, cuts, least, high):
    factor_of, own = 1.0, jax.random.fold_in(rng, 6)
    for dim, blocks in cuts:
        draws = jnp.exp(jax.random.uniform(jax.random.fold_in(own, dim), (blocks,), jnp.float32, least / len(cuts), high / len(cuts)))
        factor_of = factor_of * jnp.repeat(draws, extent[dim] // blocks).reshape([-1 if axis == dim else 1 for axis in range(len(extent))])
    return factor_of


def scatter_about(stream_key, dims, width, most, shards=(), kind=jnp.bfloat16):
    level = block_scale(stream_key, dims, shards, -0.22, 0.18) if shards else 1.0
    values = jax.random.normal(stream_key, dims, jnp.float32) * width * level
    return jnp.minimum(jnp.maximum(values, -most), most).astype(kind)


def setup_inputs(seed: int = 0, part: int = 0) -> dict:
    splits = jax.random.split(jax.random.key(seed), 13)
    own_keys = jax.random.split(jax.random.fold_in(splits[12], part), 13)
    return {
        "latent": draw_latent(jax.random.fold_in(jax.random.fold_in(splits[12], part), 71), part),
        "context": scatter_about(own_keys[1], (CTX, D), 1.0, 6.0, ((0, 4),)),
        "conditioning": scatter_about(own_keys[2], (D,), 1.5, 6.0, ((0, 4),)),
        "norm_gain": jnp.clip(1.0 + 0.18 * jax.random.normal(splits[3], (D,), jnp.float32), 0.1, 1.9),
        "shift_weight": scatter_about(splits[4], (D, D), D ** -0.5, 0.09375, ((0, 4), (1, 4))),
        "scale_weight": scatter_about(splits[5], (D, D), D ** -0.5, 0.09375, ((0, 4), (1, 4))),
        "gate_weight": scatter_about(splits[6], (D, D), D ** -0.5, 0.09375, ((0, 4), (1, 4))),
        "query_weight": draw_query_weight(jax.random.fold_in(splits[12], 71), part),
        "key_weight": draw_key_weight(jax.random.fold_in(splits[12], 71), part),
        "value_weight": scatter_about(splits[9], (D, KV_HEADS * HD), D ** -0.5, 0.09375, ((1, 4),)),
        "out_weight": scatter_about(splits[10], (HEADS * HD, D), (HD // 4) ** -0.5, 1.5, ((1, 4),)),
        "sink_logit": jnp.clip(3.0 + 4.0 * jax.random.uniform(splits[11], (HEADS,), jnp.float32) ** block_scale(splits[11], (HEADS,), ((0, 4),), -0.2, 0.2), 3.0, 7.0),
    }


epsilon = 1e-06
rope_base = 10000.0
neg_large = -1e+30

def row_norm(matrix, norm_gain):
    values = matrix.astype(jnp.float32)
    return values * lax.rsqrt(lax.optimization_barrier(jnp.mean(values * values, axis=-1, keepdims=True)) + epsilon) * norm_gain

def axial_turn(values, position):
    half_dim = values.shape[-1] // 2
    quarter = half_dim // 2
    inverse = rope_base ** (-jnp.arange(quarter, dtype=jnp.float32) / quarter)

    def turn(section, coordinate):
        angles = coordinate.astype(jnp.float32)[:, None] * inverse[None, :]
        cosine = jnp.cos(angles)[:, None, :]
        sine_part = jnp.sin(angles)[:, None, :]
        leading = section[..., :quarter]
        trailing = section[..., quarter:]
        return jnp.concatenate([leading * cosine - trailing * sine_part, leading * sine_part + trailing * cosine], axis=-1)
    return jnp.concatenate([turn(values[..., :half_dim], position // GRID_W), turn(values[..., half_dim:], position % GRID_W)], axis=-1)

def reference(latent, context, conditioning, norm_gain, shift_weight, scale_weight, gate_weight, query_weight, key_weight, value_weight, out_weight, sink_logit):
    lifted = jax.nn.silu(conditioning.astype(jnp.float32)).astype(jnp.bfloat16)[None, :]
    shift_vec = jnp.dot(lifted, shift_weight, preferred_element_type=jnp.float32)[0]
    scale_vec = jnp.dot(lifted, scale_weight, preferred_element_type=jnp.float32)[0]
    gate_vec = jnp.dot(lifted, gate_weight, preferred_element_type=jnp.float32)[0]
    normed = (row_norm(latent, norm_gain) * (1.0 + scale_vec) + shift_vec).astype(jnp.bfloat16)
    position = jnp.arange(SEQ, dtype=jnp.int32)
    queries = axial_turn(jnp.dot(normed, query_weight, preferred_element_type=jnp.float32).reshape(SEQ, HEADS, HD), position).astype(jnp.bfloat16)
    latent_keys = axial_turn(jnp.dot(normed, key_weight, preferred_element_type=jnp.float32).reshape(SEQ, KV_HEADS, HD), position).astype(jnp.bfloat16)
    latent_values = jnp.dot(normed, value_weight, preferred_element_type=jnp.float32).astype(jnp.bfloat16).reshape(SEQ, KV_HEADS, HD)
    prepared = row_norm(context, norm_gain).astype(jnp.bfloat16)
    context_keys = jnp.dot(prepared, key_weight, preferred_element_type=jnp.float32).astype(jnp.bfloat16).reshape(CTX, KV_HEADS, HD).astype(jnp.float32)
    context_values = jnp.dot(prepared, value_weight, preferred_element_type=jnp.float32).astype(jnp.bfloat16).reshape(CTX, KV_HEADS, HD).astype(jnp.float32)
    group_size = HEADS // KV_HEADS
    factor = HD ** (-0.5)
    padded_keys = jnp.pad(latent_keys, ((WIN, WIN), (0, 0), (0, 0)))
    padded_values = jnp.pad(latent_values, ((WIN, WIN), (0, 0), (0, 0)))
    sink_values = sink_logit.astype(jnp.float32).reshape(KV_HEADS, group_size)[:, :, None, None]

    def one_block(block_index):
        first_row = block_index * WIN
        block_queries = lax.dynamic_slice_in_dim(queries, first_row, WIN, 0).reshape(WIN, KV_HEADS, group_size, HD).astype(jnp.float32)
        block_keys = lax.dynamic_slice_in_dim(padded_keys, first_row, 3 * WIN, 0).astype(jnp.float32)
        block_values = lax.dynamic_slice_in_dim(padded_values, first_row, 3 * WIN, 0).astype(jnp.float32)
        local_scores = jnp.einsum('qhgd,khd->hgqk', block_queries, block_keys) * factor
        query_pos = first_row + jnp.arange(WIN, dtype=jnp.int32)
        key_pos = first_row - WIN + jnp.arange(3 * WIN, dtype=jnp.int32)
        allowed = (jnp.abs(key_pos[None, :] - query_pos[:, None]) <= WIN) & (key_pos[None, :] >= 0) & (key_pos[None, :] < SEQ)
        local_scores = jnp.where(allowed, local_scores, neg_large)
        context_scores = jnp.einsum('qhgd,thd->hgqt', block_queries, context_keys) * factor
        joined = jnp.concatenate([local_scores, context_scores, jnp.broadcast_to(sink_values, local_scores.shape[:-1] + (1,))], axis=-1)
        highest = lax.optimization_barrier(jnp.max(joined, axis=-1, keepdims=True))
        exponent = jnp.exp(joined - highest)
        weights = (exponent / lax.optimization_barrier(jnp.sum(exponent, axis=-1, keepdims=True))).astype(jnp.bfloat16)
        weights = lax.optimization_barrier(weights).astype(jnp.float32)
        out_block = jnp.einsum('hgqk,khd->qhgd', weights[..., :3 * WIN], block_values) + jnp.einsum('hgqt,thd->qhgd', weights[..., 3 * WIN:3 * WIN + CTX], context_values)
        return out_block.reshape(WIN, HEADS * HD).astype(jnp.bfloat16)
    attended = lax.map(one_block, jnp.arange(SEQ // WIN, dtype=jnp.int32)).reshape(SEQ, HEADS * HD)
    blended = jnp.dot(attended, out_weight, preferred_element_type=jnp.float32).astype(jnp.bfloat16)
    blended = lax.optimization_barrier(blended).astype(jnp.float32)
    return (latent.astype(jnp.float32) + gate_vec * blended).astype(jnp.bfloat16)
```

```python
import functools

import jax
import jax.numpy as jnp
from jax import lax
from jax.experimental import pallas as pl
from jax.experimental.pallas import tpu as pltpu
from jax.sharding import PartitionSpec as P

HEADS = 16
KV_HEADS = 8
HD = 64
GRID_W = 64
WIN = 128


epsilon = 1e-06
rope_base = 10000.0
neg_large = -1e30


def with_halo(cells, sides, width):
    for axis, dim in sides:
        count = lax.axis_size(axis)
        ends = count - 1
        head = lax.slice_in_dim(cells, 0, width, axis=dim)
        tail = lax.slice_in_dim(cells, cells.shape[dim] - width, cells.shape[dim], axis=dim)
        cells = jnp.concatenate(
            [
                lax.ppermute(tail, axis, [(i, (i + 1) % count) for i in range(ends)]),
                cells,
                lax.ppermute(head, axis, [((i + 1) % count, i) for i in range(ends)]),
            ],
            axis=dim,
        )
    return cells


def row_norm(matrix, norm_gain):
    values = matrix.astype(jnp.float32)
    return (
        values * lax.rsqrt(jnp.mean(values * values, axis=-1, keepdims=True) + epsilon) * norm_gain
    )


def axial_turn(values, position):
    half_dim = values.shape[-1] // 2
    quarter = half_dim // 2
    inverse = rope_base ** (-jnp.arange(quarter, dtype=jnp.float32) / quarter)

    def turn(section, coordinate):
        angles = coordinate.astype(jnp.float32)[:, None] * inverse[None, :]
        cosine = jnp.cos(angles)[:, None, :]
        sine_part = jnp.sin(angles)[:, None, :]
        leading = section[..., :quarter]
        trailing = section[..., quarter:]
        return jnp.concatenate(
            [leading * cosine - trailing * sine_part, leading * sine_part + trailing * cosine],
            axis=-1,
        )

    return jnp.concatenate(
        [
            turn(values[..., :half_dim], position // GRID_W),
            turn(values[..., half_dim:], position % GRID_W),
        ],
        axis=-1,
    )


def context_pairs(context_rows, norm_gain, key_weight, value_weight):
    prepared = row_norm(context_rows, norm_gain).astype(jnp.bfloat16)
    return jnp.concatenate(
        [
            jnp.dot(prepared, key_weight, preferred_element_type=jnp.float32),
            jnp.dot(prepared, value_weight, preferred_element_type=jnp.float32),
        ],
        axis=1,
    ).astype(jnp.bfloat16)


def local_plain(
    latent,
    context,
    conditioning,
    norm_gain,
    shift_weight,
    scale_weight,
    gate_weight,
    query_weight,
    key_weight,
    value_weight,
    out_weight,
    sink_logit,
):
    lifted = jax.nn.silu(conditioning.astype(jnp.float32)).astype(jnp.bfloat16)[None, :]
    shift_part = jnp.dot(lifted, shift_weight, preferred_element_type=jnp.float32)[0]
    scale_part = jnp.dot(lifted, scale_weight, preferred_element_type=jnp.float32)[0]
    gate_part = jnp.dot(lifted, gate_weight, preferred_element_type=jnp.float32)[0]
    summed = lax.psum((shift_part, scale_part, gate_part), "sp")
    shift_vec, scale_vec, gate_vec = (
        lax.all_gather(summed[0], "tp", axis=0, tiled=True),
        lax.all_gather(summed[1], "tp", axis=0, tiled=True),
        lax.all_gather(summed[2], "tp", axis=0, tiled=True),
    )
    normed = (row_norm(latent, norm_gain) * (1.0 + scale_vec) + shift_vec).astype(jnp.bfloat16)
    segment = lax.all_gather(normed, "tp", axis=0, tiled=True)
    projected = jnp.concatenate(
        [
            jnp.dot(segment, query_weight, preferred_element_type=jnp.float32),
            jnp.dot(segment, key_weight, preferred_element_type=jnp.float32),
            jnp.dot(segment, value_weight, preferred_element_type=jnp.float32),
        ],
        axis=1,
    )
    row_count = projected.shape[0]
    query_width = query_weight.shape[1]
    key_width = key_weight.shape[1]
    query_heads = query_width // HD
    pair_heads = key_width // HD
    group_size = HEADS // KV_HEADS
    row_offset = lax.axis_index("sp") * row_count
    position = row_offset + jnp.arange(row_count, dtype=jnp.int32)
    queries = axial_turn(
        projected[:, :query_width].reshape(row_count, query_heads, HD), position
    ).astype(jnp.bfloat16)
    latent_keys = axial_turn(
        projected[:, query_width : query_width + key_width].reshape(row_count, pair_heads, HD),
        position,
    ).astype(jnp.bfloat16)
    latent_values = projected[:, query_width + key_width :].astype(jnp.bfloat16)
    key_value = jnp.concatenate([latent_keys.reshape(row_count, key_width), latent_values], axis=1)
    widened = with_halo(key_value, (("sp", 0),), WIN)
    context_all = lax.all_gather(
        context_pairs(context, norm_gain, key_weight, value_weight), "sp", axis=0, tiled=True
    )
    block_count = row_count // WIN
    context_count = context_all.shape[0]
    query_blocks = queries.reshape(block_count, WIN, pair_heads, group_size, HD)
    band_blocks = widened.reshape(block_count + 2, WIN, 2 * key_width)
    band_rows = jnp.concatenate(
        [band_blocks[:block_count], band_blocks[1 : block_count + 1], band_blocks[2:]], axis=1
    )
    band_keys = band_rows[..., :key_width].reshape(block_count, 3 * WIN, pair_heads, HD)
    band_values = band_rows[..., key_width:].reshape(block_count, 3 * WIN, pair_heads, HD)
    context_keys = context_all[:, :key_width].reshape(context_count, pair_heads, HD)
    context_values = context_all[:, key_width:].reshape(context_count, pair_heads, HD)
    factor = HD ** (-0.5)
    local_scores = (
        jnp.einsum("nqhgd,nkhd->nhgqk", query_blocks, band_keys, preferred_element_type=jnp.float32)
        * factor
    )
    query_pos = position.reshape(block_count, WIN)
    key_pos = (
        row_offset
        - WIN
        + jnp.arange(block_count, dtype=jnp.int32)[:, None] * WIN
        + jnp.arange(3 * WIN, dtype=jnp.int32)[None, :]
    )
    seq_total = row_count * lax.axis_size("sp")
    allowed = (
        (jnp.abs(key_pos[:, None, :] - query_pos[:, :, None]) <= WIN)
        & (key_pos[:, None, :] >= 0)
        & (key_pos[:, None, :] < seq_total)
    )
    local_scores = jnp.where(allowed[:, None, None], local_scores, neg_large)
    context_scores = (
        jnp.einsum(
            "nqhgd,thd->nhgqt", query_blocks, context_keys, preferred_element_type=jnp.float32
        )
        * factor
    )
    sink_values = sink_logit.reshape(pair_heads, group_size)[None, :, :, None, None]
    highest = jnp.maximum(
        jnp.maximum(
            jnp.max(local_scores, axis=-1, keepdims=True),
            jnp.max(context_scores, axis=-1, keepdims=True),
        ),
        sink_values,
    )
    local_exp = jnp.exp(local_scores - highest)
    context_exp = jnp.exp(context_scores - highest)
    denominator = (
        jnp.sum(local_exp, axis=-1, keepdims=True)
        + jnp.sum(context_exp, axis=-1, keepdims=True)
        + jnp.exp(sink_values - highest)
    )
    local_weights = (local_exp / denominator).astype(jnp.bfloat16)
    context_weights = (context_exp / denominator).astype(jnp.bfloat16)
    attended = jnp.einsum(
        "nhgqk,nkhd->nqhgd", local_weights, band_values, preferred_element_type=jnp.float32
    ) + jnp.einsum(
        "nhgqt,thd->nqhgd", context_weights, context_values, preferred_element_type=jnp.float32
    )
    attended = attended.reshape(row_count, query_width).astype(jnp.bfloat16)
    columns_part = jnp.dot(
        lax.all_gather(attended, "tp", axis=1, tiled=True),
        out_weight,
        preferred_element_type=jnp.float32,
    ).astype(jnp.bfloat16)
    blended = lax.all_to_all(columns_part, "tp", split_axis=0, concat_axis=1, tiled=True)
    return (latent.astype(jnp.float32) + gate_vec * blended.astype(jnp.float32)).astype(
        jnp.bfloat16
    )


LATENT_CHUNKS = 8
WEIGHT_CHUNKS = 4
AHEAD = 3
NORM_ROWS = 16


def remote(src, dst, send, recv, device):
    return pltpu.make_async_remote_copy(
        src_ref=src,
        dst_ref=dst,
        send_sem=send,
        recv_sem=recv,
        device_id=device,
        device_id_type=pl.DeviceIdType.MESH,
    )


def fused_kernel(
    sp,
    latent,
    context,
    conditioning,
    norm_gain,
    shift_weight,
    scale_weight,
    gate_weight,
    query_weight,
    key_weight,
    value_weight,
    out_weight,
    sink,
    mixed,
    cond_v,
    gain_v,
    mod_w,
    proj_w,
    wo,
    ctx_v,
    lat_own,
    lat_far,
    normed,
    stat_out,
    stat_in,
    row_scale,
    sink_v,
    mod_part,
    mod_all,
    factor_v,
    shift_v,
    gate_v,
    turn_cos,
    turn_sin,
    acc,
    queries,
    key_value,
    ctx_kv,
    att,
    att_out,
    out_part,
    mixed_v,
    load_sem,
    lat_send,
    lat_recv,
    stat_sem,
    pair_send,
    pair_recv,
    wox_send,
    wo_send,
    wo_recv,
    woy_send,
    woy_recv,
    wop_send,
    wop_recv,
    modz_send,
    modz_recv,
    modt_send,
    modt_recv,
    ctxz_send,
    ctxz_recv,
    ctxp_sem,
    kv_send,
    kv_recv,
    halo_sem,
    att_send,
    att_recv,
):
    g = lax.axis_index("grp")
    s = lax.axis_index("sp")
    t = lax.axis_index("tp")
    chip = t // 2
    core = lax.rem(t, 2)
    pair = chip * 2 + 1 - core
    far = (1 - chip) * 2 + core
    pair_dev, far_dev, y_dev = {"tp": pair}, {"tp": far}, {"grp": 1 - g}
    right_dev = {"sp": lax.rem(s + 1, sp)}
    left_dev = {"sp": lax.rem(s + sp - 1, sp)}
    has_right, has_left = s < sp - 1, s > 0
    rows, width = latent.shape
    ctx_rows = context.shape[0]
    mod_cols = shift_weight.shape[1]
    qw = query_weight.shape[1]
    kw = key_weight.shape[1]
    heads = qw // HD
    group = heads // (kw // HD)
    tp = 4
    total = tp * rows
    out_rows, out_width = out_weight.shape
    half = rows // 2
    f32, bf16 = jnp.float32, jnp.bfloat16
    chunk = width // LATENT_CHUNKS
    shard = out_rows // (2 * sp)
    slab = shard // WEIGHT_CHUNKS
    MESH = pl.DeviceIdType.MESH

    loads = [
        (latent, lat_own),
        (conditioning, cond_v),
        (shift_weight, mod_w.at[0]),
        (scale_weight, mod_w.at[1]),
        (gate_weight, mod_w.at[2]),
        (norm_gain, gain_v),
        (context, ctx_v),
        (key_weight, proj_w.at[core, :, qw : qw + kw]),
        (value_weight, proj_w.at[core, :, qw + kw : qw + 2 * kw]),
        (query_weight, proj_w.at[core, :, 0:qw]),
        (out_weight, wo.at[t]),
    ]
    loads = [pltpu.make_async_copy(a, b, load_sem.at[i]) for i, (a, b) in enumerate(loads)]
    for load in loads:
        load.start()

    barrier = pltpu.get_barrier_semaphore()
    for k in range(1, tp):
        pl.semaphore_signal(
            barrier, inc=1, device_id={"tp": lax.rem(t + k, tp)}, device_id_type=MESH
        )
    pl.semaphore_signal(barrier, inc=1, device_id=y_dev, device_id_type=MESH)
    for has, place in ((has_right, right_dev), (has_left, left_dev)):

        @pl.when(has)
        def _():
            for peer in (t, pair):
                pl.semaphore_signal(
                    barrier, inc=1, device_id={**place, "tp": peer}, device_id_type=MESH
                )

    lane = lax.broadcasted_iota(jnp.int32, (rows, 128), 1)
    row = lax.broadcasted_iota(jnp.int32, (rows, 128), 0)
    diagonal = lane == row

    loads[0].wait()

    def row_stat(i, carry):
        part = pl.ds(pl.multiple_of(i * NORM_ROWS, NORM_ROWS), NORM_ROWS)
        values = lat_own[part].astype(f32)
        scale = lax.rsqrt(jnp.mean(values * values, axis=-1, keepdims=True) + epsilon)
        row_scale[0, part] = jnp.broadcast_to(scale, (NORM_ROWS, 128))
        return carry

    lax.fori_loop(0, rows // NORM_ROWS, row_stat, 0)
    flat = jnp.sum(jnp.where(diagonal, row_scale[0], 0.0), axis=0, keepdims=True)
    stat_out[...] = jnp.broadcast_to(flat, (8, 128))
    sink_row = lax.broadcasted_iota(jnp.int32, (8, 128), 0)
    sink_all = jnp.full((8, 128), sink[0], f32)
    for h in range(1, heads):
        sink_all = jnp.where(sink_row == h, sink[h], sink_all)
    sink_v[core] = sink_all

    pl.semaphore_wait(
        barrier, tp + jnp.where(has_right, 2, 0) + jnp.where(has_left, 2, 0)
    )

    def lat_copy(j):
        cols = pl.ds(pl.multiple_of(j * chunk, 128), chunk)
        return remote(
            latent.at[:, cols], lat_far.at[:, cols], lat_send.at[j], lat_recv.at[j], far_dev
        )

    def wo_rows(gg, j, c):
        return pl.ds(pl.multiple_of((gg * sp + j) * shard + c * slab, 16), slab)

    def wo_cross(c):
        part = wo_rows(g, s, c)
        return remote(
            out_weight.at[part], wo.at[t, part], wox_send.at[c], wo_recv.at[s, c], far_dev
        )

    stat_copy = remote(stat_out, stat_in, stat_sem.at[0], stat_sem.at[1], far_dev)
    stat_copy.start()
    for c in range(WEIGHT_CHUNKS):
        wo_cross(c).start()
    for j in range(AHEAD):
        lat_copy(j).start()
    pair_copies = [
        (sink_v.at[core], sink_v.at[core]),
        (query_weight, proj_w.at[core, :, 0:qw]),
        (key_weight, proj_w.at[core, :, qw : qw + kw]),
        (value_weight, proj_w.at[core, :, qw + kw : qw + 2 * kw]),
        (out_weight, wo.at[t]),
    ]
    pair_copies = [
        remote(a, b, pair_send.at[i], pair_recv.at[i], pair_dev)
        for i, (a, b) in enumerate(pair_copies)
    ]
    for copy in pair_copies:
        copy.start()

    def line_copy(at, j, send, recv, toward):
        return remote(at(j), at(j), send.at[toward, j], recv.at[j], (left_dev, right_dev)[toward])

    def line_start(at, send, recv):
        for toward, has in ((0, has_left), (1, has_right)):

            @pl.when(has)
            def _():
                line_copy(at, s, send, recv, toward).start()

    def line_relay(k, at, send, recv):
        for toward, has, j, there in (
            (1, has_right, s - k, s >= k),
            (0, has_left, s + k, s + k < sp),
        ):

            @pl.when(there)
            def _():
                line_copy(at, j, send, recv, toward).wait_recv()

                @pl.when(has)
                def _():
                    line_copy(at, j, send, recv, toward).start()

    def line_finish(at, send, recv):
        for j in range(sp):
            for toward, has, sent in ((1, has_right, j <= s), (0, has_left, j >= s)):

                @pl.when(jnp.logical_and(has, sent))
                def _():
                    line_copy(at, j, send, recv, toward).wait_send()

    def mod_at(j):
        return mod_part.at[j]

    def ctx_at(j):
        return ctx_kv.at[core, pl.ds(pl.multiple_of(j * ctx_rows, 16), ctx_rows)]

    for i in range(1, 5):
        loads[i].wait()
    cond = cond_v[...].astype(f32).reshape(1, cond_v.shape[0])
    lifted = jnp.broadcast_to(cond / (1.0 + jnp.exp(-cond)), (16, cond.shape[1])).astype(bf16)
    for i in range(3):
        mod_part[s, :, i * mod_cols : (i + 1) * mod_cols] = jnp.dot(
            lifted, mod_w[i], preferred_element_type=f32
        )[0:1]
    line_start(mod_at, modz_send, modz_recv)

    for i in range(5, 9):
        loads[i].wait()

    def norm_context(i, carry):
        part = pl.ds(pl.multiple_of(i * NORM_ROWS, NORM_ROWS), NORM_ROWS)
        values = ctx_v[part].astype(f32)
        scale = lax.rsqrt(jnp.mean(values * values, axis=-1, keepdims=True) + epsilon)
        ctx_v[part] = (values * scale * gain_v[...]).astype(bf16)
        return carry

    lax.fori_loop(0, ctx_rows // NORM_ROWS, norm_context, 0)
    own_ctx = pl.ds(pl.multiple_of(s * ctx_rows, 16), ctx_rows)
    ctx_kv[core, own_ctx] = jnp.dot(
        ctx_v[...], proj_w[core, :, qw : qw + 2 * kw], preferred_element_type=f32
    ).astype(bf16)
    line_relay(1, mod_at, modz_send, modz_recv)
    line_start(ctx_at, ctxz_send, ctxz_recv)

    def wo_line(j, c, toward):
        part = wo.at[far, wo_rows(g, j, c)]
        return remote(
            part, part, wo_send.at[toward, j, c], wo_recv.at[j, c], (left_dev, right_dev)[toward]
        )

    def wo_across(j, c):
        part = wo.at[far, wo_rows(g, j, c)]
        return remote(part, part, woy_send, woy_recv, y_dev)

    def wo_own(c):
        wo_line(s, c, 0).wait_recv()
        for toward, has in ((0, has_left), (1, has_right)):

            @pl.when(has)
            def _():
                wo_line(s, c, toward).start()

        wo_across(s, c).start()

    def wo_relay(e):
        k, c = e // WEIGHT_CHUNKS, lax.rem(e, WEIGHT_CHUNKS)
        for toward, has, j, there in (
            (1, has_right, s - k, s >= k),
            (0, has_left, s + k, s + k < sp),
        ):

            @pl.when(there)
            def _():
                wo_line(j, c, toward).wait_recv()

                @pl.when(has)
                def _():
                    wo_line(j, c, toward).start()

                wo_across(j, c).start()

    def wo_relays(low, high):
        def step(e, carry):
            wo_relay(e)
            return carry

        lax.fori_loop(low, high, step, 0)

    quarter = HD // 4
    inverse = jnp.exp(
        lax.rem(lane, quarter).astype(f32) * (-jnp.log(jnp.float32(rope_base)) / quarter)
    )
    first = lax.rem(lane, 2 * quarter) < quarter
    by_row = lax.rem(lane, HD) < HD // 2

    def tables(b, carry):
        place = s * total + jnp.where(b == 0, t, far) * rows + row
        coordinate = jnp.where(by_row, place // GRID_W, lax.rem(place, GRID_W))
        angles = coordinate.astype(f32) * inverse
        turn_cos[b] = jnp.cos(angles)
        sines = jnp.sin(angles)
        turn_sin[b] = jnp.where(first, -sines, sines)
        return carry

    wo_own(0)
    line_relay(2, mod_at, modz_send, modz_recv)
    lax.fori_loop(0, 2, tables, 0)
    wo_own(1)
    line_relay(1, ctx_at, ctxz_send, ctxz_recv)
    for k in range(3, sp):
        line_relay(k, mod_at, modz_send, modz_recv)
    summed = mod_part[0]
    for k in range(1, sp):
        summed = summed + mod_part[k]
    mod_all[t] = summed
    mods = []
    for k in range(1, tp):
        copy = remote(
            mod_all.at[t],
            mod_all.at[t],
            modt_send.at[k - 1],
            modt_recv.at[k - 1],
            {"tp": lax.rem(t + k, tp)},
        )
        copy.start()
        mods.append(copy)
    for c in range(2, WEIGHT_CHUNKS):
        wo_own(c)
    line_relay(2, ctx_at, ctxz_send, ctxz_recv)
    wo_relays(WEIGHT_CHUNKS, 2 * WEIGHT_CHUNKS)
    for k in range(3, sp):
        line_relay(k, ctx_at, ctxz_send, ctxz_recv)
    ctx_pair = remote(ctx_kv.at[core], ctx_kv.at[core], ctxp_sem.at[0], ctxp_sem.at[1], pair_dev)
    ctx_pair.start()

    stat_copy.wait_recv()
    column = jnp.sum(
        jnp.where(diagonal, jnp.broadcast_to(stat_in[0:1], (rows, 128)), 0.0), axis=1, keepdims=True
    )
    row_scale[1] = jnp.broadcast_to(column, (rows, 128))

    for copy in mods:
        copy.wait_recv()
    for i in range(tp):
        cols = slice(i * mod_cols, (i + 1) * mod_cols)
        shift_v[:, cols] = mod_all[i, :, 0:mod_cols]
        factor_v[:, cols] = gain_v[:, cols] * (1.0 + mod_all[i, :, mod_cols : 2 * mod_cols])
        gate_v[:, cols] = mod_all[i, :, 2 * mod_cols : 3 * mod_cols]

    def project(j, block, source):
        cols = pl.ds(pl.multiple_of(j * chunk, 128), chunk)

        def norm_rows(i, carry):
            part = pl.ds(pl.multiple_of(i * NORM_ROWS, NORM_ROWS), NORM_ROWS)
            values = source[part, cols].astype(f32)
            scale = row_scale[block, part, 0:1]
            normed[part] = (values * scale * factor_v[:, cols] + shift_v[:, cols]).astype(bf16)
            return carry

        lax.fori_loop(0, rows // NORM_ROWS, norm_rows, 0)
        for slot in range(2):
            product = jnp.dot(
                normed[...], proj_w[slot, cols], preferred_element_type=f32
            )

            @pl.when(j == 0)
            def _():
                acc[slot] = product

            @pl.when(j != 0)
            def _():
                acc[slot] = acc[slot] + product

    low = lane < HD

    def finish_projection(block, position):
        cosine, sine = turn_cos[block], turn_sin[block]

        def turned(values):
            swapped = jnp.where(
                first, pltpu.roll(values, 128 - quarter, 1), pltpu.roll(values, quarter, 1)
            )
            return values * cosine + swapped * sine

        factor = HD ** (-0.5)
        base = pl.ds(pl.multiple_of(position * rows, rows), rows)
        for slot in range(2):
            key_value[slot, base, 0:kw] = turned(acc[slot, :, qw : qw + kw]).astype(bf16)
            key_value[slot, base, kw : 2 * kw] = acc[slot, :, qw + kw : qw + 2 * kw].astype(bf16)
            for h in range(heads):
                lanes = acc[slot, :, (h // 2) * 128 : (h // 2 + 1) * 128]
                lanes = turned(lanes).astype(bf16).astype(f32) * factor
                at, want = h % 2, h // group
                if at != want:
                    lanes = pltpu.roll(lanes, HD, 1)
                keep = low if want == 0 else jnp.logical_not(low)
                lanes = jnp.where(keep, lanes, 0.0).astype(bf16)
                for n in range(2):
                    queries[block, n, slot, h * half : (h + 1) * half] = lanes[
                        n * half : (n + 1) * half
                    ]

    def kv_at(position):
        return key_value.at[:, pl.ds(pl.multiple_of(position * rows, rows), rows)]

    def kv_pair(block, position):
        return remote(
            kv_at(position), kv_at(position), kv_send.at[block], kv_recv.at[block], pair_dev
        )

    halo_down = remote(
        kv_at(1), kv_at(tp + 1), halo_sem.at[0], halo_sem.at[1], {**left_dev, "tp": pair}
    )
    halo_up = remote(kv_at(tp), kv_at(0), halo_sem.at[0], halo_sem.at[1], {**right_dev, "tp": pair})
    sends_down = jnp.logical_and(core == 0, has_left)
    sends_up = jnp.logical_and(core == 1, has_right)

    def send_halo(mine):
        @pl.when(jnp.logical_and(mine, sends_down))
        def _():
            halo_down.start()

        @pl.when(jnp.logical_and(mine, sends_up))
        def _():
            halo_up.start()

    def wait_halo(mine):
        @pl.when(jnp.logical_and(mine, sends_down))
        def _():
            halo_up.wait_recv()

        @pl.when(jnp.logical_and(mine, sends_up))
        def _():
            halo_down.wait_recv()

    edge = jnp.zeros((2, rows, 2 * kw), bf16)

    @pl.when(jnp.logical_and(core == 0, jnp.logical_not(has_left)))
    def _():
        key_value[:, 0:rows] = edge

    @pl.when(jnp.logical_and(core == 1, jnp.logical_not(has_right)))
    def _():
        key_value[:, (tp + 1) * rows : (tp + 2) * rows] = edge

    for i in range(9, 11):
        loads[i].wait()
    for copy in pair_copies[0:4]:
        copy.wait_recv()

    def own_step(j, carry):
        project(j, 0, lat_own)
        return carry

    lax.fori_loop(0, LATENT_CHUNKS, own_step, 0)
    finish_projection(0, t + 1)
    kv_pair(0, t + 1).start()
    send_halo(chip == core)

    def far_step(j, carry):
        @pl.when(j < 4)
        def _():
            wo_relays(2 * WEIGHT_CHUNKS + 2 * j, 2 * WEIGHT_CHUNKS + 2 * j + 2)

        lat_copy(j).wait_recv()

        @pl.when(j + AHEAD < LATENT_CHUNKS)
        def _():
            lat_copy(j + AHEAD).start()

        project(j, 1, lat_far)
        return carry

    lax.fori_loop(0, LATENT_CHUNKS, far_step, 0)
    finish_projection(1, far + 1)
    kv_pair(1, far + 1).start()
    send_halo(chip != core)

    def wo_pair(gg):
        part = wo.at[far, pl.ds(pl.multiple_of(gg * sp * shard, 16), sp * shard)]
        return remote(part, part, wop_send.at[gg], wop_recv.at[gg], pair_dev)

    wo_pair(g).start()

    kv_pair(0, pair + 1).wait_recv()
    ctx_pair.wait_recv()

    contract = (((1,), (1,)), ((), ()))
    band = 2 * WIN + half
    stack = heads * half
    q_pos = lax.rem(lax.broadcasted_iota(jnp.int32, (stack, band), 0), half)
    k_pos = lax.broadcasted_iota(jnp.int32, (stack, band), 1)
    in_window = jnp.logical_and(k_pos >= q_pos, k_pos <= q_pos + 2 * WIN)

    def attend(block, position, n, slot, target):
        start = pl.multiple_of((position - 1) * rows + n * half, half)
        band_k = key_value[slot, pl.ds(start, band), 0:kw]
        band_v = key_value[slot, pl.ds(start, band), kw : 2 * kw]
        ctx_k = ctx_kv[slot, :, 0:kw]
        ctx_v_ = ctx_kv[slot, :, kw : 2 * kw]
        sinks = jnp.concatenate(
            [jnp.broadcast_to(sink_v[slot, h : h + 1, 0:1], (half, 1)) for h in range(heads)],
            axis=0,
        )
        place = s * total + start - WIN + k_pos
        allowed = jnp.logical_and(in_window, jnp.logical_and(place >= 0, place < sp * total))
        q = queries[block, n, slot]
        near_s = lax.dot_general(q, band_k, contract, preferred_element_type=f32)
        near_s = jnp.where(allowed, near_s, neg_large)
        ctx_s = lax.dot_general(q, ctx_k, contract, preferred_element_type=f32)
        top = jnp.maximum(
            jnp.max(near_s, axis=-1, keepdims=True), jnp.max(ctx_s, axis=-1, keepdims=True)
        )
        top = jnp.maximum(top, sinks)
        near_e = jnp.exp(near_s - top)
        ctx_e = jnp.exp(ctx_s - top)
        bottom = (
            jnp.sum(near_e, axis=-1, keepdims=True)
            + jnp.sum(ctx_e, axis=-1, keepdims=True)
            + jnp.exp(sinks - top)
        )
        share = 1.0 / bottom
        result = jnp.dot(
            (near_e * share).astype(bf16), band_v, preferred_element_type=f32
        ) + jnp.dot((ctx_e * share).astype(bf16), ctx_v_, preferred_element_type=f32)
        for v in range(qw // 128):
            sides = []
            for at in range(2):
                h = 2 * v + at
                lanes = result[h * half : (h + 1) * half]
                if h // group != at:
                    lanes = pltpu.roll(lanes, HD, 1)
                sides.append(lanes)
            target[
                slot, pl.ds(pl.multiple_of(n * half, half), half), v * 128 : (v + 1) * 128
            ] = jnp.where(low[:half], sides[0], sides[1]).astype(bf16)

    def att_copy(n):
        part = pl.ds(pl.multiple_of(n * half, half), half)
        return remote(
            att_out.at[:, part], att.at[chip, :, part], att_send.at[n], att_recv.at[n], far_dev
        )

    kv_pair(1, pair + 1).wait_recv()
    wait_halo(chip != core)

    def far_attend(i, carry):
        n, slot = i // 2, lax.rem(i, 2)
        attend(1, far + 1, n, slot, att_out)

        @pl.when(slot == 1)
        def _():
            att_copy(n).start()

        return carry

    lax.fori_loop(0, 4, far_attend, 0)
    wo_gathered = wo.at[far, pl.ds(pl.multiple_of((1 - g) * sp * shard, 16), sp * shard)]
    remote(wo_gathered, wo_gathered, woy_send, woy_recv, y_dev).wait_recv()
    wo_pair(1 - g).start()
    wait_halo(chip == core)

    def own_attend(i, carry):
        n, slot = i // 2, lax.rem(i, 2)
        attend(0, t + 1, n, slot, att.at[chip])
        return carry

    lax.fori_loop(0, 4, own_attend, 0)

    pair_copies[4].wait_recv()

    def out_product(x, i):
        sums = None
        for slot in range(2):
            part = pl.ds(pl.multiple_of((2 * x + slot) * qw, qw), qw)
            product = jnp.dot(att[x, slot], wo[i, part], preferred_element_type=f32)
            sums = product if sums is None else sums + product
        return sums

    order = (t, pair, far, (1 - chip) * 2 + 1 - core)
    other = (1 - chip) * 2 + 1 - core
    for k, i in enumerate(order):
        if k == 3:
            for gg in range(2):
                part = wo.at[other, pl.ds(gg * sp * shard, sp * shard)]
                remote(part, part, wop_send.at[gg], wop_recv.at[gg], pair_dev).wait_recv()
        out_part[k] = out_product(chip, i)
    att_copy(0).wait_recv()
    att_copy(1).wait_recv()
    stores = []
    for k, i in enumerate(order):
        cols = pl.ds(pl.multiple_of(i * out_width, 128), out_width)
        blended = (out_part[k] + out_product(1 - chip, i)).astype(bf16).astype(f32)
        mixed_v[:, cols] = (lat_own[:, cols].astype(f32) + gate_v[:, cols] * blended).astype(bf16)
        store = pltpu.make_async_copy(
            mixed_v.at[:, cols], mixed.at[:, cols], load_sem.at[len(loads) + k]
        )
        store.start()
        stores.append(store)

    stat_copy.wait_send()
    for c in range(WEIGHT_CHUNKS):
        wo_cross(c).wait_send()
    for j in range(LATENT_CHUNKS):
        lat_copy(j).wait_send()
    for copy in pair_copies:
        copy.wait_send()
    for copy in mods:
        copy.wait_send()
    line_finish(mod_at, modz_send, modz_recv)
    line_finish(ctx_at, ctxz_send, ctxz_recv)
    ctx_pair.wait_send()
    for j in range(sp):
        for toward, has, sent in ((1, has_right, j <= s), (0, has_left, j >= s)):

            @pl.when(jnp.logical_and(has, sent))
            def _():
                def step(c, carry):
                    wo_line(j, c, toward).wait_send()
                    return carry

                lax.fori_loop(0, WEIGHT_CHUNKS, step, 0)

    wo_sent = wo.at[far, pl.ds(pl.multiple_of(g * sp * shard, 16), sp * shard)]
    remote(wo_sent, wo_sent, woy_send, woy_recv, y_dev).wait_send()
    wo_pair(0).wait_send()
    wo_pair(1).wait_send()
    kv_pair(0, t + 1).wait_send()
    kv_pair(1, far + 1).wait_send()

    @pl.when(sends_down)
    def _():
        halo_down.wait_send()

    @pl.when(sends_up)
    def _():
        halo_up.wait_send()

    att_copy(0).wait_send()
    att_copy(1).wait_send()
    for store in stores:
        store.wait()


def local(
    latent,
    context,
    conditioning,
    norm_gain,
    shift_weight,
    scale_weight,
    gate_weight,
    query_weight,
    key_weight,
    value_weight,
    out_weight,
    sink_logit,
):
    tp, sp, grp = lax.axis_size("tp"), lax.axis_size("sp"), lax.axis_size("grp")
    rows, width = latent.shape
    ctx_rows = context.shape[0]
    mod_rows, mod_cols = shift_weight.shape
    query_width, key_width = query_weight.shape[1], key_weight.shape[1]
    out_rows, out_width = out_weight.shape
    fits = (
        rows == WIN
        and rows == 128
        and key_width == 2 * HD
        and query_width == 4 * HD
        and tp == 4
        and grp == 2
        and sp >= 3
        and ctx_rows % NORM_ROWS == 0
        and mod_cols % 128 == 0
        and width % (128 * LATENT_CHUNKS) == 0
        and out_width % 128 == 0
        and tp * out_width == width
        and out_rows == tp * query_width
        and out_rows % (2 * sp * WEIGHT_CHUNKS * 16) == 0
    )
    if not fits:
        return local_plain(
            latent,
            context,
            conditioning,
            norm_gain,
            shift_weight,
            scale_weight,
            gate_weight,
            query_weight,
            key_weight,
            value_weight,
            out_weight,
            sink_logit,
        )
    f32, bf16 = jnp.float32, jnp.bfloat16
    dma = pltpu.SemaphoreType.DMA
    anywhere = pl.BlockSpec(memory_space=pl.ANY)
    return pl.pallas_call(
        functools.partial(fused_kernel, sp),
        out_shape=jax.ShapeDtypeStruct((rows, width), bf16),
        in_specs=[anywhere] * 11 + [pl.BlockSpec(memory_space=pltpu.SMEM)],
        out_specs=anywhere,
        scratch_shapes=[
            pltpu.VMEM((mod_rows,), bf16),
            pltpu.VMEM((1, width), f32),
            pltpu.VMEM((3, mod_rows, mod_cols), bf16),
            pltpu.VMEM((2, width, query_width + 2 * key_width), bf16),
            pltpu.VMEM((tp, out_rows, out_width), bf16),
            pltpu.VMEM(context.shape, bf16),
            pltpu.VMEM((rows, width), bf16),
            pltpu.VMEM((rows, width), bf16),
            pltpu.VMEM((rows, width // LATENT_CHUNKS), bf16),
            pltpu.VMEM((8, 128), f32),
            pltpu.VMEM((8, 128), f32),
            pltpu.VMEM((2, rows, 128), f32),
            pltpu.VMEM((2, 8, 128), f32),
            pltpu.VMEM((sp, 1, 3 * mod_cols), f32),
            pltpu.VMEM((tp, 1, 3 * mod_cols), f32),
            pltpu.VMEM((1, width), f32),
            pltpu.VMEM((1, width), f32),
            pltpu.VMEM((1, width), f32),
            pltpu.VMEM((2, rows, 128), f32),
            pltpu.VMEM((2, rows, 128), f32),
            pltpu.VMEM((2, rows, query_width + 2 * key_width), f32),
            pltpu.VMEM((2, 2, 2, query_width // HD * (rows // 2), key_width), bf16),
            pltpu.VMEM((2, (tp + 2) * rows, 2 * key_width), bf16),
            pltpu.VMEM((2, sp * ctx_rows, 2 * key_width), bf16),
            pltpu.VMEM((2, 2, rows, query_width), bf16),
            pltpu.VMEM((2, rows, query_width), bf16),
            pltpu.VMEM((tp, rows, out_width), f32),
            pltpu.VMEM((rows, width), bf16),
            dma((15,)),
            dma((LATENT_CHUNKS,)),
            dma((LATENT_CHUNKS,)),
            dma((2,)),
            dma((5,)),
            dma((5,)),
            dma((WEIGHT_CHUNKS,)),
            dma((2, sp, WEIGHT_CHUNKS)),
            dma((sp, WEIGHT_CHUNKS)),
            dma,
            dma,
            dma((2,)),
            dma((2,)),
            dma((2, sp)),
            dma((sp,)),
            dma((tp - 1,)),
            dma((tp - 1,)),
            dma((2, sp)),
            dma((sp,)),
            dma((2,)),
            dma((2,)),
            dma((2,)),
            dma((2,)),
            dma((2,)),
            dma((2,)),
        ],
        compiler_params=pltpu.CompilerParams(
            collective_id=0, has_side_effects=True, vmem_limit_bytes=60 * 1024 * 1024
        ),
        name="fused",
    )(
        latent,
        context,
        conditioning,
        norm_gain.reshape(1, width),
        shift_weight,
        scale_weight,
        gate_weight,
        query_weight,
        key_weight,
        value_weight,
        out_weight,
        sink_logit,
    )


def solution(mesh):
    in_specs = (
        P(("grp", "sp", "tp"), None),
        P(("grp", "sp"), None),
        P(("grp", "sp")),
        P(),
        P("sp", "tp"),
        P("sp", "tp"),
        P("sp", "tp"),
        P(None, "tp"),
        P(None, "tp"),
        P(None, "tp"),
        P(None, "tp"),
        P("tp"),
    )
    out_specs = P(("grp", "sp", "tp"), None)
    return jax.shard_map(local, mesh=mesh, in_specs=in_specs, out_specs=out_specs, check_vma=False)
```

```python
import functools

import jax
import jax.numpy as jnp
from jax import lax
from jax.experimental import pallas as pl
from jax.experimental.pallas import tpu as pltpu
from jax.sharding import PartitionSpec as P

HEADS = 16
KV_HEADS = 8
HD = 64
GRID_W = 64
WIN = 128


epsilon = 1e-06
rope_base = 10000.0
neg_large = -1e30


def with_halo(cells, sides, width):
    for axis, dim in sides:
        count = lax.axis_size(axis)
        ends = count - 1
        head = lax.slice_in_dim(cells, 0, width, axis=dim)
        tail = lax.slice_in_dim(cells, cells.shape[dim] - width, cells.shape[dim], axis=dim)
        cells = jnp.concatenate(
            [
                lax.ppermute(tail, axis, [(i, (i + 1) % count) for i in range(ends)]),
                cells,
                lax.ppermute(head, axis, [((i + 1) % count, i) for i in range(ends)]),
            ],
            axis=dim,
        )
    return cells


def row_norm(matrix, norm_gain):
    values = matrix.astype(jnp.float32)
    return (
        values * lax.rsqrt(jnp.mean(values * values, axis=-1, keepdims=True) + epsilon) * norm_gain
    )


def axial_turn(values, position):
    half_dim = values.shape[-1] // 2
    quarter = half_dim // 2
    inverse = rope_base ** (-jnp.arange(quarter, dtype=jnp.float32) / quarter)

    def turn(section, coordinate):
        angles = coordinate.astype(jnp.float32)[:, None] * inverse[None, :]
        cosine = jnp.cos(angles)[:, None, :]
        sine_part = jnp.sin(angles)[:, None, :]
        leading = section[..., :quarter]
        trailing = section[..., quarter:]
        return jnp.concatenate(
            [leading * cosine - trailing * sine_part, leading * sine_part + trailing * cosine],
            axis=-1,
        )

    return jnp.concatenate(
        [
            turn(values[..., :half_dim], position // GRID_W),
            turn(values[..., half_dim:], position % GRID_W),
        ],
        axis=-1,
    )


def context_pairs(context_rows, norm_gain, key_weight, value_weight):
    prepared = row_norm(context_rows, norm_gain).astype(jnp.bfloat16)
    return jnp.concatenate(
        [
            jnp.dot(prepared, key_weight, preferred_element_type=jnp.float32),
            jnp.dot(prepared, value_weight, preferred_element_type=jnp.float32),
        ],
        axis=1,
    ).astype(jnp.bfloat16)


def local_plain(
    latent,
    context,
    conditioning,
    norm_gain,
    shift_weight,
    scale_weight,
    gate_weight,
    query_weight,
    key_weight,
    value_weight,
    out_weight,
    sink_logit,
):
    lifted = jax.nn.silu(conditioning.astype(jnp.float32)).astype(jnp.bfloat16)[None, :]
    shift_part = jnp.dot(lifted, shift_weight, preferred_element_type=jnp.float32)[0]
    scale_part = jnp.dot(lifted, scale_weight, preferred_element_type=jnp.float32)[0]
    gate_part = jnp.dot(lifted, gate_weight, preferred_element_type=jnp.float32)[0]
    summed = lax.psum((shift_part, scale_part, gate_part), "sp")
    shift_vec, scale_vec, gate_vec = (
        lax.all_gather(summed[0], "tp", axis=0, tiled=True),
        lax.all_gather(summed[1], "tp", axis=0, tiled=True),
        lax.all_gather(summed[2], "tp", axis=0, tiled=True),
    )
    normed = (row_norm(latent, norm_gain) * (1.0 + scale_vec) + shift_vec).astype(jnp.bfloat16)
    segment = lax.all_gather(normed, "tp", axis=0, tiled=True)
    projected = jnp.concatenate(
        [
            jnp.dot(segment, query_weight, preferred_element_type=jnp.float32),
            jnp.dot(segment, key_weight, preferred_element_type=jnp.float32),
            jnp.dot(segment, value_weight, preferred_element_type=jnp.float32),
        ],
        axis=1,
    )
    row_count = projected.shape[0]
    query_width = query_weight.shape[1]
    key_width = key_weight.shape[1]
    query_heads = query_width // HD
    pair_heads = key_width // HD
    group_size = HEADS // KV_HEADS
    row_offset = lax.axis_index("sp") * row_count
    position = row_offset + jnp.arange(row_count, dtype=jnp.int32)
    queries = axial_turn(
        projected[:, :query_width].reshape(row_count, query_heads, HD), position
    ).astype(jnp.bfloat16)
    latent_keys = axial_turn(
        projected[:, query_width : query_width + key_width].reshape(row_count, pair_heads, HD),
        position,
    ).astype(jnp.bfloat16)
    latent_values = projected[:, query_width + key_width :].astype(jnp.bfloat16)
    key_value = jnp.concatenate([latent_keys.reshape(row_count, key_width), latent_values], axis=1)
    widened = with_halo(key_value, (("sp", 0),), WIN)
    context_all = lax.all_gather(
        context_pairs(context, norm_gain, key_weight, value_weight), "sp", axis=0, tiled=True
    )
    block_count = row_count // WIN
    context_count = context_all.shape[0]
    query_blocks = queries.reshape(block_count, WIN, pair_heads, group_size, HD)
    band_blocks = widened.reshape(block_count + 2, WIN, 2 * key_width)
    band_rows = jnp.concatenate(
        [band_blocks[:block_count], band_blocks[1 : block_count + 1], band_blocks[2:]], axis=1
    )
    band_keys = band_rows[..., :key_width].reshape(block_count, 3 * WIN, pair_heads, HD)
    band_values = band_rows[..., key_width:].reshape(block_count, 3 * WIN, pair_heads, HD)
    context_keys = context_all[:, :key_width].reshape(context_count, pair_heads, HD)
    context_values = context_all[:, key_width:].reshape(context_count, pair_heads, HD)
    factor = HD ** (-0.5)
    local_scores = (
        jnp.einsum("nqhgd,nkhd->nhgqk", query_blocks, band_keys, preferred_element_type=jnp.float32)
        * factor
    )
    query_pos = position.reshape(block_count, WIN)
    key_pos = (
        row_offset
        - WIN
        + jnp.arange(block_count, dtype=jnp.int32)[:, None] * WIN
        + jnp.arange(3 * WIN, dtype=jnp.int32)[None, :]
    )
    seq_total = row_count * lax.axis_size("sp")
    allowed = (
        (jnp.abs(key_pos[:, None, :] - query_pos[:, :, None]) <= WIN)
        & (key_pos[:, None, :] >= 0)
        & (key_pos[:, None, :] < seq_total)
    )
    local_scores = jnp.where(allowed[:, None, None], local_scores, neg_large)
    context_scores = (
        jnp.einsum(
            "nqhgd,thd->nhgqt", query_blocks, context_keys, preferred_element_type=jnp.float32
        )
        * factor
    )
    sink_values = sink_logit.reshape(pair_heads, group_size)[None, :, :, None, None]
    highest = jnp.maximum(
        jnp.maximum(
            jnp.max(local_scores, axis=-1, keepdims=True),
            jnp.max(context_scores, axis=-1, keepdims=True),
        ),
        sink_values,
    )
    local_exp = jnp.exp(local_scores - highest)
    context_exp = jnp.exp(context_scores - highest)
    denominator = (
        jnp.sum(local_exp, axis=-1, keepdims=True)
        + jnp.sum(context_exp, axis=-1, keepdims=True)
        + jnp.exp(sink_values - highest)
    )
    local_weights = (local_exp / denominator).astype(jnp.bfloat16)
    context_weights = (context_exp / denominator).astype(jnp.bfloat16)
    attended = jnp.einsum(
        "nhgqk,nkhd->nqhgd", local_weights, band_values, preferred_element_type=jnp.float32
    ) + jnp.einsum(
        "nhgqt,thd->nqhgd", context_weights, context_values, preferred_element_type=jnp.float32
    )
    attended = attended.reshape(row_count, query_width).astype(jnp.bfloat16)
    columns_part = jnp.dot(
        lax.all_gather(attended, "tp", axis=1, tiled=True),
        out_weight,
        preferred_element_type=jnp.float32,
    ).astype(jnp.bfloat16)
    blended = lax.all_to_all(columns_part, "tp", split_axis=0, concat_axis=1, tiled=True)
    return (latent.astype(jnp.float32) + gate_vec * blended.astype(jnp.float32)).astype(
        jnp.bfloat16
    )


LATENT_CHUNKS = 8
WEIGHT_CHUNKS = 4
AHEAD = 3
NORM_ROWS = 16
CONTEXT_ROWS = 32


def remote(src, dst, send, recv, device):
    return pltpu.make_async_remote_copy(
        src_ref=src,
        dst_ref=dst,
        send_sem=send,
        recv_sem=recv,
        device_id=device,
        device_id_type=pl.DeviceIdType.MESH,
    )


def fused_kernel(
    sp,
    latent,
    context,
    conditioning,
    norm_gain,
    shift_weight,
    scale_weight,
    gate_weight,
    query_weight,
    key_weight,
    value_weight,
    out_weight,
    sink,
    mixed,
    cond_v,
    gain_v,
    mod_w,
    proj_w,
    wo,
    wo_shard,
    ctx_v,
    lat_own,
    lat_far,
    normed,
    stat_out,
    stat_in,
    row_scale,
    sink_v,
    mod_part,
    mod_all,
    factor_v,
    shift_v,
    gate_v,
    turn_cos,
    turn_sin,
    acc,
    queries,
    key_value,
    ctx_kv,
    att,
    att_out,
    ctx_vt,
    bias,
    part_out,
    part_top,
    part_sum,
    out_part,
    load_sem,
    lat_send,
    lat_recv,
    stat_sem,
    pair_send,
    pair_recv,
    wox_send,
    wo_send,
    wo_recv,
    woy_send,
    woy_recv,
    wop_send,
    wop_recv,
    modz_send,
    modz_recv,
    modt_send,
    modt_recv,
    ctxz_send,
    ctxz_recv,
    ctxp_sem,
    kv_send,
    kv_recv,
    halo_sem,
    att_send,
    att_recv,
):
    g = lax.axis_index("grp")
    s = lax.axis_index("sp")
    t = lax.axis_index("tp")
    chip = t // 2
    core = lax.rem(t, 2)
    pair = chip * 2 + 1 - core
    far = (1 - chip) * 2 + core
    pair_dev, far_dev, y_dev = {"tp": pair}, {"tp": far}, {"grp": 1 - g}
    right_dev = {"sp": lax.rem(s + 1, sp)}
    left_dev = {"sp": lax.rem(s + sp - 1, sp)}
    has_right, has_left = s < sp - 1, s > 0
    rows, width = latent.shape
    ctx_rows = context.shape[0]
    mod_cols = shift_weight.shape[1]
    qw = query_weight.shape[1]
    kw = key_weight.shape[1]
    heads = qw // HD
    group = heads // (kw // HD)
    tp = 4
    total = tp * rows
    out_rows, out_width = out_weight.shape
    half = rows // 2
    f32, bf16 = jnp.float32, jnp.bfloat16
    chunk = width // LATENT_CHUNKS
    shard = out_rows // (2 * sp)
    slab = shard // WEIGHT_CHUNKS
    MESH = pl.DeviceIdType.MESH

    loads = [
        (latent, lat_own),
        (out_weight.at[pl.ds(pl.multiple_of((g * sp + s) * shard, 16), shard)], wo_shard),
        (norm_gain, gain_v),
        (context, ctx_v),
        (key_weight, proj_w.at[core, :, qw : qw + kw]),
        (value_weight, proj_w.at[core, :, qw + kw : qw + 2 * kw]),
        (conditioning, cond_v),
        (shift_weight, mod_w.at[0]),
        (scale_weight, mod_w.at[1]),
        (gate_weight, mod_w.at[2]),
        (query_weight, proj_w.at[core, :, 0:qw]),
        (out_weight, wo.at[t]),
    ]
    loads = [pltpu.make_async_copy(a, b, load_sem.at[i]) for i, (a, b) in enumerate(loads)]
    for load in loads:
        load.start()

    barrier = pltpu.get_barrier_semaphore()
    for k in range(1, tp):
        pl.semaphore_signal(
            barrier, inc=1, device_id={"tp": lax.rem(t + k, tp)}, device_id_type=MESH
        )
    pl.semaphore_signal(barrier, inc=1, device_id=y_dev, device_id_type=MESH)
    for has, place in ((has_right, right_dev), (has_left, left_dev)):

        @pl.when(has)
        def _():
            for peer in (t, pair):
                pl.semaphore_signal(
                    barrier, inc=1, device_id={**place, "tp": peer}, device_id_type=MESH
                )

    def row_factor(source, part):
        squares = None
        for at in range(0, width, 512):
            values = source[part, at : at + 512].astype(f32)
            values = values * values
            squares = values if squares is None else squares + values
        return lax.rsqrt(jnp.sum(squares, axis=-1, keepdims=True) * (1.0 / width) + epsilon)

    lane = lax.broadcasted_iota(jnp.int32, (rows, 128), 1)
    row = lax.broadcasted_iota(jnp.int32, (rows, 128), 0)
    diagonal = lane == row

    loads[0].wait()
    loads[1].wait()

    def row_stat(i, carry):
        part = pl.ds(pl.multiple_of(i * CONTEXT_ROWS, 16), CONTEXT_ROWS)
        row_scale[0, part] = jnp.broadcast_to(row_factor(lat_own, part), (CONTEXT_ROWS, 128))
        return carry

    lax.fori_loop(0, rows // CONTEXT_ROWS, row_stat, 0)
    flat = jnp.sum(jnp.where(diagonal, row_scale[0], 0.0), axis=0, keepdims=True)
    stat_out[...] = jnp.broadcast_to(flat, (8, 128))
    sink_row = lax.broadcasted_iota(jnp.int32, (8, 128), 0)
    sink_all = jnp.full((8, 128), sink[0], f32)
    for h in range(1, heads):
        sink_all = jnp.where(sink_row == h, sink[h], sink_all)
    sink_v[core] = sink_all

    pl.semaphore_wait(
        barrier, tp + jnp.where(has_right, 2, 0) + jnp.where(has_left, 2, 0)
    )

    def lat_copy(j):
        cols = pl.ds(pl.multiple_of(j * chunk, 128), chunk)
        return remote(
            lat_own.at[:, cols], lat_far.at[:, cols], lat_send.at[j], lat_recv.at[j], far_dev
        )

    def wo_rows(gg, j, c):
        return pl.ds(pl.multiple_of((gg * sp + j) * shard + c * slab, 16), slab)

    def wo_cross(c):
        part = wo_rows(g, s, c)
        return remote(
            wo_shard.at[pl.ds(c * slab, slab)],
            wo.at[t, part],
            wox_send.at[c],
            wo_recv.at[s, c],
            far_dev,
        )

    stat_copy = remote(stat_out, stat_in, stat_sem.at[0], stat_sem.at[1], far_dev)
    stat_copy.start()
    for c in range(WEIGHT_CHUNKS):
        wo_cross(c).start()
    for j in range(2):
        lat_copy(j).start()
    pair_copies = [
        (sink_v.at[core], sink_v.at[core]),
        (query_weight, proj_w.at[core, :, 0:qw]),
        (key_weight, proj_w.at[core, :, qw : qw + kw]),
        (value_weight, proj_w.at[core, :, qw + kw : qw + 2 * kw]),
        (out_weight, wo.at[t]),
    ]
    pair_copies = [
        remote(a, b, pair_send.at[i], pair_recv.at[i], pair_dev)
        for i, (a, b) in enumerate(pair_copies)
    ]
    pair_copies[0].start()

    def line_copy(at, j, send, recv, toward):
        return remote(at(j), at(j), send.at[toward, j], recv.at[j], (left_dev, right_dev)[toward])

    def line_start(at, send, recv):
        for toward, has in ((0, has_left), (1, has_right)):

            @pl.when(has)
            def _():
                line_copy(at, s, send, recv, toward).start()

    def line_relay(k, at, send, recv):
        for toward, has, j, there in (
            (1, has_right, s - k, s >= k),
            (0, has_left, s + k, s + k < sp),
        ):

            @pl.when(there)
            def _():
                line_copy(at, j, send, recv, toward).wait_recv()

                @pl.when(has)
                def _():
                    line_copy(at, j, send, recv, toward).start()

    def line_finish(at, send, recv):
        for j in range(sp):
            for toward, has, sent in ((1, has_right, j <= s), (0, has_left, j >= s)):

                @pl.when(jnp.logical_and(has, sent))
                def _():
                    line_copy(at, j, send, recv, toward).wait_send()

    def mod_at(j):
        return mod_part.at[j]

    def ctx_at(j):
        return ctx_kv.at[core, pl.ds(pl.multiple_of(j * ctx_rows, 16), ctx_rows)]

    for i in range(2, 6):
        loads[i].wait()

    def norm_context(i, carry):
        part = pl.ds(pl.multiple_of(i * CONTEXT_ROWS, 16), CONTEXT_ROWS)
        scale = row_factor(ctx_v, part)
        for at in range(0, width, 512):
            here = slice(at, at + 512)
            values = ctx_v[part, here].astype(f32)
            ctx_v[part, here] = (values * scale * gain_v[:, here]).astype(bf16)
        return carry

    lax.fori_loop(0, ctx_rows // CONTEXT_ROWS, norm_context, 0)
    own_ctx = pl.ds(pl.multiple_of(s * ctx_rows, 16), ctx_rows)
    ctx_kv[core, own_ctx] = jnp.dot(
        ctx_v[...], proj_w[core, :, qw : qw + 2 * kw], preferred_element_type=f32
    ).astype(bf16)
    line_start(ctx_at, ctxz_send, ctxz_recv)
    for i in range(6, 10):
        loads[i].wait()
    cond = cond_v[...].astype(f32).reshape(1, cond_v.shape[0])
    lifted = jnp.broadcast_to(cond / (1.0 + jnp.exp(-cond)), (16, cond.shape[1])).astype(bf16)
    for i in range(3):
        mod_part[s, :, i * mod_cols : (i + 1) * mod_cols] = jnp.dot(
            lifted, mod_w[i], preferred_element_type=f32
        )[0:1]
    line_start(mod_at, modz_send, modz_recv)
    for copy in pair_copies[1:4]:
        copy.start()

    def wo_line(j, c, toward):
        part = wo.at[far, wo_rows(g, j, c)]
        return remote(
            part, part, wo_send.at[toward, j, c], wo_recv.at[j, c], (left_dev, right_dev)[toward]
        )

    def wo_across(j, c):
        part = wo.at[far, wo_rows(g, j, c)]
        return remote(part, part, woy_send, woy_recv.at[j, c], y_dev)

    def wo_share(j, c):
        part = wo.at[far, wo_rows(1 - g, j, c)]
        remote(part, part, woy_send, woy_recv.at[j, c], y_dev).wait_recv()
        remote(part, part, wop_send.at[1 - g], wop_recv.at[1 - g], pair_dev).start()

    def wo_shares(k):
        def step(c, carry):
            for j, there in ((s - k, s >= k), (s + k, s + k < sp)):

                @pl.when(there)
                def _():
                    wo_share(j, c)

            return carry

        lax.fori_loop(0, WEIGHT_CHUNKS, step, 0)

    def wo_share_own():
        def step(c, carry):
            wo_share(s, c)
            return carry

        lax.fori_loop(0, WEIGHT_CHUNKS, step, 0)

    def wo_own(c):
        wo_line(s, c, 0).wait_recv()
        wo_across(s, c).start()

    def wo_own_line(c):
        for toward, has in ((0, has_left), (1, has_right)):

            @pl.when(has)
            def _():
                wo_line(s, c, toward).start()

    def wo_relay(e):
        k, c = e // WEIGHT_CHUNKS, lax.rem(e, WEIGHT_CHUNKS)
        for toward, has, j, there in (
            (1, has_right, s - k, s >= k),
            (0, has_left, s + k, s + k < sp),
        ):

            @pl.when(there)
            def _():
                wo_line(j, c, toward).wait_recv()

                @pl.when(has)
                def _():
                    wo_line(j, c, toward).start()

                wo_across(j, c).start()

    def wo_relays(low, high):
        def step(e, carry):
            wo_relay(e)
            return carry

        lax.fori_loop(low, high, step, 0)

    quarter = HD // 4
    inverse = jnp.exp(
        lax.rem(lane, quarter).astype(f32) * (-jnp.log(jnp.float32(rope_base)) / quarter)
    )
    first = lax.rem(lane, 2 * quarter) < quarter
    by_row = lax.rem(lane, HD) < HD // 2

    def tables(b, carry):
        place = s * total + jnp.where(b == 0, t, far) * rows + row
        coordinate = jnp.where(by_row, place // GRID_W, lax.rem(place, GRID_W))
        angles = coordinate.astype(f32) * inverse
        turn_cos[b] = jnp.cos(angles)
        sines = jnp.sin(angles)
        turn_sin[b] = jnp.where(first, -sines, sines)
        return carry

    contract = (((1,), (1,)), ((), ()))
    band = 3 * rows
    pairs = kw // HD
    stack = group * rows

    def biases(block, carry):
        q_pos = lax.broadcasted_iota(jnp.int32, (band, rows), 1)
        k_pos = lax.broadcasted_iota(jnp.int32, (band, rows), 0)
        place = s * total + jnp.where(block == 0, t, far) * rows - WIN + k_pos
        allowed = jnp.logical_and(
            jnp.logical_and(k_pos >= q_pos, k_pos <= q_pos + 2 * WIN),
            jnp.logical_and(place >= 0, place < sp * total),
        )
        bias[block] = jnp.where(allowed, 0.0, neg_large)
        return carry

    wo_own(0)
    wo_own_line(0)
    line_relay(1, mod_at, modz_send, modz_recv)
    line_relay(1, ctx_at, ctxz_send, ctxz_recv)
    wo_own(1)
    lax.fori_loop(0, 2, tables, 0)
    lax.fori_loop(0, 2, biases, 0)
    line_relay(2, mod_at, modz_send, modz_recv)
    for j in range(2, AHEAD):
        lat_copy(j).start()
    wo_own_line(1)
    for c in range(2, WEIGHT_CHUNKS):
        wo_own(c)
        wo_own_line(c)
    wo_relays(WEIGHT_CHUNKS, WEIGHT_CHUNKS + 1)
    pair_copies[4].start()
    line_relay(2, ctx_at, ctxz_send, ctxz_recv)
    for k in range(3, sp):
        line_relay(k, mod_at, modz_send, modz_recv)
    summed = mod_part[0]
    for k in range(1, sp):
        summed = summed + mod_part[k]
    mod_all[t] = summed
    mods = []
    for k in range(1, tp):
        copy = remote(
            mod_all.at[t],
            mod_all.at[t],
            modt_send.at[k - 1],
            modt_recv.at[k - 1],
            {"tp": lax.rem(t + k, tp)},
        )
        copy.start()
        mods.append(copy)
    for j in range(AHEAD, LATENT_CHUNKS):
        lat_copy(j).start()
    wo_relays(WEIGHT_CHUNKS + 1, WEIGHT_CHUNKS + 3)
    stat_copy.wait_recv()
    column = jnp.sum(
        jnp.where(diagonal, jnp.broadcast_to(stat_in[0:1], (rows, 128)), 0.0), axis=1, keepdims=True
    )
    row_scale[1] = jnp.broadcast_to(column, (rows, 128))

    for copy in mods:
        copy.wait_recv()
    for i in range(tp):
        cols = slice(i * mod_cols, (i + 1) * mod_cols)
        shift_v[:, cols] = mod_all[i, :, 0:mod_cols]
        factor_v[:, cols] = gain_v[:, cols] * (1.0 + mod_all[i, :, mod_cols : 2 * mod_cols])
        gate_v[:, cols] = mod_all[i, :, 2 * mod_cols : 3 * mod_cols]

    def normalize(block, source, cols, lanes, target):
        scale = row_scale[block]
        for at in range(0, lanes, 128):
            here = pl.ds(pl.multiple_of(cols + at, 128), 128)
            values = source[:, here].astype(f32) * scale
            target[:, at : at + 128] = (values * factor_v[:, here] + shift_v[:, here]).astype(bf16)

    def project(j):
        normalize(1, lat_far, j * chunk, chunk, normed)
        cols = pl.ds(pl.multiple_of(j * chunk, 128), chunk)
        for slot in range(2):
            acc[slot] += jnp.dot(
                normed[:, 0:chunk], proj_w[slot, cols], preferred_element_type=f32
            )

    low = lane < HD

    def finish_projection(block, position):
        cosine, sine = turn_cos[block], turn_sin[block]

        def turned(values):
            swapped = jnp.where(
                first, pltpu.roll(values, 128 - quarter, 1), pltpu.roll(values, quarter, 1)
            )
            return values * cosine + swapped * sine

        factor = HD ** (-0.5)
        base = pl.ds(pl.multiple_of(position * rows, rows), rows)
        for slot in range(2):
            key_value[slot, base, 0:kw] = turned(acc[slot, :, qw : qw + kw]).astype(bf16)
            key_value[slot, base, kw : 2 * kw] = acc[slot, :, qw + kw : qw + 2 * kw].astype(bf16)
            for u in range(heads // 2):
                lanes = turned(acc[slot, :, u * 128 : (u + 1) * 128]).astype(bf16)
                swapped = pltpu.roll(lanes.astype(f32), HD, 1) * factor
                lanes = lanes.astype(f32) * factor
                keep = low if u == 0 else jnp.logical_not(low)
                for at in range(2):
                    aligned = lanes if at == u else swapped
                    queries[block, slot, u, at * rows : (at + 1) * rows] = jnp.where(
                        keep, aligned, 0.0
                    ).astype(bf16)

    def kv_at(position):
        return key_value.at[:, pl.ds(pl.multiple_of(position * rows, rows), rows)]

    def kv_pair(block, position):
        return remote(
            kv_at(position), kv_at(position), kv_send.at[block], kv_recv.at[block], pair_dev
        )

    halo_down = remote(
        kv_at(1), kv_at(tp + 1), halo_sem.at[0], halo_sem.at[1], {**left_dev, "tp": pair}
    )
    halo_up = remote(kv_at(tp), kv_at(0), halo_sem.at[0], halo_sem.at[1], {**right_dev, "tp": pair})
    sends_down = jnp.logical_and(core == 0, has_left)
    sends_up = jnp.logical_and(core == 1, has_right)

    def send_halo(mine):
        @pl.when(jnp.logical_and(mine, sends_down))
        def _():
            halo_down.start()

        @pl.when(jnp.logical_and(mine, sends_up))
        def _():
            halo_up.start()

    def wait_halo(mine):
        @pl.when(jnp.logical_and(mine, sends_down))
        def _():
            halo_up.wait_recv()

        @pl.when(jnp.logical_and(mine, sends_up))
        def _():
            halo_down.wait_recv()

    def context_part(block, slot):
        units = range(pairs)
        scores = [
            lax.dot_general(
                ctx_kv[slot, :, 0:kw],
                queries[block, slot, u],
                contract,
                preferred_element_type=f32,
            )
            for u in units
        ]
        sinks = [
            jnp.concatenate(
                [sink_v[slot, u * group + h : u * group + h + 1] for h in range(group)], axis=1
            )
            for u in units
        ]
        tops = [
            jnp.maximum(jnp.max(scores[u], axis=0, keepdims=True), sinks[u]) for u in units
        ]
        exps = [jnp.exp(scores[u] - tops[u]) for u in units]
        for u in units:
            part_top[block, slot, u] = tops[u]
            part_sum[block, slot, u] = jnp.sum(exps[u], axis=0, keepdims=True) + jnp.exp(
                sinks[u] - tops[u]
            )
            part_out[block, slot, u] = jnp.dot(
                ctx_vt[slot, u * HD : (u + 1) * HD],
                exps[u].astype(bf16),
                preferred_element_type=f32,
            )

    def window_part(block, position, slot, target):
        units = range(pairs)
        window = pl.ds(pl.multiple_of((position - 1) * rows, rows), band)
        mask = jnp.concatenate([bias[block]] * group, axis=1)
        scores = [
            lax.dot_general(
                key_value[slot, window, 0:kw],
                queries[block, slot, u],
                contract,
                preferred_element_type=f32,
            )
            + mask
            for u in units
        ]
        befores = [part_top[block, slot, u] for u in units]
        tops = [
            jnp.maximum(jnp.max(scores[u], axis=0, keepdims=True), befores[u]) for u in units
        ]
        exps = [jnp.exp(scores[u] - tops[u]) for u in units]
        keeps = [jnp.exp(befores[u] - tops[u]) for u in units]
        values = jnp.transpose(key_value[slot, window, kw : 2 * kw])
        for u in units:
            bottom = (
                jnp.sum(exps[u], axis=0, keepdims=True) + part_sum[block, slot, u] * keeps[u]
            )
            result = (
                jnp.dot(
                    values[u * HD : (u + 1) * HD],
                    exps[u].astype(bf16),
                    preferred_element_type=f32,
                )
                + part_out[block, slot, u] * keeps[u]
            ) / bottom
            turned_back = jnp.concatenate(
                [result[:, h * rows : (h + 1) * rows] for h in range(group)], axis=0
            )
            target[slot, :, u * 128 : (u + 1) * 128] = jnp.transpose(turned_back).astype(bf16)

    edge = jnp.zeros((2, rows, 2 * kw), bf16)

    @pl.when(jnp.logical_and(core == 0, jnp.logical_not(has_left)))
    def _():
        key_value[:, 0:rows] = edge

    @pl.when(jnp.logical_and(core == 1, jnp.logical_not(has_right)))
    def _():
        key_value[:, (tp + 1) * rows : (tp + 2) * rows] = edge

    for i in range(10, 12):
        loads[i].wait()
    for copy in pair_copies[0:4]:
        copy.wait_recv()

    def far_step(j, carry):
        lat_copy(j).wait_recv()
        project(j)
        return carry

    normalize(0, lat_own, 0, width, normed)
    for slot in range(2):
        acc[slot] = jnp.dot(normed[...], proj_w[slot], preferred_element_type=f32)
    finish_projection(0, t + 1)
    kv_pair(0, t + 1).start()
    send_halo(chip == core)
    def wo_pair(gg):
        part = wo.at[far, pl.ds(pl.multiple_of(gg * sp * shard, 16), sp * shard)]
        return remote(part, part, wop_send.at[gg], wop_recv.at[gg], pair_dev)


    def wo_last(c):
        for k in range(3, sp):
            wo_relays(k * WEIGHT_CHUNKS + c, k * WEIGHT_CHUNKS + c + 1)

    wo_relays(WEIGHT_CHUNKS + 3, 2 * WEIGHT_CHUNKS + 1)
    for slot in range(2):
        acc[slot] = jnp.zeros(acc.shape[1:], f32)
    lax.fori_loop(0, 3, far_step, 0)
    wo_relays(2 * WEIGHT_CHUNKS + 1, 3 * WEIGHT_CHUNKS)
    for k in range(3, sp):
        line_relay(k, ctx_at, ctxz_send, ctxz_recv)
    ctx_pair = remote(ctx_kv.at[core], ctx_kv.at[core], ctxp_sem.at[0], ctxp_sem.at[1], pair_dev)
    ctx_pair.start()
    lax.fori_loop(3, 5, far_step, 0)
    ctx_pair.wait_recv()
    for slot in range(2):
        ctx_vt[slot] = jnp.transpose(ctx_kv[slot, :, kw : 2 * kw])

    for slot in range(2):
        context_part(0, slot)
    wo_last(0)
    lax.fori_loop(5, 6, far_step, 0)
    wo_last(1)
    lax.fori_loop(6, 7, far_step, 0)
    wo_last(2)
    lax.fori_loop(7, LATENT_CHUNKS, far_step, 0)
    finish_projection(1, far + 1)
    kv_pair(1, far + 1).start()
    send_halo(chip != core)

    for c in range(3, WEIGHT_CHUNKS):
        wo_last(c)
    wo_pair(g).start()
    for slot in range(2):
        context_part(1, slot)
    wo_share_own()
    wo_shares(1)
    kv_pair(0, pair + 1).wait_recv()

    def att_copy(slot):
        return remote(
            att_out.at[slot], att.at[chip, slot], att_send.at[slot], att_recv.at[slot], far_dev
        )

    kv_pair(1, pair + 1).wait_recv()
    wait_halo(chip != core)

    def far_attend(n, carry):
        window_part(1, far + 1, n, att_out)
        att_copy(n).start()
        return carry

    lax.fori_loop(0, 2, far_attend, 0)
    wo_shares(2)
    wait_halo(chip == core)

    def own_attend(n, carry):
        window_part(0, t + 1, n, att.at[chip])
        return carry

    lax.fori_loop(0, 2, own_attend, 0)
    for k in range(3, sp):
        wo_shares(k)
    pair_copies[4].wait_recv()

    def out_product(x, i):
        sums = None
        for slot in range(2):
            part = pl.ds(pl.multiple_of((2 * x + slot) * qw, qw), qw)
            product = jnp.dot(att[x, slot], wo[i, part], preferred_element_type=f32)
            sums = product if sums is None else sums + product
        return sums

    order = (t, pair, far, (1 - chip) * 2 + 1 - core)
    other = (1 - chip) * 2 + 1 - core
    for k, i in enumerate(order):
        if k == 3:
            for gg in range(2):
                part = wo.at[other, pl.ds(gg * sp * shard, sp * shard)]
                remote(part, part, wop_send.at[gg], wop_recv.at[gg], pair_dev).wait_recv()
        out_part[k] = out_product(chip, i)
    att_copy(0).wait_recv()
    att_copy(1).wait_recv()
    for k, i in enumerate(order):
        cols = pl.ds(pl.multiple_of(i * out_width, 128), out_width)
        blended = (out_part[k] + out_product(1 - chip, i)).astype(bf16).astype(f32)
        mixed[:, cols] = (lat_own[:, cols].astype(f32) + gate_v[:, cols] * blended).astype(bf16)

    stat_copy.wait_send()
    for c in range(WEIGHT_CHUNKS):
        wo_cross(c).wait_send()
    for j in range(LATENT_CHUNKS):
        lat_copy(j).wait_send()
    for copy in pair_copies:
        copy.wait_send()
    for copy in mods:
        copy.wait_send()
    line_finish(mod_at, modz_send, modz_recv)
    line_finish(ctx_at, ctxz_send, ctxz_recv)
    ctx_pair.wait_send()
    for j in range(sp):
        for toward, has, sent in ((1, has_right, j <= s), (0, has_left, j >= s)):

            @pl.when(jnp.logical_and(has, sent))
            def _():
                def step(c, carry):
                    wo_line(j, c, toward).wait_send()
                    return carry

                lax.fori_loop(0, WEIGHT_CHUNKS, step, 0)

    wo_sent = wo.at[far, pl.ds(pl.multiple_of(g * sp * shard, 16), sp * shard)]
    remote(wo_sent, wo_sent, woy_send, woy_recv.at[0, 0], y_dev).wait_send()
    wo_pair(0).wait_send()
    wo_pair(1).wait_send()
    kv_pair(0, t + 1).wait_send()
    kv_pair(1, far + 1).wait_send()

    @pl.when(sends_down)
    def _():
        halo_down.wait_send()

    @pl.when(sends_up)
    def _():
        halo_up.wait_send()

    att_copy(0).wait_send()
    att_copy(1).wait_send()


def local(
    latent,
    context,
    conditioning,
    norm_gain,
    shift_weight,
    scale_weight,
    gate_weight,
    query_weight,
    key_weight,
    value_weight,
    out_weight,
    sink_logit,
):
    tp, sp, grp = lax.axis_size("tp"), lax.axis_size("sp"), lax.axis_size("grp")
    rows, width = latent.shape
    ctx_rows = context.shape[0]
    mod_rows, mod_cols = shift_weight.shape
    query_width, key_width = query_weight.shape[1], key_weight.shape[1]
    out_rows, out_width = out_weight.shape
    fits = (
        rows == WIN
        and rows == 128
        and key_width == 2 * HD
        and query_width == 4 * HD
        and tp == 4
        and grp == 2
        and sp >= 3
        and sp * ctx_rows % 128 == 0
        and ctx_rows % CONTEXT_ROWS == 0
        and width % 512 == 0
        and mod_cols % 128 == 0
        and width % (128 * LATENT_CHUNKS) == 0
        and out_width % 128 == 0
        and tp * out_width == width
        and out_rows == tp * query_width
        and out_rows % (2 * sp * WEIGHT_CHUNKS * 16) == 0
    )
    if not fits:
        return local_plain(
            latent,
            context,
            conditioning,
            norm_gain,
            shift_weight,
            scale_weight,
            gate_weight,
            query_weight,
            key_weight,
            value_weight,
            out_weight,
            sink_logit,
        )
    f32, bf16 = jnp.float32, jnp.bfloat16
    dma = pltpu.SemaphoreType.DMA
    anywhere = pl.BlockSpec(memory_space=pl.ANY)
    return pl.pallas_call(
        functools.partial(fused_kernel, sp),
        out_shape=pltpu.VMEM((rows, width), bf16),
        in_specs=[anywhere] * 11 + [pl.BlockSpec(memory_space=pltpu.SMEM)],
        out_specs=pl.BlockSpec(memory_space=pltpu.VMEM),
        scratch_shapes=[
            pltpu.VMEM((mod_rows,), bf16),
            pltpu.VMEM((1, width), f32),
            pltpu.VMEM((3, mod_rows, mod_cols), bf16),
            pltpu.VMEM((2, width, query_width + 2 * key_width), bf16),
            pltpu.VMEM((tp, out_rows, out_width), bf16),
            pltpu.VMEM((out_rows // (2 * sp), out_width), bf16),
            pltpu.VMEM(context.shape, bf16),
            pltpu.VMEM((rows, width), bf16),
            pltpu.VMEM((rows, width), bf16),
            pltpu.VMEM((rows, width), bf16),
            pltpu.VMEM((8, 128), f32),
            pltpu.VMEM((8, 128), f32),
            pltpu.VMEM((2, rows, 128), f32),
            pltpu.VMEM((2, 8, 128), f32),
            pltpu.VMEM((sp, 1, 3 * mod_cols), f32),
            pltpu.VMEM((tp, 1, 3 * mod_cols), f32),
            pltpu.VMEM((1, width), f32),
            pltpu.VMEM((1, width), f32),
            pltpu.VMEM((1, width), f32),
            pltpu.VMEM((2, rows, 128), f32),
            pltpu.VMEM((2, rows, 128), f32),
            pltpu.VMEM((2, rows, query_width + 2 * key_width), f32),
            pltpu.VMEM((2, 2, 2, 2 * rows, key_width), bf16),
            pltpu.VMEM((2, (tp + 2) * rows, 2 * key_width), bf16),
            pltpu.VMEM((2, sp * ctx_rows, 2 * key_width), bf16),
            pltpu.VMEM((2, 2, rows, query_width), bf16),
            pltpu.VMEM((2, rows, query_width), bf16),
            pltpu.VMEM((2, key_width, sp * ctx_rows), bf16),
            pltpu.VMEM((2, 3 * rows, rows), f32),
            pltpu.VMEM((2, 2, 2, HD, 2 * rows), f32),
            pltpu.VMEM((2, 2, 2, 1, 2 * rows), f32),
            pltpu.VMEM((2, 2, 2, 1, 2 * rows), f32),
            pltpu.VMEM((tp, rows, out_width), f32),
            dma((12,)),
            dma((LATENT_CHUNKS,)),
            dma((LATENT_CHUNKS,)),
            dma((2,)),
            dma((5,)),
            dma((5,)),
            dma((WEIGHT_CHUNKS,)),
            dma((2, sp, WEIGHT_CHUNKS)),
            dma((sp, WEIGHT_CHUNKS)),
            dma,
            dma((sp, WEIGHT_CHUNKS)),
            dma((2,)),
            dma((2,)),
            dma((2, sp)),
            dma((sp,)),
            dma((tp - 1,)),
            dma((tp - 1,)),
            dma((2, sp)),
            dma((sp,)),
            dma((2,)),
            dma((2,)),
            dma((2,)),
            dma((2,)),
            dma((2,)),
            dma((2,)),
        ],
        compiler_params=pltpu.CompilerParams(
            collective_id=0, has_side_effects=True, vmem_limit_bytes=60 * 1024 * 1024
        ),
        name="fused",
    )(
        latent,
        context,
        conditioning,
        norm_gain.reshape(1, width),
        shift_weight,
        scale_weight,
        gate_weight,
        query_weight,
        key_weight,
        value_weight,
        out_weight,
        sink_logit,
    )


def solution(mesh):
    in_specs = (
        P(("grp", "sp", "tp"), None),
        P(("grp", "sp"), None),
        P(("grp", "sp")),
        P(),
        P("sp", "tp"),
        P("sp", "tp"),
        P("sp", "tp"),
        P(None, "tp"),
        P(None, "tp"),
        P(None, "tp"),
        P(None, "tp"),
        P("tp"),
    )
    out_specs = P(("grp", "sp", "tp"), None)
    return jax.shard_map(local, mesh=mesh, in_specs=in_specs, out_specs=out_specs, check_vma=False)
```

```python
import functools

import jax
import jax.numpy as jnp
from jax import lax
from jax.experimental import pallas as pl
from jax.experimental.pallas import tpu as pltpu
from jax.sharding import PartitionSpec as P

HEADS = 16
KV_HEADS = 8
HD = 64
GRID_W = 64
WIN = 128


epsilon = 1e-06
rope_base = 10000.0
neg_large = -1e30


def with_halo(cells, sides, width):
    for axis, dim in sides:
        count = lax.axis_size(axis)
        ends = count - 1
        head = lax.slice_in_dim(cells, 0, width, axis=dim)
        tail = lax.slice_in_dim(cells, cells.shape[dim] - width, cells.shape[dim], axis=dim)
        cells = jnp.concatenate(
            [
                lax.ppermute(tail, axis, [(i, (i + 1) % count) for i in range(ends)]),
                cells,
                lax.ppermute(head, axis, [((i + 1) % count, i) for i in range(ends)]),
            ],
            axis=dim,
        )
    return cells


def row_norm(matrix, norm_gain):
    values = matrix.astype(jnp.float32)
    return (
        values * lax.rsqrt(jnp.mean(values * values, axis=-1, keepdims=True) + epsilon) * norm_gain
    )


def axial_turn(values, position):
    half_dim = values.shape[-1] // 2
    quarter = half_dim // 2
    inverse = rope_base ** (-jnp.arange(quarter, dtype=jnp.float32) / quarter)

    def turn(section, coordinate):
        angles = coordinate.astype(jnp.float32)[:, None] * inverse[None, :]
        cosine = jnp.cos(angles)[:, None, :]
        sine_part = jnp.sin(angles)[:, None, :]
        leading = section[..., :quarter]
        trailing = section[..., quarter:]
        return jnp.concatenate(
            [leading * cosine - trailing * sine_part, leading * sine_part + trailing * cosine],
            axis=-1,
        )

    return jnp.concatenate(
        [
            turn(values[..., :half_dim], position // GRID_W),
            turn(values[..., half_dim:], position % GRID_W),
        ],
        axis=-1,
    )


def context_pairs(context_rows, norm_gain, key_weight, value_weight):
    prepared = row_norm(context_rows, norm_gain).astype(jnp.bfloat16)
    return jnp.concatenate(
        [
            jnp.dot(prepared, key_weight, preferred_element_type=jnp.float32),
            jnp.dot(prepared, value_weight, preferred_element_type=jnp.float32),
        ],
        axis=1,
    ).astype(jnp.bfloat16)


def local_plain(
    latent,
    context,
    conditioning,
    norm_gain,
    shift_weight,
    scale_weight,
    gate_weight,
    query_weight,
    key_weight,
    value_weight,
    out_weight,
    sink_logit,
):
    lifted = jax.nn.silu(conditioning.astype(jnp.float32)).astype(jnp.bfloat16)[None, :]
    shift_part = jnp.dot(lifted, shift_weight, preferred_element_type=jnp.float32)[0]
    scale_part = jnp.dot(lifted, scale_weight, preferred_element_type=jnp.float32)[0]
    gate_part = jnp.dot(lifted, gate_weight, preferred_element_type=jnp.float32)[0]
    summed = lax.psum((shift_part, scale_part, gate_part), "sp")
    shift_vec, scale_vec, gate_vec = (
        lax.all_gather(summed[0], "tp", axis=0, tiled=True),
        lax.all_gather(summed[1], "tp", axis=0, tiled=True),
        lax.all_gather(summed[2], "tp", axis=0, tiled=True),
    )
    normed = (row_norm(latent, norm_gain) * (1.0 + scale_vec) + shift_vec).astype(jnp.bfloat16)
    segment = lax.all_gather(normed, "tp", axis=0, tiled=True)
    projected = jnp.concatenate(
        [
            jnp.dot(segment, query_weight, preferred_element_type=jnp.float32),
            jnp.dot(segment, key_weight, preferred_element_type=jnp.float32),
            jnp.dot(segment, value_weight, preferred_element_type=jnp.float32),
        ],
        axis=1,
    )
    row_count = projected.shape[0]
    query_width = query_weight.shape[1]
    key_width = key_weight.shape[1]
    query_heads = query_width // HD
    pair_heads = key_width // HD
    group_size = HEADS // KV_HEADS
    row_offset = lax.axis_index("sp") * row_count
    position = row_offset + jnp.arange(row_count, dtype=jnp.int32)
    queries = axial_turn(
        projected[:, :query_width].reshape(row_count, query_heads, HD), position
    ).astype(jnp.bfloat16)
    latent_keys = axial_turn(
        projected[:, query_width : query_width + key_width].reshape(row_count, pair_heads, HD),
        position,
    ).astype(jnp.bfloat16)
    latent_values = projected[:, query_width + key_width :].astype(jnp.bfloat16)
    key_value = jnp.concatenate([latent_keys.reshape(row_count, key_width), latent_values], axis=1)
    widened = with_halo(key_value, (("sp", 0),), WIN)
    context_all = lax.all_gather(
        context_pairs(context, norm_gain, key_weight, value_weight), "sp", axis=0, tiled=True
    )
    block_count = row_count // WIN
    context_count = context_all.shape[0]
    query_blocks = queries.reshape(block_count, WIN, pair_heads, group_size, HD)
    band_blocks = widened.reshape(block_count + 2, WIN, 2 * key_width)
    band_rows = jnp.concatenate(
        [band_blocks[:block_count], band_blocks[1 : block_count + 1], band_blocks[2:]], axis=1
    )
    band_keys = band_rows[..., :key_width].reshape(block_count, 3 * WIN, pair_heads, HD)
    band_values = band_rows[..., key_width:].reshape(block_count, 3 * WIN, pair_heads, HD)
    context_keys = context_all[:, :key_width].reshape(context_count, pair_heads, HD)
    context_values = context_all[:, key_width:].reshape(context_count, pair_heads, HD)
    factor = HD ** (-0.5)
    local_scores = (
        jnp.einsum("nqhgd,nkhd->nhgqk", query_blocks, band_keys, preferred_element_type=jnp.float32)
        * factor
    )
    query_pos = position.reshape(block_count, WIN)
    key_pos = (
        row_offset
        - WIN
        + jnp.arange(block_count, dtype=jnp.int32)[:, None] * WIN
        + jnp.arange(3 * WIN, dtype=jnp.int32)[None, :]
    )
    seq_total = row_count * lax.axis_size("sp")
    allowed = (
        (jnp.abs(key_pos[:, None, :] - query_pos[:, :, None]) <= WIN)
        & (key_pos[:, None, :] >= 0)
        & (key_pos[:, None, :] < seq_total)
    )
    local_scores = jnp.where(allowed[:, None, None], local_scores, neg_large)
    context_scores = (
        jnp.einsum(
            "nqhgd,thd->nhgqt", query_blocks, context_keys, preferred_element_type=jnp.float32
        )
        * factor
    )
    sink_values = sink_logit.reshape(pair_heads, group_size)[None, :, :, None, None]
    highest = jnp.maximum(
        jnp.maximum(
            jnp.max(local_scores, axis=-1, keepdims=True),
            jnp.max(context_scores, axis=-1, keepdims=True),
        ),
        sink_values,
    )
    local_exp = jnp.exp(local_scores - highest)
    context_exp = jnp.exp(context_scores - highest)
    denominator = (
        jnp.sum(local_exp, axis=-1, keepdims=True)
        + jnp.sum(context_exp, axis=-1, keepdims=True)
        + jnp.exp(sink_values - highest)
    )
    local_weights = (local_exp / denominator).astype(jnp.bfloat16)
    context_weights = (context_exp / denominator).astype(jnp.bfloat16)
    attended = jnp.einsum(
        "nhgqk,nkhd->nqhgd", local_weights, band_values, preferred_element_type=jnp.float32
    ) + jnp.einsum(
        "nhgqt,thd->nqhgd", context_weights, context_values, preferred_element_type=jnp.float32
    )
    attended = attended.reshape(row_count, query_width).astype(jnp.bfloat16)
    columns_part = jnp.dot(
        lax.all_gather(attended, "tp", axis=1, tiled=True),
        out_weight,
        preferred_element_type=jnp.float32,
    ).astype(jnp.bfloat16)
    blended = lax.all_to_all(columns_part, "tp", split_axis=0, concat_axis=1, tiled=True)
    return (latent.astype(jnp.float32) + gate_vec * blended.astype(jnp.float32)).astype(
        jnp.bfloat16
    )


LATENT_CHUNKS = 8
WEIGHT_CHUNKS = 4
AHEAD = 3
NORM_ROWS = 16
CONTEXT_ROWS = 32


def remote(src, dst, send, recv, device):
    return pltpu.make_async_remote_copy(
        src_ref=src,
        dst_ref=dst,
        send_sem=send,
        recv_sem=recv,
        device_id=device,
        device_id_type=pl.DeviceIdType.MESH,
    )


def fused_kernel(
    sp,
    latent,
    context,
    conditioning,
    norm_gain,
    shift_weight,
    scale_weight,
    gate_weight,
    query_weight,
    key_weight,
    value_weight,
    out_weight,
    sink,
    mixed,
    cond_v,
    gain_v,
    mod_w,
    proj_w,
    wo,
    wo_shard,
    ctx_v,
    lat_own,
    lat_far,
    normed,
    stat_out,
    stat_in,
    row_scale,
    sink_v,
    mod_part,
    mod_all,
    factor_v,
    shift_v,
    gate_v,
    turn_cos,
    turn_sin,
    acc,
    queries,
    key_value,
    ctx_kv,
    att,
    att_out,
    ctx_vt,
    bias,
    part_out,
    part_top,
    part_sum,
    out_part,
    load_sem,
    lat_send,
    lat_recv,
    stat_sem,
    pair_send,
    pair_recv,
    wox_send,
    wo_send,
    wo_recv,
    woy_send,
    woy_recv,
    wop_send,
    wop_recv,
    modz_send,
    modz_recv,
    modt_send,
    modt_recv,
    ctxz_send,
    ctxz_recv,
    ctxp_sem,
    kv_send,
    kv_recv,
    halo_sem,
    att_send,
    att_recv,
):
    g = lax.axis_index("grp")
    s = lax.axis_index("sp")
    t = lax.axis_index("tp")
    chip = t // 2
    core = lax.rem(t, 2)
    pair = chip * 2 + 1 - core
    far = (1 - chip) * 2 + core
    pair_dev, far_dev, y_dev = {"tp": pair}, {"tp": far}, {"grp": 1 - g}
    right_dev = {"sp": lax.rem(s + 1, sp)}
    left_dev = {"sp": lax.rem(s + sp - 1, sp)}
    has_right, has_left = s < sp - 1, s > 0
    rows, width = latent.shape
    ctx_rows = context.shape[0]
    mod_cols = shift_weight.shape[1]
    qw = query_weight.shape[1]
    kw = key_weight.shape[1]
    heads = qw // HD
    group = heads // (kw // HD)
    tp = 4
    total = tp * rows
    out_rows, out_width = out_weight.shape
    half = rows // 2
    f32, bf16 = jnp.float32, jnp.bfloat16
    chunk = width // LATENT_CHUNKS
    shard = out_rows // (2 * sp)
    slab = shard // WEIGHT_CHUNKS
    MESH = pl.DeviceIdType.MESH

    loads = [
        (out_weight.at[pl.ds(pl.multiple_of((g * sp + s) * shard, 16), shard)], wo_shard),
        (latent, lat_own),
        (norm_gain, gain_v),
        (context, ctx_v),
        (key_weight, proj_w.at[core, :, qw : qw + kw]),
        (value_weight, proj_w.at[core, :, qw + kw : qw + 2 * kw]),
        (conditioning, cond_v),
        (shift_weight, mod_w.at[0]),
        (scale_weight, mod_w.at[1]),
        (gate_weight, mod_w.at[2]),
        (query_weight, proj_w.at[core, :, 0:qw]),
        (out_weight, wo.at[t]),
    ]
    loads = [pltpu.make_async_copy(a, b, load_sem.at[i]) for i, (a, b) in enumerate(loads)]
    for load in loads:
        load.start()

    barrier = pltpu.get_barrier_semaphore()
    for k in range(1, tp):
        pl.semaphore_signal(
            barrier, inc=1, device_id={"tp": lax.rem(t + k, tp)}, device_id_type=MESH
        )
    pl.semaphore_signal(barrier, inc=1, device_id=y_dev, device_id_type=MESH)
    for has, place in ((has_right, right_dev), (has_left, left_dev)):

        @pl.when(has)
        def _():
            for peer in (t, pair):
                pl.semaphore_signal(
                    barrier, inc=1, device_id={**place, "tp": peer}, device_id_type=MESH
                )

    def row_factor(source, part):
        squares = None
        for at in range(0, width, 512):
            values = source[part, at : at + 512].astype(f32)
            values = values * values
            squares = values if squares is None else squares + values
        return lax.rsqrt(jnp.sum(squares, axis=-1, keepdims=True) * (1.0 / width) + epsilon)

    lane = lax.broadcasted_iota(jnp.int32, (rows, 128), 1)
    row = lax.broadcasted_iota(jnp.int32, (rows, 128), 0)
    diagonal = lane == row

    pl.semaphore_wait(
        barrier, tp + jnp.where(has_right, 2, 0) + jnp.where(has_left, 2, 0)
    )

    def lat_copy(j):
        cols = pl.ds(pl.multiple_of(j * chunk, 128), chunk)
        return remote(
            lat_own.at[:, cols], lat_far.at[:, cols], lat_send, lat_recv.at[j], far_dev
        )

    def wo_rows(gg, j, c):
        return pl.ds(pl.multiple_of((gg * sp + j) * shard + c * slab, 16), slab)

    def wo_cross(c):
        part = wo_rows(g, s, c)
        return remote(
            wo_shard.at[pl.ds(c * slab, slab)],
            wo.at[t, part],
            wox_send,
            wo_recv.at[s, c],
            far_dev,
        )

    loads[0].wait()
    for c in range(WEIGHT_CHUNKS):
        wo_cross(c).start()
    loads[1].wait()

    def row_stat(i, carry):
        part = pl.ds(pl.multiple_of(i * CONTEXT_ROWS, 16), CONTEXT_ROWS)
        row_scale[0, part] = jnp.broadcast_to(row_factor(lat_own, part), (CONTEXT_ROWS, 128))
        return carry

    lax.fori_loop(0, rows // CONTEXT_ROWS, row_stat, 0)
    flat = jnp.sum(jnp.where(diagonal, row_scale[0], 0.0), axis=0, keepdims=True)
    stat_out[...] = jnp.broadcast_to(flat, (8, 128))
    sink_row = lax.broadcasted_iota(jnp.int32, (8, 128), 0)
    sink_all = jnp.full((8, 128), sink[0], f32)
    for h in range(1, heads):
        sink_all = jnp.where(sink_row == h, sink[h], sink_all)
    sink_v[core] = sink_all

    stat_copy = remote(stat_out, stat_in, stat_sem.at[0], stat_sem.at[1], far_dev)
    stat_copy.start()
    for j in range(2):
        lat_copy(j).start()
    pair_copies = [
        (sink_v.at[core], sink_v.at[core]),
        (query_weight, proj_w.at[core, :, 0:qw]),
        (key_weight, proj_w.at[core, :, qw : qw + kw]),
        (value_weight, proj_w.at[core, :, qw + kw : qw + 2 * kw]),
        (out_weight, wo.at[t]),
    ]
    pair_copies = [
        remote(a, b, pair_send.at[i], pair_recv.at[i], pair_dev)
        for i, (a, b) in enumerate(pair_copies)
    ]
    pair_copies[0].start()

    def line_copy(at, j, send, recv, toward):
        return remote(at(j), at(j), send.at[toward], recv.at[j], (left_dev, right_dev)[toward])

    def line_start(at, send, recv):
        for toward, has in ((0, has_left), (1, has_right)):

            @pl.when(has)
            def _():
                line_copy(at, s, send, recv, toward).start()

    def line_relay(k, at, send, recv):
        for toward, has, j, there in (
            (1, has_right, s - k, s >= k),
            (0, has_left, s + k, s + k < sp),
        ):

            @pl.when(there)
            def _():
                line_copy(at, j, send, recv, toward).wait_recv()

                @pl.when(has)
                def _():
                    line_copy(at, j, send, recv, toward).start()

    def line_finish(total_of, send):
        for toward, has, sent in ((1, has_right, s + 1), (0, has_left, sp - s)):
            for count in range(1, sp + 1):

                @pl.when(jnp.logical_and(has, sent == count))
                def _():
                    part = total_of(count)
                    remote(part, part, send.at[toward], stat_sem.at[1], right_dev).wait_send()

    def mod_at(j):
        return mod_part.at[j]

    def ctx_at(j):
        return ctx_kv.at[core, pl.ds(pl.multiple_of(j * ctx_rows, 16), ctx_rows)]

    for i in range(2, 6):
        loads[i].wait()

    def norm_context(i, carry):
        part = pl.ds(pl.multiple_of(i * CONTEXT_ROWS, 16), CONTEXT_ROWS)
        scale = row_factor(ctx_v, part)
        for at in range(0, width, 512):
            here = slice(at, at + 512)
            values = ctx_v[part, here].astype(f32)
            ctx_v[part, here] = (values * scale * gain_v[:, here]).astype(bf16)
        return carry

    lax.fori_loop(0, ctx_rows // CONTEXT_ROWS, norm_context, 0)
    own_ctx = pl.ds(pl.multiple_of(s * ctx_rows, 16), ctx_rows)
    ctx_kv[core, own_ctx] = jnp.dot(
        ctx_v[...], proj_w[core, :, qw : qw + 2 * kw], preferred_element_type=f32
    ).astype(bf16)
    line_start(ctx_at, ctxz_send, ctxz_recv)
    for i in range(6, 10):
        loads[i].wait()
    cond = cond_v[...].astype(f32).reshape(1, cond_v.shape[0])
    lifted = jnp.broadcast_to(cond / (1.0 + jnp.exp(-cond)), (16, cond.shape[1])).astype(bf16)
    for i in range(3):
        mod_part[s, :, i * mod_cols : (i + 1) * mod_cols] = jnp.dot(
            lifted, mod_w[i], preferred_element_type=f32
        )[0:1]
    line_start(mod_at, modz_send, modz_recv)
    for copy in pair_copies[1:4]:
        copy.start()

    def wo_line(j, c, toward):
        part = wo.at[far, wo_rows(g, j, c)]
        return remote(
            part, part, wo_send.at[toward], wo_recv.at[j, c], (left_dev, right_dev)[toward]
        )

    def wo_across(j, c):
        part = wo.at[far, wo_rows(g, j, c)]
        return remote(part, part, woy_send, woy_recv.at[j, c], y_dev)

    def wo_pass(j, c):
        part = wo.at[far, wo_rows(g, j, c)]
        remote(part, part, wop_send.at[g], wop_recv.at[g], pair_dev).start()

    def wo_share(j, c):
        part = wo.at[far, wo_rows(1 - g, j, c)]
        remote(part, part, woy_send, woy_recv.at[j, c], y_dev).wait_recv()
        remote(part, part, wop_send.at[1 - g], wop_recv.at[1 - g], pair_dev).start()

    def wo_shares(k):
        def step(c, carry):
            for j, there in ((s - k, s >= k), (s + k, s + k < sp)):

                @pl.when(there)
                def _():
                    wo_share(j, c)

            return carry

        lax.fori_loop(0, WEIGHT_CHUNKS, step, 0)

    def wo_share_own():
        def step(c, carry):
            wo_share(s, c)
            return carry

        lax.fori_loop(0, WEIGHT_CHUNKS, step, 0)

    def wo_own(c):
        wo_line(s, c, 0).wait_recv()
        wo_across(s, c).start()
        wo_pass(s, c)

    def wo_own_line(c):
        for toward, has in ((0, has_left), (1, has_right)):

            @pl.when(has)
            def _():
                wo_line(s, c, toward).start()

    def wo_relay(e):
        k, c = e // WEIGHT_CHUNKS, lax.rem(e, WEIGHT_CHUNKS)
        for toward, has, j, there in (
            (1, has_right, s - k, s >= k),
            (0, has_left, s + k, s + k < sp),
        ):

            @pl.when(there)
            def _():
                wo_line(j, c, toward).wait_recv()

                @pl.when(has)
                def _():
                    wo_line(j, c, toward).start()

                wo_across(j, c).start()
                wo_pass(j, c)

    def wo_relays(low, high):
        def step(e, carry):
            wo_relay(e)
            return carry

        lax.fori_loop(low, high, step, 0)

    quarter = HD // 4
    inverse = jnp.exp(
        lax.rem(lane, quarter).astype(f32) * (-jnp.log(jnp.float32(rope_base)) / quarter)
    )
    first = lax.rem(lane, 2 * quarter) < quarter
    by_row = lax.rem(lane, HD) < HD // 2

    def tables(b, carry):
        place = s * total + jnp.where(b == 0, t, far) * rows + row
        coordinate = jnp.where(by_row, place // GRID_W, lax.rem(place, GRID_W))
        angles = coordinate.astype(f32) * inverse
        turn_cos[b] = jnp.cos(angles)
        sines = jnp.sin(angles)
        turn_sin[b] = jnp.where(first, -sines, sines)
        return carry

    contract = (((1,), (1,)), ((), ()))
    band = 3 * rows
    pairs = kw // HD
    stack = group * rows

    def biases(block, carry):
        q_pos = lax.broadcasted_iota(jnp.int32, (band, rows), 1)
        k_pos = lax.broadcasted_iota(jnp.int32, (band, rows), 0)
        place = s * total + jnp.where(block == 0, t, far) * rows - WIN + k_pos
        allowed = jnp.logical_and(
            jnp.logical_and(k_pos >= q_pos, k_pos <= q_pos + 2 * WIN),
            jnp.logical_and(place >= 0, place < sp * total),
        )
        bias[block] = jnp.where(allowed, 0.0, neg_large)
        return carry

    wo_own(0)
    wo_own_line(0)
    line_relay(1, mod_at, modz_send, modz_recv)
    line_relay(1, ctx_at, ctxz_send, ctxz_recv)
    wo_own(1)
    lax.fori_loop(0, 2, tables, 0)
    lax.fori_loop(0, 2, biases, 0)
    line_relay(2, mod_at, modz_send, modz_recv)
    for j in range(2, AHEAD):
        lat_copy(j).start()
    wo_own_line(1)
    for c in range(2, WEIGHT_CHUNKS):
        wo_own(c)
        wo_own_line(c)
    wo_relays(WEIGHT_CHUNKS, WEIGHT_CHUNKS + 1)
    pair_copies[4].start()
    line_relay(2, ctx_at, ctxz_send, ctxz_recv)
    for k in range(3, sp):
        line_relay(k, mod_at, modz_send, modz_recv)
    summed = mod_part[0]
    for k in range(1, sp):
        summed = summed + mod_part[k]
    mod_all[t] = summed
    for k in range(1, tp):
        remote(
            mod_all.at[t], mod_all.at[t], modt_send, modt_recv, {"tp": lax.rem(t + k, tp)}
        ).start()
    mods = remote(
        mod_all.at[0 : tp - 1], mod_all.at[0 : tp - 1], modt_send, modt_recv, pair_dev
    )
    for j in range(AHEAD, LATENT_CHUNKS):
        lat_copy(j).start()
    wo_relays(WEIGHT_CHUNKS + 1, WEIGHT_CHUNKS + 3)
    stat_copy.wait_recv()
    column = jnp.sum(
        jnp.where(diagonal, jnp.broadcast_to(stat_in[0:1], (rows, 128)), 0.0), axis=1, keepdims=True
    )
    row_scale[1] = jnp.broadcast_to(column, (rows, 128))

    mods.wait_recv()
    for i in range(tp):
        cols = slice(i * mod_cols, (i + 1) * mod_cols)
        shift_v[:, cols] = mod_all[i, :, 0:mod_cols]
        factor_v[:, cols] = gain_v[:, cols] * (1.0 + mod_all[i, :, mod_cols : 2 * mod_cols])
        gate_v[:, cols] = mod_all[i, :, 2 * mod_cols : 3 * mod_cols]

    def normalize(block, source, cols, lanes, target):
        scale = row_scale[block]
        for at in range(0, lanes, 128):
            here = pl.ds(pl.multiple_of(cols + at, 128), 128)
            values = source[:, here].astype(f32) * scale
            target[:, at : at + 128] = (values * factor_v[:, here] + shift_v[:, here]).astype(bf16)

    def project(j):
        normalize(1, lat_far, j * chunk, chunk, normed)
        cols = pl.ds(pl.multiple_of(j * chunk, 128), chunk)
        for slot in range(2):
            acc[slot] += jnp.dot(
                normed[:, 0:chunk], proj_w[slot, cols], preferred_element_type=f32
            )

    low = lane < HD

    def finish_projection(block, position):
        cosine, sine = turn_cos[block], turn_sin[block]

        def turned(values):
            swapped = jnp.where(
                first, pltpu.roll(values, 128 - quarter, 1), pltpu.roll(values, quarter, 1)
            )
            return values * cosine + swapped * sine

        factor = HD ** (-0.5)
        base = pl.ds(pl.multiple_of(position * rows, rows), rows)
        for slot in range(2):
            key_value[slot, base, 0:kw] = turned(acc[slot, :, qw : qw + kw]).astype(bf16)
            key_value[slot, base, kw : 2 * kw] = acc[slot, :, qw + kw : qw + 2 * kw].astype(bf16)
            for u in range(heads // 2):
                lanes = turned(acc[slot, :, u * 128 : (u + 1) * 128]).astype(bf16)
                swapped = pltpu.roll(lanes.astype(f32), HD, 1) * factor
                lanes = lanes.astype(f32) * factor
                keep = low if u == 0 else jnp.logical_not(low)
                for at in range(2):
                    aligned = lanes if at == u else swapped
                    queries[block, slot, u, at * rows : (at + 1) * rows] = jnp.where(
                        keep, aligned, 0.0
                    ).astype(bf16)

    def kv_at(position):
        return key_value.at[:, pl.ds(pl.multiple_of(position * rows, rows), rows)]

    def kv_pair(block, position):
        return remote(
            kv_at(position), kv_at(position), kv_send, kv_recv.at[block], pair_dev
        )

    halo_down = remote(
        kv_at(1), kv_at(tp + 1), halo_sem.at[0], halo_sem.at[1], {**left_dev, "tp": pair}
    )
    halo_up = remote(kv_at(tp), kv_at(0), halo_sem.at[0], halo_sem.at[1], {**right_dev, "tp": pair})
    sends_down = jnp.logical_and(core == 0, has_left)
    sends_up = jnp.logical_and(core == 1, has_right)

    def send_halo(mine):
        @pl.when(jnp.logical_and(mine, sends_down))
        def _():
            halo_down.start()

        @pl.when(jnp.logical_and(mine, sends_up))
        def _():
            halo_up.start()

    def wait_halo(mine):
        @pl.when(jnp.logical_and(mine, sends_down))
        def _():
            halo_up.wait_recv()

        @pl.when(jnp.logical_and(mine, sends_up))
        def _():
            halo_down.wait_recv()

    def context_part(block, slot):
        units = range(pairs)
        scores = [
            lax.dot_general(
                ctx_kv[slot, :, 0:kw],
                queries[block, slot, u],
                contract,
                preferred_element_type=f32,
            )
            for u in units
        ]
        sinks = [
            jnp.concatenate(
                [sink_v[slot, u * group + h : u * group + h + 1] for h in range(group)], axis=1
            )
            for u in units
        ]
        tops = [
            jnp.maximum(jnp.max(scores[u], axis=0, keepdims=True), sinks[u]) for u in units
        ]
        exps = [jnp.exp(scores[u] - tops[u]) for u in units]
        for u in units:
            part_top[block, slot, u] = tops[u]
            part_sum[block, slot, u] = jnp.sum(exps[u], axis=0, keepdims=True) + jnp.exp(
                sinks[u] - tops[u]
            )
            part_out[block, slot, u] = jnp.dot(
                ctx_vt[slot, u * HD : (u + 1) * HD],
                exps[u].astype(bf16),
                preferred_element_type=f32,
            )

    def window_part(block, position, slot, skip, blocks):
        units = range(pairs)
        here = pl.ds(pl.multiple_of(skip * rows, rows), blocks * rows)
        window = pl.ds(pl.multiple_of((position - 1 + skip) * rows, rows), blocks * rows)
        mask = jnp.concatenate([bias[block, here]] * group, axis=1)
        scores = [
            lax.dot_general(
                key_value[slot, window, 0:kw],
                queries[block, slot, u],
                contract,
                preferred_element_type=f32,
            )
            + mask
            for u in units
        ]
        befores = [part_top[block, slot, u] for u in units]
        tops = [
            jnp.maximum(jnp.max(scores[u], axis=0, keepdims=True), befores[u]) for u in units
        ]
        exps = [jnp.exp(scores[u] - tops[u]) for u in units]
        keeps = [jnp.exp(befores[u] - tops[u]) for u in units]
        values = jnp.transpose(key_value[slot, window, kw : 2 * kw])
        bottoms = [
            jnp.sum(exps[u], axis=0, keepdims=True) + part_sum[block, slot, u] * keeps[u]
            for u in units
        ]
        results = [
            jnp.dot(
                values[u * HD : (u + 1) * HD], exps[u].astype(bf16), preferred_element_type=f32
            )
            + part_out[block, slot, u] * keeps[u]
            for u in units
        ]
        return tops, bottoms, results

    def window_early(block, position, slot, skip, blocks):
        tops, bottoms, results = window_part(block, position, slot, skip, blocks)
        for u in range(pairs):
            part_top[block, slot, u] = tops[u]
            part_sum[block, slot, u] = bottoms[u]
            part_out[block, slot, u] = results[u]

    def window_last(block, position, slot, skip, blocks, target):
        _, bottoms, results = window_part(block, position, slot, skip, blocks)
        for u in range(pairs):
            result = results[u] / bottoms[u]
            turned_back = jnp.concatenate(
                [result[:, h * rows : (h + 1) * rows] for h in range(group)], axis=0
            )
            target[slot, :, u * 128 : (u + 1) * 128] = jnp.transpose(turned_back).astype(bf16)

    edge = jnp.zeros((2, rows, 2 * kw), bf16)

    @pl.when(jnp.logical_and(core == 0, jnp.logical_not(has_left)))
    def _():
        key_value[:, 0:rows] = edge

    @pl.when(jnp.logical_and(core == 1, jnp.logical_not(has_right)))
    def _():
        key_value[:, (tp + 1) * rows : (tp + 2) * rows] = edge

    for i in range(10, 12):
        loads[i].wait()
    for copy in pair_copies[0:4]:
        copy.wait_recv()

    def far_step(j, carry):
        lat_copy(j).wait_recv()
        project(j)
        return carry

    normalize(0, lat_own, 0, width, normed)
    for slot in range(2):
        acc[slot] = jnp.dot(normed[...], proj_w[slot], preferred_element_type=f32)
    finish_projection(0, t + 1)
    kv_pair(0, t + 1).start()
    send_halo(chip == core)
    def wo_pair(gg):
        part = wo.at[far, pl.ds(pl.multiple_of(gg * sp * shard, 16), sp * shard)]
        return remote(part, part, wop_send.at[gg], wop_recv.at[gg], pair_dev)


    def wo_last(c):
        for k in range(3, sp):
            wo_relays(k * WEIGHT_CHUNKS + c, k * WEIGHT_CHUNKS + c + 1)

    wo_relays(WEIGHT_CHUNKS + 3, 2 * WEIGHT_CHUNKS + 1)
    for slot in range(2):
        acc[slot] = jnp.zeros(acc.shape[1:], f32)
    lax.fori_loop(0, 3, far_step, 0)
    for k in range(3, sp):
        line_relay(k, ctx_at, ctxz_send, ctxz_recv)
    ctx_pair = remote(ctx_kv.at[core], ctx_kv.at[core], ctxp_sem.at[0], ctxp_sem.at[1], pair_dev)
    ctx_pair.start()
    wo_relays(2 * WEIGHT_CHUNKS + 1, 2 * WEIGHT_CHUNKS + 2)
    lax.fori_loop(3, 5, far_step, 0)
    wo_relays(2 * WEIGHT_CHUNKS + 2, 2 * WEIGHT_CHUNKS + 3)
    ctx_pair.wait_recv()
    for slot in range(2):
        ctx_vt[slot] = jnp.transpose(ctx_kv[slot, :, kw : 2 * kw])
    context_part(0, 0)
    kv_pair(0, pair + 1).wait_recv()
    window_early(0, t + 1, 0, 1 - core, 2)
    wo_relays(2 * WEIGHT_CHUNKS + 3, 3 * WEIGHT_CHUNKS)
    context_part(0, 1)
    window_early(0, t + 1, 1, 1 - core, 2)
    wo_last(0)
    wo_share_own()
    wo_shares(1)
    lax.fori_loop(5, 6, far_step, 0)
    wo_last(1)
    lax.fori_loop(6, 7, far_step, 0)
    wo_last(2)
    lax.fori_loop(7, LATENT_CHUNKS, far_step, 0)
    for c in range(3, WEIGHT_CHUNKS):
        wo_last(c)
    finish_projection(1, far + 1)
    kv_pair(1, far + 1).start()
    send_halo(chip != core)

    context_part(1, 0)

    def att_copy(slot):
        return remote(
            att_out.at[slot], att.at[chip, slot], att_send, att_recv.at[slot], far_dev
        )

    kv_pair(1, pair + 1).wait_recv()
    wait_halo(chip != core)
    window_last(1, far + 1, 0, 0, 3, att_out)
    att_copy(0).start()
    context_part(1, 1)
    window_last(1, far + 1, 1, 0, 3, att_out)
    att_copy(1).start()
    wo_shares(2)
    wait_halo(chip == core)
    for slot in range(2):
        window_last(0, t + 1, slot, 2 * core, 1, att.at[chip])
    for k in range(3, sp):
        wo_shares(k)
    pair_copies[4].wait_recv()

    def out_product(x, i):
        sums = None
        for slot in range(2):
            part = pl.ds(pl.multiple_of((2 * x + slot) * qw, qw), qw)
            product = jnp.dot(att[x, slot], wo[i, part], preferred_element_type=f32)
            sums = product if sums is None else sums + product
        return sums

    order = (t, pair, far, (1 - chip) * 2 + 1 - core)
    other = (1 - chip) * 2 + 1 - core
    for k, i in enumerate(order):
        if k == 3:
            for gg in range(2):
                part = wo.at[other, pl.ds(gg * sp * shard, sp * shard)]
                remote(part, part, wop_send.at[gg], wop_recv.at[gg], pair_dev).wait_recv()
        out_part[k] = out_product(chip, i)
    att_copy(0).wait_recv()
    first_rows = pl.ds(pl.multiple_of(2 * (1 - chip) * qw, qw), qw)
    last_rows = pl.ds(pl.multiple_of((2 * (1 - chip) + 1) * qw, qw), qw)
    for k, i in enumerate(order):
        out_part[k] += jnp.dot(
            att[1 - chip, 0], wo[i, first_rows], preferred_element_type=f32
        )
    att_copy(1).wait_recv()
    for k, i in enumerate(order):
        cols = pl.ds(pl.multiple_of(i * out_width, 128), out_width)
        product = jnp.dot(att[1 - chip, 1], wo[i, last_rows], preferred_element_type=f32)
        blended = (out_part[k] + product).astype(bf16).astype(f32)
        mixed[:, cols] = (lat_own[:, cols].astype(f32) + gate_v[:, cols] * blended).astype(bf16)

    stat_copy.wait_send()
    remote(wo_shard, wo_shard, wox_send, wo_recv.at[0, 0], far_dev).wait_send()
    remote(lat_own, lat_far, lat_send, lat_recv.at[0], far_dev).wait_send()
    for copy in pair_copies:
        copy.wait_send()
    mods.wait_send()
    line_finish(lambda count: mod_part.at[0:count], modz_send)
    line_finish(lambda count: ctx_kv.at[core, 0 : count * ctx_rows], ctxz_send)
    ctx_pair.wait_send()
    def wo_total(count):
        return wo.at[far, 0 : count * shard]

    line_finish(wo_total, wo_send)
    wo_sent = wo.at[far, pl.ds(pl.multiple_of(g * sp * shard, 16), sp * shard)]
    remote(wo_sent, wo_sent, woy_send, woy_recv.at[0, 0], y_dev).wait_send()
    wo_pair(0).wait_send()
    wo_pair(1).wait_send()
    both = key_value.at[:, 0 : 2 * rows]
    remote(both, both, kv_send, kv_recv.at[0], pair_dev).wait_send()

    @pl.when(sends_down)
    def _():
        halo_down.wait_send()

    @pl.when(sends_up)
    def _():
        halo_up.wait_send()

    remote(att_out, att_out, att_send, att_recv.at[0], far_dev).wait_send()


def local(
    latent,
    context,
    conditioning,
    norm_gain,
    shift_weight,
    scale_weight,
    gate_weight,
    query_weight,
    key_weight,
    value_weight,
    out_weight,
    sink_logit,
):
    tp, sp, grp = lax.axis_size("tp"), lax.axis_size("sp"), lax.axis_size("grp")
    rows, width = latent.shape
    ctx_rows = context.shape[0]
    mod_rows, mod_cols = shift_weight.shape
    query_width, key_width = query_weight.shape[1], key_weight.shape[1]
    out_rows, out_width = out_weight.shape
    fits = (
        rows == WIN
        and rows == 128
        and key_width == 2 * HD
        and query_width == 4 * HD
        and tp == 4
        and grp == 2
        and sp >= 3
        and sp * ctx_rows % 128 == 0
        and ctx_rows % CONTEXT_ROWS == 0
        and width % 512 == 0
        and mod_cols % 128 == 0
        and width % (128 * LATENT_CHUNKS) == 0
        and out_width % 128 == 0
        and tp * out_width == width
        and out_rows == tp * query_width
        and out_rows % (2 * sp * WEIGHT_CHUNKS * 16) == 0
    )
    if not fits:
        return local_plain(
            latent,
            context,
            conditioning,
            norm_gain,
            shift_weight,
            scale_weight,
            gate_weight,
            query_weight,
            key_weight,
            value_weight,
            out_weight,
            sink_logit,
        )
    f32, bf16 = jnp.float32, jnp.bfloat16
    dma = pltpu.SemaphoreType.DMA
    anywhere = pl.BlockSpec(memory_space=pl.ANY)
    return pl.pallas_call(
        functools.partial(fused_kernel, sp),
        out_shape=pltpu.VMEM((rows, width), bf16),
        in_specs=[anywhere] * 11 + [pl.BlockSpec(memory_space=pltpu.SMEM)],
        out_specs=pl.BlockSpec(memory_space=pltpu.VMEM),
        scratch_shapes=[
            pltpu.VMEM((mod_rows,), bf16),
            pltpu.VMEM((1, width), f32),
            pltpu.VMEM((3, mod_rows, mod_cols), bf16),
            pltpu.VMEM((2, width, query_width + 2 * key_width), bf16),
            pltpu.VMEM((tp, out_rows, out_width), bf16),
            pltpu.VMEM((out_rows // (2 * sp), out_width), bf16),
            pltpu.VMEM(context.shape, bf16),
            pltpu.VMEM((rows, width), bf16),
            pltpu.VMEM((rows, width), bf16),
            pltpu.VMEM((rows, width), bf16),
            pltpu.VMEM((8, 128), f32),
            pltpu.VMEM((8, 128), f32),
            pltpu.VMEM((2, rows, 128), f32),
            pltpu.VMEM((2, 8, 128), f32),
            pltpu.VMEM((sp, 1, 3 * mod_cols), f32),
            pltpu.VMEM((tp, 1, 3 * mod_cols), f32),
            pltpu.VMEM((1, width), f32),
            pltpu.VMEM((1, width), f32),
            pltpu.VMEM((1, width), f32),
            pltpu.VMEM((2, rows, 128), f32),
            pltpu.VMEM((2, rows, 128), f32),
            pltpu.VMEM((2, rows, query_width + 2 * key_width), f32),
            pltpu.VMEM((2, 2, 2, 2 * rows, key_width), bf16),
            pltpu.VMEM((2, (tp + 2) * rows, 2 * key_width), bf16),
            pltpu.VMEM((2, sp * ctx_rows, 2 * key_width), bf16),
            pltpu.VMEM((2, 2, rows, query_width), bf16),
            pltpu.VMEM((2, rows, query_width), bf16),
            pltpu.VMEM((2, key_width, sp * ctx_rows), bf16),
            pltpu.VMEM((2, 3 * rows, rows), f32),
            pltpu.VMEM((2, 2, 2, HD, 2 * rows), f32),
            pltpu.VMEM((2, 2, 2, 1, 2 * rows), f32),
            pltpu.VMEM((2, 2, 2, 1, 2 * rows), f32),
            pltpu.VMEM((tp, rows, out_width), f32),
            dma((12,)),
            dma,
            dma((LATENT_CHUNKS,)),
            dma((2,)),
            dma((5,)),
            dma((5,)),
            dma,
            dma((2,)),
            dma((sp, WEIGHT_CHUNKS)),
            dma,
            dma((sp, WEIGHT_CHUNKS)),
            dma((2,)),
            dma((2,)),
            dma((2,)),
            dma((sp,)),
            dma,
            dma,
            dma((2,)),
            dma((sp,)),
            dma((2,)),
            dma,
            dma((2,)),
            dma((2,)),
            dma,
            dma((2,)),
        ],
        compiler_params=pltpu.CompilerParams(
            collective_id=0, has_side_effects=True, vmem_limit_bytes=60 * 1024 * 1024
        ),
        name="fused",
    )(
        latent,
        context,
        conditioning,
        norm_gain.reshape(1, width),
        shift_weight,
        scale_weight,
        gate_weight,
        query_weight,
        key_weight,
        value_weight,
        out_weight,
        sink_logit,
    )


def solution(mesh):
    in_specs = (
        P(("grp", "sp", "tp"), None),
        P(("grp", "sp"), None),
        P(("grp", "sp")),
        P(),
        P("sp", "tp"),
        P("sp", "tp"),
        P("sp", "tp"),
        P(None, "tp"),
        P(None, "tp"),
        P(None, "tp"),
        P(None, "tp"),
        P("tp"),
    )
    out_specs = P(("grp", "sp", "tp"), None)
    return jax.shard_map(local, mesh=mesh, in_specs=in_specs, out_specs=out_specs, check_vma=False)
```

```python
import functools

import jax
import jax.numpy as jnp
from jax import lax
from jax.experimental import pallas as pl
from jax.experimental.pallas import tpu as pltpu
from jax.sharding import PartitionSpec as P

HEADS = 16
KV_HEADS = 8
HD = 64
GRID_W = 64
WIN = 128


epsilon = 1e-06
rope_base = 10000.0
neg_large = -1e30


def with_halo(cells, sides, width):
    for axis, dim in sides:
        count = lax.axis_size(axis)
        ends = count - 1
        head = lax.slice_in_dim(cells, 0, width, axis=dim)
        tail = lax.slice_in_dim(cells, cells.shape[dim] - width, cells.shape[dim], axis=dim)
        cells = jnp.concatenate(
            [
                lax.ppermute(tail, axis, [(i, (i + 1) % count) for i in range(ends)]),
                cells,
                lax.ppermute(head, axis, [((i + 1) % count, i) for i in range(ends)]),
            ],
            axis=dim,
        )
    return cells


def row_norm(matrix, norm_gain):
    values = matrix.astype(jnp.float32)
    return (
        values * lax.rsqrt(jnp.mean(values * values, axis=-1, keepdims=True) + epsilon) * norm_gain
    )


def axial_turn(values, position):
    half_dim = values.shape[-1] // 2
    quarter = half_dim // 2
    inverse = rope_base ** (-jnp.arange(quarter, dtype=jnp.float32) / quarter)

    def turn(section, coordinate):
        angles = coordinate.astype(jnp.float32)[:, None] * inverse[None, :]
        cosine = jnp.cos(angles)[:, None, :]
        sine_part = jnp.sin(angles)[:, None, :]
        leading = section[..., :quarter]
        trailing = section[..., quarter:]
        return jnp.concatenate(
            [leading * cosine - trailing * sine_part, leading * sine_part + trailing * cosine],
            axis=-1,
        )

    return jnp.concatenate(
        [
            turn(values[..., :half_dim], position // GRID_W),
            turn(values[..., half_dim:], position % GRID_W),
        ],
        axis=-1,
    )


def context_pairs(context_rows, norm_gain, key_weight, value_weight):
    prepared = row_norm(context_rows, norm_gain).astype(jnp.bfloat16)
    return jnp.concatenate(
        [
            jnp.dot(prepared, key_weight, preferred_element_type=jnp.float32),
            jnp.dot(prepared, value_weight, preferred_element_type=jnp.float32),
        ],
        axis=1,
    ).astype(jnp.bfloat16)


def local_plain(
    latent,
    context,
    conditioning,
    norm_gain,
    shift_weight,
    scale_weight,
    gate_weight,
    query_weight,
    key_weight,
    value_weight,
    out_weight,
    sink_logit,
):
    lifted = jax.nn.silu(conditioning.astype(jnp.float32)).astype(jnp.bfloat16)[None, :]
    shift_part = jnp.dot(lifted, shift_weight, preferred_element_type=jnp.float32)[0]
    scale_part = jnp.dot(lifted, scale_weight, preferred_element_type=jnp.float32)[0]
    gate_part = jnp.dot(lifted, gate_weight, preferred_element_type=jnp.float32)[0]
    summed = lax.psum((shift_part, scale_part, gate_part), "sp")
    shift_vec, scale_vec, gate_vec = (
        lax.all_gather(summed[0], "tp", axis=0, tiled=True),
        lax.all_gather(summed[1], "tp", axis=0, tiled=True),
        lax.all_gather(summed[2], "tp", axis=0, tiled=True),
    )
    normed = (row_norm(latent, norm_gain) * (1.0 + scale_vec) + shift_vec).astype(jnp.bfloat16)
    segment = lax.all_gather(normed, "tp", axis=0, tiled=True)
    projected = jnp.concatenate(
        [
            jnp.dot(segment, query_weight, preferred_element_type=jnp.float32),
            jnp.dot(segment, key_weight, preferred_element_type=jnp.float32),
            jnp.dot(segment, value_weight, preferred_element_type=jnp.float32),
        ],
        axis=1,
    )
    row_count = projected.shape[0]
    query_width = query_weight.shape[1]
    key_width = key_weight.shape[1]
    query_heads = query_width // HD
    pair_heads = key_width // HD
    group_size = HEADS // KV_HEADS
    row_offset = lax.axis_index("sp") * row_count
    position = row_offset + jnp.arange(row_count, dtype=jnp.int32)
    queries = axial_turn(
        projected[:, :query_width].reshape(row_count, query_heads, HD), position
    ).astype(jnp.bfloat16)
    latent_keys = axial_turn(
        projected[:, query_width : query_width + key_width].reshape(row_count, pair_heads, HD),
        position,
    ).astype(jnp.bfloat16)
    latent_values = projected[:, query_width + key_width :].astype(jnp.bfloat16)
    key_value = jnp.concatenate([latent_keys.reshape(row_count, key_width), latent_values], axis=1)
    widened = with_halo(key_value, (("sp", 0),), WIN)
    context_all = lax.all_gather(
        context_pairs(context, norm_gain, key_weight, value_weight), "sp", axis=0, tiled=True
    )
    block_count = row_count // WIN
    context_count = context_all.shape[0]
    query_blocks = queries.reshape(block_count, WIN, pair_heads, group_size, HD)
    band_blocks = widened.reshape(block_count + 2, WIN, 2 * key_width)
    band_rows = jnp.concatenate(
        [band_blocks[:block_count], band_blocks[1 : block_count + 1], band_blocks[2:]], axis=1
    )
    band_keys = band_rows[..., :key_width].reshape(block_count, 3 * WIN, pair_heads, HD)
    band_values = band_rows[..., key_width:].reshape(block_count, 3 * WIN, pair_heads, HD)
    context_keys = context_all[:, :key_width].reshape(context_count, pair_heads, HD)
    context_values = context_all[:, key_width:].reshape(context_count, pair_heads, HD)
    factor = HD ** (-0.5)
    local_scores = (
        jnp.einsum("nqhgd,nkhd->nhgqk", query_blocks, band_keys, preferred_element_type=jnp.float32)
        * factor
    )
    query_pos = position.reshape(block_count, WIN)
    key_pos = (
        row_offset
        - WIN
        + jnp.arange(block_count, dtype=jnp.int32)[:, None] * WIN
        + jnp.arange(3 * WIN, dtype=jnp.int32)[None, :]
    )
    seq_total = row_count * lax.axis_size("sp")
    allowed = (
        (jnp.abs(key_pos[:, None, :] - query_pos[:, :, None]) <= WIN)
        & (key_pos[:, None, :] >= 0)
        & (key_pos[:, None, :] < seq_total)
    )
    local_scores = jnp.where(allowed[:, None, None], local_scores, neg_large)
    context_scores = (
        jnp.einsum(
            "nqhgd,thd->nhgqt", query_blocks, context_keys, preferred_element_type=jnp.float32
        )
        * factor
    )
    sink_values = sink_logit.reshape(pair_heads, group_size)[None, :, :, None, None]
    highest = jnp.maximum(
        jnp.maximum(
            jnp.max(local_scores, axis=-1, keepdims=True),
            jnp.max(context_scores, axis=-1, keepdims=True),
        ),
        sink_values,
    )
    local_exp = jnp.exp(local_scores - highest)
    context_exp = jnp.exp(context_scores - highest)
    denominator = (
        jnp.sum(local_exp, axis=-1, keepdims=True)
        + jnp.sum(context_exp, axis=-1, keepdims=True)
        + jnp.exp(sink_values - highest)
    )
    local_weights = (local_exp / denominator).astype(jnp.bfloat16)
    context_weights = (context_exp / denominator).astype(jnp.bfloat16)
    attended = jnp.einsum(
        "nhgqk,nkhd->nqhgd", local_weights, band_values, preferred_element_type=jnp.float32
    ) + jnp.einsum(
        "nhgqt,thd->nqhgd", context_weights, context_values, preferred_element_type=jnp.float32
    )
    attended = attended.reshape(row_count, query_width).astype(jnp.bfloat16)
    columns_part = jnp.dot(
        lax.all_gather(attended, "tp", axis=1, tiled=True),
        out_weight,
        preferred_element_type=jnp.float32,
    ).astype(jnp.bfloat16)
    blended = lax.all_to_all(columns_part, "tp", split_axis=0, concat_axis=1, tiled=True)
    return (latent.astype(jnp.float32) + gate_vec * blended.astype(jnp.float32)).astype(
        jnp.bfloat16
    )


LATENT_CHUNKS = 16
WEIGHT_CHUNKS = 4
HELD = 2
AHEAD = 3 * LATENT_CHUNKS // 8
NORM_ROWS = 16
CONTEXT_ROWS = 32


def remote(src, dst, send, recv, device):
    return pltpu.make_async_remote_copy(
        src_ref=src,
        dst_ref=dst,
        send_sem=send,
        recv_sem=recv,
        device_id=device,
        device_id_type=pl.DeviceIdType.MESH,
    )


def fused_kernel(
    sp,
    latent,
    context,
    conditioning,
    norm_gain,
    shift_weight,
    scale_weight,
    gate_weight,
    query_weight,
    key_weight,
    value_weight,
    out_weight,
    sink,
    mixed,
    cond_v,
    gain_v,
    mod_w,
    proj_w,
    wo,
    wo_shard,
    ctx_v,
    lat_own,
    lat_far,
    normed,
    stat_out,
    stat_in,
    row_scale,
    sink_v,
    mod_part,
    mod_all,
    factor_v,
    shift_v,
    gate_v,
    turn_cos,
    turn_sin,
    acc,
    queries,
    key_value,
    ctx_kv,
    att,
    att_out,
    ctx_vt,
    bias,
    part_out,
    part_top,
    part_sum,
    out_part,
    load_sem,
    lat_send,
    lat_recv,
    stat_sem,
    pair_send,
    pair_recv,
    wox_send,
    wo_send,
    wo_recv,
    woy_send,
    woy_recv,
    wop_send,
    wop_recv,
    modz_send,
    modz_recv,
    modt_send,
    modt_recv,
    ctxz_send,
    ctxz_recv,
    ctxp_sem,
    kv_send,
    kv_recv,
    halo_sem,
    att_send,
    att_recv,
):
    g = lax.axis_index("grp")
    s = lax.axis_index("sp")
    t = lax.axis_index("tp")
    chip = t // 2
    core = lax.rem(t, 2)
    pair = chip * 2 + 1 - core
    far = (1 - chip) * 2 + core
    pair_dev, far_dev, y_dev = {"tp": pair}, {"tp": far}, {"grp": 1 - g}
    right_dev = {"sp": lax.rem(s + 1, sp)}
    left_dev = {"sp": lax.rem(s + sp - 1, sp)}
    has_right, has_left = s < sp - 1, s > 0
    rows, width = latent.shape
    ctx_rows = context.shape[0]
    mod_cols = shift_weight.shape[1]
    qw = query_weight.shape[1]
    kw = key_weight.shape[1]
    heads = qw // HD
    group = heads // (kw // HD)
    tp = 4
    total = tp * rows
    out_rows, out_width = out_weight.shape
    half = rows // 2
    f32, bf16 = jnp.float32, jnp.bfloat16
    chunk = width // LATENT_CHUNKS
    shard = out_rows // (2 * sp)
    slab = shard // WEIGHT_CHUNKS
    MESH = pl.DeviceIdType.MESH

    loads = [
        (out_weight.at[pl.ds(pl.multiple_of((g * sp + s) * shard, 16), shard)], wo_shard),
        (latent, lat_own),
        (norm_gain, gain_v),
        (context, ctx_v),
        (key_weight, proj_w.at[core, :, qw : qw + kw]),
        (value_weight, proj_w.at[core, :, qw + kw : qw + 2 * kw]),
        (conditioning, cond_v),
        (shift_weight, mod_w.at[0]),
        (scale_weight, mod_w.at[1]),
        (gate_weight, mod_w.at[2]),
        (query_weight, proj_w.at[core, :, 0:qw]),
        (out_weight, wo.at[t]),
    ]
    slots = (0, 1, 2, 3, 4, 4, 5, 6, 6, 6, 7, 8)
    loads = [
        pltpu.make_async_copy(a, b, load_sem.at[i]) for i, (a, b) in zip(slots, loads, strict=True)
    ]
    for load in loads:
        load.start()

    barrier = pltpu.get_barrier_semaphore()
    for k in range(1, tp):
        pl.semaphore_signal(
            barrier, inc=1, device_id={"tp": lax.rem(t + k, tp)}, device_id_type=MESH
        )
    pl.semaphore_signal(barrier, inc=1, device_id=y_dev, device_id_type=MESH)
    for has, place in ((has_right, right_dev), (has_left, left_dev)):

        @pl.when(has)
        def _():
            for peer in (t, pair):
                pl.semaphore_signal(
                    barrier, inc=1, device_id={**place, "tp": peer}, device_id_type=MESH
                )

    def row_factor(source, part):
        squares = None
        for at in range(0, width, 512):
            values = source[part, at : at + 512].astype(f32)
            values = values * values
            squares = values if squares is None else squares + values
        return lax.rsqrt(jnp.sum(squares, axis=-1, keepdims=True) * (1.0 / width) + epsilon)

    lane = lax.broadcasted_iota(jnp.int32, (rows, 128), 1)
    row = lax.broadcasted_iota(jnp.int32, (rows, 128), 0)
    diagonal = lane == row

    pl.semaphore_wait(
        barrier, tp + jnp.where(has_right, 2, 0) + jnp.where(has_left, 2, 0)
    )

    def lat_copy(j):
        cols = pl.ds(pl.multiple_of(j * chunk, 128), chunk)
        return remote(
            lat_own.at[:, cols], lat_far.at[:, cols], lat_send, lat_recv.at[j], far_dev
        )

    def wo_rows(gg, j, c):
        return pl.ds(pl.multiple_of((gg * sp + j) * shard + c * slab, 16), slab)

    def wo_cross(c):
        part = wo_rows(g, s, c)
        return remote(
            wo_shard.at[pl.ds(c * slab, slab)],
            wo.at[t, part],
            wox_send,
            wo_recv.at[s, c],
            far_dev,
        )

    loads[0].wait()
    for c in range(WEIGHT_CHUNKS):
        wo_cross(c).start()
    loads[1].wait()

    def row_stat(i, carry):
        part = pl.ds(pl.multiple_of(i * CONTEXT_ROWS, 16), CONTEXT_ROWS)
        row_scale[0, part] = jnp.broadcast_to(row_factor(lat_own, part), (CONTEXT_ROWS, 128))
        return carry

    lax.fori_loop(0, rows // CONTEXT_ROWS, row_stat, 0)
    flat = jnp.sum(jnp.where(diagonal, row_scale[0], 0.0), axis=0, keepdims=True)
    stat_out[...] = jnp.broadcast_to(flat, (8, 128))
    sink_row = lax.broadcasted_iota(jnp.int32, (8, 128), 0)
    sink_all = jnp.full((8, 128), sink[0], f32)
    for h in range(1, heads):
        sink_all = jnp.where(sink_row == h, sink[h], sink_all)
    sink_v[core] = sink_all

    stat_copy = remote(stat_out, stat_in, stat_sem.at[0], stat_sem.at[1], far_dev)
    stat_copy.start()
    for j in range(LATENT_CHUNKS // 4):
        lat_copy(j).start()
    pair_copies = [
        (sink_v.at[core], sink_v.at[core]),
        (query_weight, proj_w.at[core, :, 0:qw]),
        (key_weight, proj_w.at[core, :, qw : qw + kw]),
        (value_weight, proj_w.at[core, :, qw + kw : qw + 2 * kw]),
        (out_weight, wo.at[t]),
    ]
    pair_copies = [
        remote(a, b, pair_send.at[i], pair_recv.at[i], pair_dev)
        for i, (a, b) in zip((0, 1, 1, 1, 2), pair_copies, strict=True)
    ]
    pair_copies[0].start()

    def line_copy(at, j, send, recv, toward):
        return remote(at(j), at(j), send.at[toward], recv.at[j], (left_dev, right_dev)[toward])

    def line_start(at, send, recv):
        for toward, has in ((0, has_left), (1, has_right)):

            @pl.when(has)
            def _():
                line_copy(at, s, send, recv, toward).start()

    def line_relay(k, at, send, recv):
        for toward, has, j, there in (
            (1, has_right, s - k, s >= k),
            (0, has_left, s + k, s + k < sp),
        ):

            @pl.when(there)
            def _():
                line_copy(at, j, send, recv, toward).wait_recv()

                @pl.when(has)
                def _():
                    line_copy(at, j, send, recv, toward).start()

    def line_finish(total_of, send):
        for toward, has, sent in ((1, has_right, s + 1), (0, has_left, sp - s)):
            for count in range(1, sp + 1):

                @pl.when(jnp.logical_and(has, sent == count))
                def _():
                    part = total_of(count)
                    remote(part, part, send.at[toward], stat_sem.at[1], right_dev).wait_send()

    def mod_at(j):
        return mod_part.at[j]

    def ctx_at(j):
        return ctx_kv.at[core, pl.ds(pl.multiple_of(j * ctx_rows, 16), ctx_rows)]

    loads[2].wait()
    loads[3].wait()
    kv_weights = proj_w.at[core, :, qw : qw + 2 * kw]
    pltpu.make_async_copy(kv_weights, kv_weights, load_sem.at[4]).wait()

    def norm_context(i, carry):
        part = pl.ds(pl.multiple_of(i * CONTEXT_ROWS, 16), CONTEXT_ROWS)
        scale = row_factor(ctx_v, part)
        for at in range(0, width, 512):
            here = slice(at, at + 512)
            values = ctx_v[part, here].astype(f32)
            ctx_v[part, here] = (values * scale * gain_v[:, here]).astype(bf16)
        return carry

    lax.fori_loop(0, ctx_rows // CONTEXT_ROWS, norm_context, 0)
    own_ctx = pl.ds(pl.multiple_of(s * ctx_rows, 16), ctx_rows)
    ctx_kv[core, own_ctx] = jnp.dot(
        ctx_v[...], proj_w[core, :, qw : qw + 2 * kw], preferred_element_type=f32
    ).astype(bf16)
    line_start(ctx_at, ctxz_send, ctxz_recv)
    loads[6].wait()
    pltpu.make_async_copy(mod_w, mod_w, load_sem.at[6]).wait()
    cond = cond_v[...].astype(f32).reshape(1, cond_v.shape[0])
    lifted = jnp.broadcast_to(cond / (1.0 + jnp.exp(-cond)), (16, cond.shape[1])).astype(bf16)
    for i in range(3):
        mod_part[s, :, i * mod_cols : (i + 1) * mod_cols] = jnp.dot(
            lifted, mod_w[i], preferred_element_type=f32
        )[0:1]
    line_start(mod_at, modz_send, modz_recv)
    for copy in pair_copies[1:4]:
        copy.start()

    def wo_line(j, c, toward):
        part = wo.at[far, wo_rows(g, j, c)]
        return remote(
            part, part, wo_send.at[toward], wo_recv.at[j, c], (left_dev, right_dev)[toward]
        )

    def wo_across(j, c):
        part = wo.at[far, wo_rows(g, j, c)]
        return remote(part, part, woy_send, woy_recv.at[j, c // (WEIGHT_CHUNKS - 1)], y_dev)

    def wo_pass(j, c):
        part = wo.at[far, wo_rows(g, j, c)]
        remote(part, part, wop_send.at[g], wop_recv.at[g], pair_dev).start()

    def wo_share(j):
        begin = ((1 - g) * sp + j) * shard
        for n, (low_row, size) in enumerate(((0, shard - slab), (shard - slab, slab))):
            part = wo.at[far, pl.ds(pl.multiple_of(begin + low_row, 16), size)]
            remote(part, part, woy_send, woy_recv.at[j, n], y_dev).wait_recv()
            remote(part, part, wop_send.at[1 - g], wop_recv.at[1 - g], pair_dev).start()

    def wo_shares(k):
        for j, there in ((s - k, s >= k), (s + k, s + k < sp)):

            @pl.when(there)
            def _():
                wo_share(j)

    def wo_own(c):
        wo_line(s, c, 0).wait_recv()
        wo_across(s, c).start()
        wo_pass(s, c)

    def wo_own_line(c):
        for toward, has in ((0, has_left), (1, has_right)):

            @pl.when(has)
            def _():
                wo_line(s, c, toward).start()

    def wo_relay(e):
        k, c = e // WEIGHT_CHUNKS, lax.rem(e, WEIGHT_CHUNKS)
        for toward, has, j, there in (
            (1, has_right, s - k, s >= k),
            (0, has_left, s + k, s + k < sp),
        ):

            @pl.when(there)
            def _():
                wo_line(j, c, toward).wait_recv()

                @pl.when(has)
                def _():
                    wo_line(j, c, toward).start()

                wo_across(j, c).start()
                wo_pass(j, c)

    def wo_relays(low, high):
        def step(e, carry):
            wo_relay(e)
            return carry

        lax.fori_loop(low, high, step, 0)

    quarter = HD // 4
    inverse = jnp.exp(
        lax.rem(lane, quarter).astype(f32) * (-jnp.log(jnp.float32(rope_base)) / quarter)
    )
    first = lax.rem(lane, 2 * quarter) < quarter
    by_row = lax.rem(lane, HD) < HD // 2

    def tables(b, carry):
        place = s * total + jnp.where(b == 0, t, far) * rows + row
        coordinate = jnp.where(by_row, place // GRID_W, lax.rem(place, GRID_W))
        angles = coordinate.astype(f32) * inverse
        turn_cos[b] = jnp.cos(angles)
        sines = jnp.sin(angles)
        turn_sin[b] = jnp.where(first, -sines, sines)
        return carry

    contract = (((1,), (1,)), ((), ()))
    band = 3 * rows
    pairs = kw // HD
    stack = group * rows

    def biases(block, carry):
        q_pos = lax.broadcasted_iota(jnp.int32, (band, rows), 1)
        k_pos = lax.broadcasted_iota(jnp.int32, (band, rows), 0)
        place = s * total + jnp.where(block == 0, t, far) * rows - WIN + k_pos
        allowed = jnp.logical_and(
            jnp.logical_and(k_pos >= q_pos, k_pos <= q_pos + 2 * WIN),
            jnp.logical_and(place >= 0, place < sp * total),
        )
        bias[block] = jnp.where(allowed, 0.0, neg_large)
        return carry

    for c in range(2):
        wo_own(c)
        wo_own_line(c)
    line_relay(1, mod_at, modz_send, modz_recv)
    line_relay(1, ctx_at, ctxz_send, ctxz_recv)
    wo_own(2)
    wo_own_line(2)
    lax.fori_loop(0, 2, tables, 0)
    lax.fori_loop(0, 2, biases, 0)
    line_relay(2, mod_at, modz_send, modz_recv)
    for j in range(LATENT_CHUNKS // 4, AHEAD):
        lat_copy(j).start()
    for c in range(3, WEIGHT_CHUNKS):
        wo_own(c)
        wo_own_line(c)
    wo_relays(WEIGHT_CHUNKS, WEIGHT_CHUNKS + 1)
    pair_copies[4].start()
    line_relay(2, ctx_at, ctxz_send, ctxz_recv)
    for k in range(3, sp):
        line_relay(k, mod_at, modz_send, modz_recv)
    summed = mod_part[0]
    for k in range(1, sp):
        summed = summed + mod_part[k]
    mod_all[t] = summed
    for k in range(1, tp):
        remote(
            mod_all.at[t], mod_all.at[t], modt_send, modt_recv, {"tp": lax.rem(t + k, tp)}
        ).start()
    mods = remote(
        mod_all.at[0 : tp - 1], mod_all.at[0 : tp - 1], modt_send, modt_recv, pair_dev
    )
    for j in range(AHEAD, LATENT_CHUNKS - HELD):
        lat_copy(j).start()

    def start_held(who):
        @pl.when(core == who)
        def _():
            for j in range(LATENT_CHUNKS - HELD, LATENT_CHUNKS):
                lat_copy(j).start()

    start_held(0)
    wo_relays(WEIGHT_CHUNKS + 1, 2 * WEIGHT_CHUNKS)
    stat_copy.wait_recv()
    column = jnp.sum(
        jnp.where(diagonal, jnp.broadcast_to(stat_in[0:1], (rows, 128)), 0.0), axis=1, keepdims=True
    )
    row_scale[1] = jnp.broadcast_to(column, (rows, 128))

    mods.wait_recv()
    for i in range(tp):
        cols = slice(i * mod_cols, (i + 1) * mod_cols)
        shift_v[:, cols] = mod_all[i, :, 0:mod_cols]
        factor_v[:, cols] = gain_v[:, cols] * (1.0 + mod_all[i, :, mod_cols : 2 * mod_cols])
        gate_v[:, cols] = mod_all[i, :, 2 * mod_cols : 3 * mod_cols]

    def normalize(block, source, cols, lanes, target):
        scale = row_scale[block]
        for at in range(0, lanes, 128):
            here = pl.ds(pl.multiple_of(cols + at, 128), 128)
            values = source[:, here].astype(f32) * scale
            target[:, at : at + 128] = (values * factor_v[:, here] + shift_v[:, here]).astype(bf16)

    def project(j):
        normalize(1, lat_far, j * chunk, chunk, normed)
        cols = pl.ds(pl.multiple_of(j * chunk, 128), chunk)
        for slot in range(2):
            acc[slot] += jnp.dot(
                normed[:, 0:chunk], proj_w[slot, cols], preferred_element_type=f32
            )

    low = lane < HD

    def turned(block, values):
        swapped = jnp.where(
            first, pltpu.roll(values, 128 - quarter, 1), pltpu.roll(values, quarter, 1)
        )
        return values * turn_cos[block] + swapped * turn_sin[block]

    def finish_pairs(block, position):
        base = pl.ds(pl.multiple_of(position * rows, rows), rows)
        for slot in range(2):
            key_value[slot, base, 0:kw] = turned(block, acc[slot, :, qw : qw + kw]).astype(bf16)
            key_value[slot, base, kw : 2 * kw] = acc[slot, :, qw + kw : qw + 2 * kw].astype(bf16)

    def finish_queries(block, slot):
        factor = HD ** (-0.5)
        for u in range(heads // 2):
            lanes = turned(block, acc[slot, :, u * 128 : (u + 1) * 128]).astype(bf16)
            lanes = lanes.astype(f32) * factor
            swapped = pltpu.roll(lanes, HD, 1)
            keep = low if u == 0 else jnp.logical_not(low)
            for at in range(2):
                aligned = lanes if at == u else swapped
                queries[block, slot, u, at * rows : (at + 1) * rows] = jnp.where(
                    keep, aligned, 0.0
                ).astype(bf16)

    def kv_at(position):
        return key_value.at[:, pl.ds(pl.multiple_of(position * rows, rows), rows)]

    def kv_pair(block, position):
        return remote(
            kv_at(position), kv_at(position), kv_send, kv_recv.at[block], pair_dev
        )

    halo_down = remote(
        kv_at(1), kv_at(tp + 1), halo_sem.at[0], halo_sem.at[1], {**left_dev, "tp": pair}
    )
    halo_up = remote(kv_at(tp), kv_at(0), halo_sem.at[0], halo_sem.at[1], {**right_dev, "tp": pair})
    sends_down = jnp.logical_and(core == 0, has_left)
    sends_up = jnp.logical_and(core == 1, has_right)

    def send_halo(mine):
        @pl.when(jnp.logical_and(mine, sends_down))
        def _():
            halo_down.start()

        @pl.when(jnp.logical_and(mine, sends_up))
        def _():
            halo_up.start()

    def wait_halo(mine):
        @pl.when(jnp.logical_and(mine, sends_down))
        def _():
            halo_up.wait_recv()

        @pl.when(jnp.logical_and(mine, sends_up))
        def _():
            halo_down.wait_recv()

    def context_part(block, slot):
        units = range(pairs)
        scores = [
            lax.dot_general(
                ctx_kv[slot, :, 0:kw],
                queries[block, slot, u],
                contract,
                preferred_element_type=f32,
            )
            for u in units
        ]
        sinks = [
            jnp.concatenate(
                [sink_v[slot, u * group + h : u * group + h + 1] for h in range(group)], axis=1
            )
            for u in units
        ]
        tops = [
            jnp.maximum(jnp.max(scores[u], axis=0, keepdims=True), sinks[u]) for u in units
        ]
        exps = [jnp.exp(scores[u] - tops[u]) for u in units]
        for u in units:
            part_top[block, slot, u] = tops[u]
            part_sum[block, slot, u] = jnp.sum(exps[u], axis=0, keepdims=True) + jnp.exp(
                sinks[u] - tops[u]
            )
            part_out[block, slot, u] = jnp.dot(
                ctx_vt[slot, u * HD : (u + 1) * HD],
                exps[u].astype(bf16),
                preferred_element_type=f32,
            )

    def window_part(block, position, slot, skip, blocks):
        units = range(pairs)
        here = pl.ds(pl.multiple_of(skip * rows, rows), blocks * rows)
        window = pl.ds(pl.multiple_of((position - 1 + skip) * rows, rows), blocks * rows)
        mask = jnp.concatenate([bias[block, here]] * group, axis=1)
        scores = [
            lax.dot_general(
                key_value[slot, window, 0:kw],
                queries[block, slot, u],
                contract,
                preferred_element_type=f32,
            )
            + mask
            for u in units
        ]
        befores = [part_top[block, slot, u] for u in units]
        tops = [
            jnp.maximum(jnp.max(scores[u], axis=0, keepdims=True), befores[u]) for u in units
        ]
        exps = [jnp.exp(scores[u] - tops[u]) for u in units]
        keeps = [jnp.exp(befores[u] - tops[u]) for u in units]
        values = jnp.transpose(key_value[slot, window, kw : 2 * kw])
        bottoms = [
            jnp.sum(exps[u], axis=0, keepdims=True) + part_sum[block, slot, u] * keeps[u]
            for u in units
        ]
        results = [
            jnp.dot(
                values[u * HD : (u + 1) * HD], exps[u].astype(bf16), preferred_element_type=f32
            )
            + part_out[block, slot, u] * keeps[u]
            for u in units
        ]
        return tops, bottoms, results

    def window_early(block, position, slot, skip, blocks):
        tops, bottoms, results = window_part(block, position, slot, skip, blocks)
        for u in range(pairs):
            part_top[block, slot, u] = tops[u]
            part_sum[block, slot, u] = bottoms[u]
            part_out[block, slot, u] = results[u]

    def store_attended(results, bottoms, slot, target):
        for u in range(pairs):
            result = results[u] / bottoms[u]
            turned_back = jnp.concatenate(
                [result[:, h * rows : (h + 1) * rows] for h in range(group)], axis=0
            )
            target[slot, :, u * 128 : (u + 1) * 128] = jnp.transpose(turned_back).astype(bf16)

    def window_last(block, position, slot, skip, blocks, target):
        _, bottoms, results = window_part(block, position, slot, skip, blocks)
        store_attended(results, bottoms, slot, target)

    def attend_whole(block, position, slot, target):
        units = range(pairs)
        window = pl.ds(pl.multiple_of((position - 1) * rows, rows), band)
        mask = jnp.concatenate([bias[block]] * group, axis=1)
        wide = [
            lax.dot_general(
                ctx_kv[slot, :, 0:kw],
                queries[block, slot, u],
                contract,
                preferred_element_type=f32,
            )
            for u in units
        ]
        near = [
            lax.dot_general(
                key_value[slot, window, 0:kw],
                queries[block, slot, u],
                contract,
                preferred_element_type=f32,
            )
            + mask
            for u in units
        ]
        values = jnp.transpose(key_value[slot, window, kw : 2 * kw])
        sinks = [
            jnp.concatenate(
                [sink_v[slot, u * group + h : u * group + h + 1] for h in range(group)], axis=1
            )
            for u in units
        ]
        tops = [
            jnp.maximum(
                jnp.maximum(
                    jnp.max(wide[u], axis=0, keepdims=True),
                    jnp.max(near[u], axis=0, keepdims=True),
                ),
                sinks[u],
            )
            for u in units
        ]
        wide = [jnp.exp(wide[u] - tops[u]) for u in units]
        near = [jnp.exp(near[u] - tops[u]) for u in units]
        bottoms = [
            jnp.sum(wide[u], axis=0, keepdims=True)
            + jnp.sum(near[u], axis=0, keepdims=True)
            + jnp.exp(sinks[u] - tops[u])
            for u in units
        ]
        results = [
            jnp.dot(
                ctx_vt[slot, u * HD : (u + 1) * HD],
                wide[u].astype(bf16),
                preferred_element_type=f32,
            )
            + jnp.dot(
                values[u * HD : (u + 1) * HD], near[u].astype(bf16), preferred_element_type=f32
            )
            for u in units
        ]
        store_attended(results, bottoms, slot, target)

    edge = jnp.zeros((2, rows, 2 * kw), bf16)

    @pl.when(jnp.logical_and(core == 0, jnp.logical_not(has_left)))
    def _():
        key_value[:, 0:rows] = edge

    @pl.when(jnp.logical_and(core == 1, jnp.logical_not(has_right)))
    def _():
        key_value[:, (tp + 1) * rows : (tp + 2) * rows] = edge

    for i in range(10, 12):
        loads[i].wait()
    pair_copies[0].wait_recv()
    pair_weights = remote(
        proj_w.at[core], proj_w.at[core], pair_send.at[1], pair_recv.at[1], pair_dev
    )
    pair_weights.wait_recv()

    def far_step(j, carry):
        lat_copy(j).wait_recv()
        project(j)
        return carry

    normalize(0, lat_own, 0, width, normed)
    for slot in range(2):
        acc[slot] = jnp.dot(normed[...], proj_w[slot], preferred_element_type=f32)
    finish_pairs(0, t + 1)
    kv_pair(0, t + 1).start()
    send_halo(chip == core)
    for slot in range(2):
        finish_queries(0, slot)
    def wo_pair(gg):
        part = wo.at[far, pl.ds(pl.multiple_of(gg * sp * shard, 16), sp * shard)]
        return remote(part, part, wop_send.at[gg], wop_recv.at[gg], pair_dev)


    def wo_last(c):
        for k in range(3, sp):
            wo_relays(k * WEIGHT_CHUNKS + c, k * WEIGHT_CHUNKS + c + 1)

    wo_relays(2 * WEIGHT_CHUNKS, 2 * WEIGHT_CHUNKS + 1)
    for slot in range(2):
        acc[slot] = jnp.zeros(acc.shape[1:], f32)
    lax.fori_loop(0 * LATENT_CHUNKS // 8, 3 * LATENT_CHUNKS // 8, far_step, 0)
    for k in range(3, sp):
        line_relay(k, ctx_at, ctxz_send, ctxz_recv)
    ctx_pair = remote(ctx_kv.at[core], ctx_kv.at[core], ctxp_sem.at[0], ctxp_sem.at[1], pair_dev)
    ctx_pair.start()
    wo_relays(2 * WEIGHT_CHUNKS + 1, 2 * WEIGHT_CHUNKS + 2)
    lax.fori_loop(3 * LATENT_CHUNKS // 8, 5 * LATENT_CHUNKS // 8, far_step, 0)
    wo_relays(2 * WEIGHT_CHUNKS + 2, 2 * WEIGHT_CHUNKS + 3)
    ctx_pair.wait_recv()
    for slot in range(2):
        ctx_vt[slot] = jnp.transpose(ctx_kv[slot, :, kw : 2 * kw])
    context_part(0, 0)
    kv_pair(0, pair + 1).wait_recv()
    window_early(0, t + 1, 0, 1 - core, 2)
    wo_relays(2 * WEIGHT_CHUNKS + 3, 3 * WEIGHT_CHUNKS)
    context_part(0, 1)
    window_early(0, t + 1, 1, 1 - core, 2)
    start_held(1)
    wo_last(0)
    wo_share(s)
    wo_shares(1)
    lax.fori_loop(5 * LATENT_CHUNKS // 8, 6 * LATENT_CHUNKS // 8, far_step, 0)
    wo_last(1)
    lax.fori_loop(6 * LATENT_CHUNKS // 8, 7 * LATENT_CHUNKS // 8, far_step, 0)
    wo_last(2)
    lax.fori_loop(7 * LATENT_CHUNKS // 8, LATENT_CHUNKS, far_step, 0)
    finish_pairs(1, far + 1)
    kv_pair(1, far + 1).start()
    send_halo(chip != core)
    for c in range(3, WEIGHT_CHUNKS):
        wo_last(c)
    finish_queries(1, 0)

    context_part(1, 0)

    def att_copy(slot):
        return remote(
            att_out.at[slot], att.at[chip, slot], att_send, att_recv.at[slot], far_dev
        )

    kv_pair(1, pair + 1).wait_recv()
    wait_halo(chip != core)
    window_last(1, far + 1, 0, 0, 3, att_out)
    att_copy(0).start()
    finish_queries(1, 1)
    attend_whole(1, far + 1, 1, att_out)
    att_copy(1).start()
    wo_shares(2)
    wait_halo(chip == core)
    for slot in range(2):
        window_last(0, t + 1, slot, 2 * core, 1, att.at[chip])
    for k in range(3, sp):
        wo_shares(k)
    pair_copies[4].wait_recv()
    other = (1 - chip) * 2 + 1 - core
    order = (t, pair, far, other)

    def product(x, slot, i):
        part = pl.ds(pl.multiple_of((2 * x + slot) * qw, qw), qw)
        return jnp.dot(att[x, slot], wo[i, part], preferred_element_type=f32)

    def out_own(k):
        out_part[k] = product(chip, 0, order[k]) + product(chip, 1, order[k])

    def out_first(k):
        out_part[k] += product(1 - chip, 0, order[k])

    def out_last(k):
        cols = pl.ds(pl.multiple_of(order[k] * out_width, 128), out_width)
        sums = out_part[k] + product(1 - chip, 1, order[k])
        blended = sums.astype(bf16).astype(f32)
        mixed[:, cols] = (lat_own[:, cols].astype(f32) + gate_v[:, cols] * blended).astype(bf16)

    out_own(0)
    out_own(1)
    out_own(2)
    att_copy(0).wait_recv()
    for k in range(3):
        out_first(k)
    for gg in range(2):
        part = wo.at[other, pl.ds(gg * sp * shard, sp * shard)]
        remote(part, part, wop_send.at[gg], wop_recv.at[gg], pair_dev).wait_recv()
    out_part[3] = (
        product(chip, 0, other) + product(chip, 1, other) + product(1 - chip, 0, other)
    )
    att_copy(1).wait_recv()
    for k in range(4):
        out_last(k)

    stat_copy.wait_send()
    remote(wo_shard, wo_shard, wox_send, wo_recv.at[0, 0], far_dev).wait_send()
    remote(lat_own, lat_far, lat_send, lat_recv.at[0], far_dev).wait_send()
    pair_copies[0].wait_send()
    pair_weights.wait_send()
    pair_copies[4].wait_send()
    mods.wait_send()
    line_finish(lambda count: mod_part.at[0:count], modz_send)
    line_finish(lambda count: ctx_kv.at[core, 0 : count * ctx_rows], ctxz_send)
    ctx_pair.wait_send()
    def wo_total(count):
        return wo.at[far, 0 : count * shard]

    line_finish(wo_total, wo_send)
    wo_sent = wo.at[far, pl.ds(pl.multiple_of(g * sp * shard, 16), sp * shard)]
    remote(wo_sent, wo_sent, woy_send, woy_recv.at[0, 0], y_dev).wait_send()
    wo_pair(0).wait_send()
    wo_pair(1).wait_send()
    both = key_value.at[:, 0 : 2 * rows]
    remote(both, both, kv_send, kv_recv.at[0], pair_dev).wait_send()

    @pl.when(sends_down)
    def _():
        halo_down.wait_send()

    @pl.when(sends_up)
    def _():
        halo_up.wait_send()

    remote(att_out, att_out, att_send, att_recv.at[0], far_dev).wait_send()


def local(
    latent,
    context,
    conditioning,
    norm_gain,
    shift_weight,
    scale_weight,
    gate_weight,
    query_weight,
    key_weight,
    value_weight,
    out_weight,
    sink_logit,
):
    tp, sp, grp = lax.axis_size("tp"), lax.axis_size("sp"), lax.axis_size("grp")
    rows, width = latent.shape
    ctx_rows = context.shape[0]
    mod_rows, mod_cols = shift_weight.shape
    query_width, key_width = query_weight.shape[1], key_weight.shape[1]
    out_rows, out_width = out_weight.shape
    fits = (
        rows == WIN
        and rows == 128
        and key_width == 2 * HD
        and query_width == 4 * HD
        and tp == 4
        and grp == 2
        and sp >= 3
        and sp * ctx_rows % 128 == 0
        and ctx_rows % CONTEXT_ROWS == 0
        and width % 512 == 0
        and mod_cols % 128 == 0
        and width % (128 * LATENT_CHUNKS) == 0
        and out_width % 128 == 0
        and tp * out_width == width
        and out_rows == tp * query_width
        and out_rows % (2 * sp * WEIGHT_CHUNKS * 16) == 0
    )
    if not fits:
        return local_plain(
            latent,
            context,
            conditioning,
            norm_gain,
            shift_weight,
            scale_weight,
            gate_weight,
            query_weight,
            key_weight,
            value_weight,
            out_weight,
            sink_logit,
        )
    f32, bf16 = jnp.float32, jnp.bfloat16
    dma = pltpu.SemaphoreType.DMA
    anywhere = pl.BlockSpec(memory_space=pl.ANY)
    return pl.pallas_call(
        functools.partial(fused_kernel, sp),
        out_shape=pltpu.VMEM((rows, width), bf16),
        in_specs=[anywhere] * 11 + [pl.BlockSpec(memory_space=pltpu.SMEM)],
        out_specs=pl.BlockSpec(memory_space=pltpu.VMEM),
        scratch_shapes=[
            pltpu.VMEM((mod_rows,), bf16),
            pltpu.VMEM((1, width), f32),
            pltpu.VMEM((3, mod_rows, mod_cols), bf16),
            pltpu.VMEM((2, width, query_width + 2 * key_width), bf16),
            pltpu.VMEM((tp, out_rows, out_width), bf16),
            pltpu.VMEM((out_rows // (2 * sp), out_width), bf16),
            pltpu.VMEM(context.shape, bf16),
            pltpu.VMEM((rows, width), bf16),
            pltpu.VMEM((rows, width), bf16),
            pltpu.VMEM((rows, width), bf16),
            pltpu.VMEM((8, 128), f32),
            pltpu.VMEM((8, 128), f32),
            pltpu.VMEM((2, rows, 128), f32),
            pltpu.VMEM((2, 8, 128), f32),
            pltpu.VMEM((sp, 1, 3 * mod_cols), f32),
            pltpu.VMEM((tp, 1, 3 * mod_cols), f32),
            pltpu.VMEM((1, width), f32),
            pltpu.VMEM((1, width), f32),
            pltpu.VMEM((1, width), f32),
            pltpu.VMEM((2, rows, 128), f32),
            pltpu.VMEM((2, rows, 128), f32),
            pltpu.VMEM((2, rows, query_width + 2 * key_width), f32),
            pltpu.VMEM((2, 2, 2, 2 * rows, key_width), bf16),
            pltpu.VMEM((2, (tp + 2) * rows, 2 * key_width), bf16),
            pltpu.VMEM((2, sp * ctx_rows, 2 * key_width), bf16),
            pltpu.VMEM((2, 2, rows, query_width), bf16),
            pltpu.VMEM((2, rows, query_width), bf16),
            pltpu.VMEM((2, key_width, sp * ctx_rows), bf16),
            pltpu.VMEM((2, 3 * rows, rows), f32),
            pltpu.VMEM((2, 2, 2, HD, 2 * rows), f32),
            pltpu.VMEM((2, 2, 2, 1, 2 * rows), f32),
            pltpu.VMEM((2, 2, 2, 1, 2 * rows), f32),
            pltpu.VMEM((tp, rows, out_width), f32),
            dma((9,)),
            dma,
            dma((LATENT_CHUNKS,)),
            dma((2,)),
            dma((3,)),
            dma((3,)),
            dma,
            dma((2,)),
            dma((sp, WEIGHT_CHUNKS)),
            dma,
            dma((sp, 2)),
            dma((2,)),
            dma((2,)),
            dma((2,)),
            dma((sp,)),
            dma,
            dma,
            dma((2,)),
            dma((sp,)),
            dma((2,)),
            dma,
            dma((2,)),
            dma((2,)),
            dma,
            dma((2,)),
        ],
        compiler_params=pltpu.CompilerParams(
            collective_id=0,
            has_side_effects=True,
            vmem_limit_bytes=60 * 1024 * 1024,
        ),
        name="fused",
    )(
        latent,
        context,
        conditioning,
        norm_gain.reshape(1, width),
        shift_weight,
        scale_weight,
        gate_weight,
        query_weight,
        key_weight,
        value_weight,
        out_weight,
        sink_logit,
    )


def solution(mesh):
    in_specs = (
        P(("grp", "sp", "tp"), None),
        P(("grp", "sp"), None),
        P(("grp", "sp")),
        P(),
        P("sp", "tp"),
        P("sp", "tp"),
        P("sp", "tp"),
        P(None, "tp"),
        P(None, "tp"),
        P(None, "tp"),
        P(None, "tp"),
        P("tp"),
    )
    out_specs = P(("grp", "sp", "tp"), None)
    return jax.shard_map(local, mesh=mesh, in_specs=in_specs, out_specs=out_specs, check_vma=False)
```

```python
import functools

import jax
import jax.numpy as jnp
from jax import lax
from jax.experimental import pallas as pl
from jax.experimental.pallas import tpu as pltpu
from jax.sharding import PartitionSpec as P

HEADS = 16
KV_HEADS = 8
HD = 64
GRID_W = 64
WIN = 128


epsilon = 1e-06
rope_base = 10000.0
neg_large = -1e30


def with_halo(cells, sides, width):
    for axis, dim in sides:
        count = lax.axis_size(axis)
        ends = count - 1
        head = lax.slice_in_dim(cells, 0, width, axis=dim)
        tail = lax.slice_in_dim(cells, cells.shape[dim] - width, cells.shape[dim], axis=dim)
        cells = jnp.concatenate(
            [
                lax.ppermute(tail, axis, [(i, (i + 1) % count) for i in range(ends)]),
                cells,
                lax.ppermute(head, axis, [((i + 1) % count, i) for i in range(ends)]),
            ],
            axis=dim,
        )
    return cells


def row_norm(matrix, norm_gain):
    values = matrix.astype(jnp.float32)
    return (
        values * lax.rsqrt(jnp.mean(values * values, axis=-1, keepdims=True) + epsilon) * norm_gain
    )


def axial_turn(values, position):
    half_dim = values.shape[-1] // 2
    quarter = half_dim // 2
    inverse = rope_base ** (-jnp.arange(quarter, dtype=jnp.float32) / quarter)

    def turn(section, coordinate):
        angles = coordinate.astype(jnp.float32)[:, None] * inverse[None, :]
        cosine = jnp.cos(angles)[:, None, :]
        sine_part = jnp.sin(angles)[:, None, :]
        leading = section[..., :quarter]
        trailing = section[..., quarter:]
        return jnp.concatenate(
            [leading * cosine - trailing * sine_part, leading * sine_part + trailing * cosine],
            axis=-1,
        )

    return jnp.concatenate(
        [
            turn(values[..., :half_dim], position // GRID_W),
            turn(values[..., half_dim:], position % GRID_W),
        ],
        axis=-1,
    )


def context_pairs(context_rows, norm_gain, key_weight, value_weight):
    prepared = row_norm(context_rows, norm_gain).astype(jnp.bfloat16)
    return jnp.concatenate(
        [
            jnp.dot(prepared, key_weight, preferred_element_type=jnp.float32),
            jnp.dot(prepared, value_weight, preferred_element_type=jnp.float32),
        ],
        axis=1,
    ).astype(jnp.bfloat16)


def local_plain(
    latent,
    context,
    conditioning,
    norm_gain,
    shift_weight,
    scale_weight,
    gate_weight,
    query_weight,
    key_weight,
    value_weight,
    out_weight,
    sink_logit,
):
    lifted = jax.nn.silu(conditioning.astype(jnp.float32)).astype(jnp.bfloat16)[None, :]
    shift_part = jnp.dot(lifted, shift_weight, preferred_element_type=jnp.float32)[0]
    scale_part = jnp.dot(lifted, scale_weight, preferred_element_type=jnp.float32)[0]
    gate_part = jnp.dot(lifted, gate_weight, preferred_element_type=jnp.float32)[0]
    summed = lax.psum((shift_part, scale_part, gate_part), "sp")
    shift_vec, scale_vec, gate_vec = (
        lax.all_gather(summed[0], "tp", axis=0, tiled=True),
        lax.all_gather(summed[1], "tp", axis=0, tiled=True),
        lax.all_gather(summed[2], "tp", axis=0, tiled=True),
    )
    normed = (row_norm(latent, norm_gain) * (1.0 + scale_vec) + shift_vec).astype(jnp.bfloat16)
    segment = lax.all_gather(normed, "tp", axis=0, tiled=True)
    projected = jnp.concatenate(
        [
            jnp.dot(segment, query_weight, preferred_element_type=jnp.float32),
            jnp.dot(segment, key_weight, preferred_element_type=jnp.float32),
            jnp.dot(segment, value_weight, preferred_element_type=jnp.float32),
        ],
        axis=1,
    )
    row_count = projected.shape[0]
    query_width = query_weight.shape[1]
    key_width = key_weight.shape[1]
    query_heads = query_width // HD
    pair_heads = key_width // HD
    group_size = HEADS // KV_HEADS
    row_offset = lax.axis_index("sp") * row_count
    position = row_offset + jnp.arange(row_count, dtype=jnp.int32)
    queries = axial_turn(
        projected[:, :query_width].reshape(row_count, query_heads, HD), position
    ).astype(jnp.bfloat16)
    latent_keys = axial_turn(
        projected[:, query_width : query_width + key_width].reshape(row_count, pair_heads, HD),
        position,
    ).astype(jnp.bfloat16)
    latent_values = projected[:, query_width + key_width :].astype(jnp.bfloat16)
    key_value = jnp.concatenate([latent_keys.reshape(row_count, key_width), latent_values], axis=1)
    widened = with_halo(key_value, (("sp", 0),), WIN)
    context_all = lax.all_gather(
        context_pairs(context, norm_gain, key_weight, value_weight), "sp", axis=0, tiled=True
    )
    block_count = row_count // WIN
    context_count = context_all.shape[0]
    query_blocks = queries.reshape(block_count, WIN, pair_heads, group_size, HD)
    band_blocks = widened.reshape(block_count + 2, WIN, 2 * key_width)
    band_rows = jnp.concatenate(
        [band_blocks[:block_count], band_blocks[1 : block_count + 1], band_blocks[2:]], axis=1
    )
    band_keys = band_rows[..., :key_width].reshape(block_count, 3 * WIN, pair_heads, HD)
    band_values = band_rows[..., key_width:].reshape(block_count, 3 * WIN, pair_heads, HD)
    context_keys = context_all[:, :key_width].reshape(context_count, pair_heads, HD)
    context_values = context_all[:, key_width:].reshape(context_count, pair_heads, HD)
    factor = HD ** (-0.5)
    local_scores = (
        jnp.einsum("nqhgd,nkhd->nhgqk", query_blocks, band_keys, preferred_element_type=jnp.float32)
        * factor
    )
    query_pos = position.reshape(block_count, WIN)
    key_pos = (
        row_offset
        - WIN
        + jnp.arange(block_count, dtype=jnp.int32)[:, None] * WIN
        + jnp.arange(3 * WIN, dtype=jnp.int32)[None, :]
    )
    seq_total = row_count * lax.axis_size("sp")
    allowed = (
        (jnp.abs(key_pos[:, None, :] - query_pos[:, :, None]) <= WIN)
        & (key_pos[:, None, :] >= 0)
        & (key_pos[:, None, :] < seq_total)
    )
    local_scores = jnp.where(allowed[:, None, None], local_scores, neg_large)
    context_scores = (
        jnp.einsum(
            "nqhgd,thd->nhgqt", query_blocks, context_keys, preferred_element_type=jnp.float32
        )
        * factor
    )
    sink_values = sink_logit.reshape(pair_heads, group_size)[None, :, :, None, None]
    highest = jnp.maximum(
        jnp.maximum(
            jnp.max(local_scores, axis=-1, keepdims=True),
            jnp.max(context_scores, axis=-1, keepdims=True),
        ),
        sink_values,
    )
    local_exp = jnp.exp(local_scores - highest)
    context_exp = jnp.exp(context_scores - highest)
    denominator = (
        jnp.sum(local_exp, axis=-1, keepdims=True)
        + jnp.sum(context_exp, axis=-1, keepdims=True)
        + jnp.exp(sink_values - highest)
    )
    local_weights = (local_exp / denominator).astype(jnp.bfloat16)
    context_weights = (context_exp / denominator).astype(jnp.bfloat16)
    attended = jnp.einsum(
        "nhgqk,nkhd->nqhgd", local_weights, band_values, preferred_element_type=jnp.float32
    ) + jnp.einsum(
        "nhgqt,thd->nqhgd", context_weights, context_values, preferred_element_type=jnp.float32
    )
    attended = attended.reshape(row_count, query_width).astype(jnp.bfloat16)
    columns_part = jnp.dot(
        lax.all_gather(attended, "tp", axis=1, tiled=True),
        out_weight,
        preferred_element_type=jnp.float32,
    ).astype(jnp.bfloat16)
    blended = lax.all_to_all(columns_part, "tp", split_axis=0, concat_axis=1, tiled=True)
    return (latent.astype(jnp.float32) + gate_vec * blended.astype(jnp.float32)).astype(
        jnp.bfloat16
    )


LATENT_CHUNKS = 16
WEIGHT_CHUNKS = 4
HELD = 2
AHEAD = 3 * LATENT_CHUNKS // 8
NORM_ROWS = 16
CONTEXT_ROWS = 32


def remote(src, dst, send, recv, device):
    return pltpu.make_async_remote_copy(
        src_ref=src,
        dst_ref=dst,
        send_sem=send,
        recv_sem=recv,
        device_id=device,
        device_id_type=pl.DeviceIdType.MESH,
    )


def fused_kernel(
    sp,
    latent,
    context,
    conditioning,
    norm_gain,
    shift_weight,
    scale_weight,
    gate_weight,
    query_weight,
    key_weight,
    value_weight,
    out_weight,
    sink,
    mixed,
    cond_v,
    gain_v,
    mod_w,
    proj_w,
    wo,
    wo_shard,
    ctx_v,
    lat_own,
    lat_far,
    normed,
    stat_out,
    stat_in,
    row_scale,
    sink_v,
    mod_part,
    mod_all,
    factor_v,
    shift_v,
    gate_v,
    turn_cos,
    turn_sin,
    acc,
    queries,
    key_value,
    ctx_kv,
    att,
    att_out,
    ctx_vt,
    bias,
    part_out,
    part_top,
    part_sum,
    out_part,
    load_sem,
    lat_send,
    lat_recv,
    stat_sem,
    pair_send,
    pair_recv,
    wox_send,
    wo_send,
    wo_recv,
    woy_send,
    woy_recv,
    wop_send,
    wop_recv,
    modz_send,
    modz_recv,
    modt_send,
    modt_recv,
    ctxz_send,
    ctxz_recv,
    ctxp_sem,
    kv_send,
    kv_recv,
    halo_sem,
    att_send,
    att_recv,
):
    g = lax.axis_index("grp")
    s = lax.axis_index("sp")
    t = lax.axis_index("tp")
    chip = t // 2
    core = lax.rem(t, 2)
    pair = chip * 2 + 1 - core
    far = (1 - chip) * 2 + core
    pair_dev, far_dev, y_dev = {"tp": pair}, {"tp": far}, {"grp": 1 - g}
    right_dev = {"sp": lax.rem(s + 1, sp)}
    left_dev = {"sp": lax.rem(s + sp - 1, sp)}
    has_right, has_left = s < sp - 1, s > 0
    rows, width = latent.shape
    ctx_rows = context.shape[0]
    mod_cols = shift_weight.shape[1]
    qw = query_weight.shape[1]
    kw = key_weight.shape[1]
    heads = qw // HD
    group = heads // (kw // HD)
    tp = 4
    total = tp * rows
    out_rows, out_width = out_weight.shape
    half = rows // 2
    f32, bf16 = jnp.float32, jnp.bfloat16
    chunk = width // LATENT_CHUNKS
    shard = out_rows // (2 * sp)
    slab = shard // WEIGHT_CHUNKS
    MESH = pl.DeviceIdType.MESH

    loads = [
        (out_weight.at[pl.ds(pl.multiple_of((g * sp + s) * shard, 16), shard)], wo_shard),
        (latent, lat_own),
        (norm_gain, gain_v),
        (context, ctx_v),
        (key_weight, proj_w.at[core, :, qw : qw + kw]),
        (value_weight, proj_w.at[core, :, qw + kw : qw + 2 * kw]),
        (conditioning, cond_v),
        (shift_weight, mod_w.at[0]),
        (scale_weight, mod_w.at[1]),
        (gate_weight, mod_w.at[2]),
        (query_weight, proj_w.at[core, :, 0:qw]),
        (out_weight, wo.at[t]),
    ]
    slots = (0, 1, 2, 3, 4, 4, 5, 6, 6, 6, 7, 8)
    loads = [
        pltpu.make_async_copy(a, b, load_sem.at[i]) for i, (a, b) in zip(slots, loads, strict=True)
    ]
    for load in loads:
        load.start()

    barrier = pltpu.get_barrier_semaphore()
    for k in range(1, tp):
        pl.semaphore_signal(
            barrier, inc=1, device_id={"tp": lax.rem(t + k, tp)}, device_id_type=MESH
        )
    pl.semaphore_signal(barrier, inc=1, device_id=y_dev, device_id_type=MESH)
    for has, place in ((has_right, right_dev), (has_left, left_dev)):

        @pl.when(has)
        def _():
            for peer in (t, pair):
                pl.semaphore_signal(
                    barrier, inc=1, device_id={**place, "tp": peer}, device_id_type=MESH
                )

    def row_factor(source, part):
        squares = None
        for at in range(0, width, 512):
            values = source[part, at : at + 512].astype(f32)
            values = values * values
            squares = values if squares is None else squares + values
        return lax.rsqrt(jnp.sum(squares, axis=-1, keepdims=True) * (1.0 / width) + epsilon)

    lane = lax.broadcasted_iota(jnp.int32, (rows, 128), 1)
    row = lax.broadcasted_iota(jnp.int32, (rows, 128), 0)
    diagonal = lane == row

    pl.semaphore_wait(
        barrier, tp + jnp.where(has_right, 2, 0) + jnp.where(has_left, 2, 0)
    )

    def lat_copy(j):
        cols = pl.ds(pl.multiple_of(j * chunk, 128), chunk)
        return remote(
            lat_own.at[:, cols], lat_far.at[:, cols], lat_send, lat_recv.at[j], far_dev
        )

    def wo_rows(gg, j, c):
        return pl.ds(pl.multiple_of((gg * sp + j) * shard + c * slab, 16), slab)

    def wo_cross(c):
        part = wo_rows(g, s, c)
        return remote(
            wo_shard.at[pl.ds(c * slab, slab)],
            wo.at[t, part],
            wox_send,
            wo_recv.at[s, c],
            far_dev,
        )

    loads[0].wait()
    for c in range(WEIGHT_CHUNKS):
        wo_cross(c).start()
    loads[1].wait()

    def row_stat(i, carry):
        part = pl.ds(pl.multiple_of(i * CONTEXT_ROWS, 16), CONTEXT_ROWS)
        row_scale[0, part] = jnp.broadcast_to(row_factor(lat_own, part), (CONTEXT_ROWS, 128))
        return carry

    lax.fori_loop(0, rows // CONTEXT_ROWS, row_stat, 0)
    flat = jnp.sum(jnp.where(diagonal, row_scale[0], 0.0), axis=0, keepdims=True)
    stat_out[...] = jnp.broadcast_to(flat, (8, 128))
    sink_row = lax.broadcasted_iota(jnp.int32, (8, 128), 0)
    sink_all = jnp.full((8, 128), sink[0], f32)
    for h in range(1, heads):
        sink_all = jnp.where(sink_row == h, sink[h], sink_all)
    sink_v[core] = sink_all

    stat_copy = remote(stat_out, stat_in, stat_sem.at[0], stat_sem.at[1], far_dev)
    stat_copy.start()
    for j in range(LATENT_CHUNKS // 4):
        lat_copy(j).start()
    pair_copies = [
        (sink_v.at[core], sink_v.at[core]),
        (query_weight, proj_w.at[core, :, 0:qw]),
        (key_weight, proj_w.at[core, :, qw : qw + kw]),
        (value_weight, proj_w.at[core, :, qw + kw : qw + 2 * kw]),
        (out_weight, wo.at[t]),
    ]
    pair_copies = [
        remote(a, b, pair_send.at[i], pair_recv.at[i], pair_dev)
        for i, (a, b) in zip((0, 1, 1, 1, 2), pair_copies, strict=True)
    ]
    pair_copies[0].start()

    def line_copy(at, j, send, recv, toward):
        return remote(at(j), at(j), send.at[toward], recv.at[j], (left_dev, right_dev)[toward])

    def line_start(at, send, recv):
        for toward, has in ((0, has_left), (1, has_right)):

            @pl.when(has)
            def _():
                line_copy(at, s, send, recv, toward).start()

    def line_relay(k, at, send, recv):
        for toward, has, j, there in (
            (1, has_right, s - k, s >= k),
            (0, has_left, s + k, s + k < sp),
        ):

            @pl.when(there)
            def _():
                line_copy(at, j, send, recv, toward).wait_recv()

                @pl.when(has)
                def _():
                    line_copy(at, j, send, recv, toward).start()

    def line_finish(total_of, send):
        for toward, has, sent in ((1, has_right, s + 1), (0, has_left, sp - s)):
            for count in range(1, sp + 1):

                @pl.when(jnp.logical_and(has, sent == count))
                def _():
                    part = total_of(count)
                    remote(part, part, send.at[toward], stat_sem.at[1], right_dev).wait_send()

    def mod_at(j):
        return mod_part.at[j]

    def ctx_at(j):
        return ctx_kv.at[core, pl.ds(pl.multiple_of(j * ctx_rows, 16), ctx_rows)]

    loads[2].wait()
    loads[3].wait()
    kv_weights = proj_w.at[core, :, qw : qw + 2 * kw]
    pltpu.make_async_copy(kv_weights, kv_weights, load_sem.at[4]).wait()

    def norm_context(i, carry):
        part = pl.ds(pl.multiple_of(i * CONTEXT_ROWS, 16), CONTEXT_ROWS)
        scale = row_factor(ctx_v, part)
        for at in range(0, width, 512):
            here = slice(at, at + 512)
            values = ctx_v[part, here].astype(f32)
            ctx_v[part, here] = (values * scale * gain_v[:, here]).astype(bf16)
        return carry

    lax.fori_loop(0, ctx_rows // CONTEXT_ROWS, norm_context, 0)
    own_ctx = pl.ds(pl.multiple_of(s * ctx_rows, 16), ctx_rows)
    ctx_kv[core, own_ctx] = jnp.dot(
        ctx_v[...], proj_w[core, :, qw : qw + 2 * kw], preferred_element_type=f32
    ).astype(bf16)
    line_start(ctx_at, ctxz_send, ctxz_recv)
    loads[6].wait()
    pltpu.make_async_copy(mod_w, mod_w, load_sem.at[6]).wait()
    cond = cond_v[...].astype(f32).reshape(1, cond_v.shape[0])
    lifted = jnp.broadcast_to(cond / (1.0 + jnp.exp(-cond)), (16, cond.shape[1])).astype(bf16)
    for i in range(3):
        mod_part[s, :, i * mod_cols : (i + 1) * mod_cols] = jnp.dot(
            lifted, mod_w[i], preferred_element_type=f32
        )[0:1]
    line_start(mod_at, modz_send, modz_recv)
    for copy in pair_copies[1:4]:
        copy.start()

    def wo_line(j, c, toward):
        part = wo.at[far, wo_rows(g, j, c)]
        return remote(
            part, part, wo_send.at[toward], wo_recv.at[j, c], (left_dev, right_dev)[toward]
        )

    def wo_across(j, c):
        part = wo.at[far, wo_rows(g, j, c)]
        return remote(part, part, woy_send, woy_recv.at[j, c // (WEIGHT_CHUNKS - 1)], y_dev)

    def wo_pass(j, c):
        part = wo.at[far, wo_rows(g, j, c)]
        remote(part, part, wop_send.at[g], wop_recv.at[g], pair_dev).start()

    def wo_share(j):
        begin = ((1 - g) * sp + j) * shard
        for n, (low_row, size) in enumerate(((0, shard - slab), (shard - slab, slab))):
            part = wo.at[far, pl.ds(pl.multiple_of(begin + low_row, 16), size)]
            remote(part, part, woy_send, woy_recv.at[j, n], y_dev).wait_recv()
            remote(part, part, wop_send.at[1 - g], wop_recv.at[1 - g], pair_dev).start()

    def wo_shares(k):
        for j, there in ((s - k, s >= k), (s + k, s + k < sp)):

            @pl.when(there)
            def _():
                wo_share(j)

    def wo_own(c):
        wo_line(s, c, 0).wait_recv()
        wo_across(s, c).start()
        wo_pass(s, c)

    def wo_own_line(c):
        for toward, has in ((0, has_left), (1, has_right)):

            @pl.when(has)
            def _():
                wo_line(s, c, toward).start()

    def wo_relay(e):
        k, c = e // WEIGHT_CHUNKS, lax.rem(e, WEIGHT_CHUNKS)
        for toward, has, j, there in (
            (1, has_right, s - k, s >= k),
            (0, has_left, s + k, s + k < sp),
        ):

            @pl.when(there)
            def _():
                wo_line(j, c, toward).wait_recv()

                @pl.when(has)
                def _():
                    wo_line(j, c, toward).start()

                wo_across(j, c).start()
                wo_pass(j, c)

    def wo_relays(low, high):
        def step(e, carry):
            wo_relay(e)
            return carry

        lax.fori_loop(low, high, step, 0)

    quarter = HD // 4
    inverse = jnp.exp(
        lax.rem(lane, quarter).astype(f32) * (-jnp.log(jnp.float32(rope_base)) / quarter)
    )
    first = lax.rem(lane, 2 * quarter) < quarter
    by_row = lax.rem(lane, HD) < HD // 2

    def tables(b, carry):
        place = s * total + jnp.where(b == 0, t, far) * rows + row
        coordinate = jnp.where(by_row, place // GRID_W, lax.rem(place, GRID_W))
        angles = coordinate.astype(f32) * inverse
        turn_cos[b] = jnp.cos(angles)
        sines = jnp.sin(angles)
        turn_sin[b] = jnp.where(first, -sines, sines)
        return carry

    contract = (((1,), (1,)), ((), ()))
    band = 3 * rows
    pairs = kw // HD
    stack = group * rows

    def biases(block, carry):
        q_pos = lax.broadcasted_iota(jnp.int32, (band, rows), 1)
        k_pos = lax.broadcasted_iota(jnp.int32, (band, rows), 0)
        place = s * total + jnp.where(block == 0, t, far) * rows - WIN + k_pos
        allowed = jnp.logical_and(
            jnp.logical_and(k_pos >= q_pos, k_pos <= q_pos + 2 * WIN),
            jnp.logical_and(place >= 0, place < sp * total),
        )
        bias[block] = jnp.where(allowed, 0.0, neg_large)
        return carry

    for c in range(2):
        wo_own(c)
        wo_own_line(c)
    line_relay(1, mod_at, modz_send, modz_recv)
    line_relay(1, ctx_at, ctxz_send, ctxz_recv)
    wo_own(2)
    wo_own_line(2)
    lax.fori_loop(0, 2, tables, 0)
    lax.fori_loop(0, 2, biases, 0)
    line_relay(2, mod_at, modz_send, modz_recv)
    for j in range(LATENT_CHUNKS // 4, AHEAD):
        lat_copy(j).start()
    for c in range(3, WEIGHT_CHUNKS):
        wo_own(c)
        wo_own_line(c)
    wo_relays(WEIGHT_CHUNKS, WEIGHT_CHUNKS + 1)
    pair_copies[4].start()
    line_relay(2, ctx_at, ctxz_send, ctxz_recv)
    for k in range(3, sp):
        line_relay(k, mod_at, modz_send, modz_recv)
    summed = mod_part[0]
    for k in range(1, sp):
        summed = summed + mod_part[k]
    mod_all[t] = summed
    for k in range(1, tp):
        remote(
            mod_all.at[t], mod_all.at[t], modt_send, modt_recv, {"tp": lax.rem(t + k, tp)}
        ).start()
    mods = remote(
        mod_all.at[0 : tp - 1], mod_all.at[0 : tp - 1], modt_send, modt_recv, pair_dev
    )
    for j in range(AHEAD, LATENT_CHUNKS - HELD):
        lat_copy(j).start()

    def start_held(who):
        @pl.when(core == who)
        def _():
            for j in range(LATENT_CHUNKS - HELD, LATENT_CHUNKS):
                lat_copy(j).start()

    start_held(0)
    wo_relays(WEIGHT_CHUNKS + 1, 2 * WEIGHT_CHUNKS)
    stat_copy.wait_recv()
    column = jnp.sum(
        jnp.where(diagonal, jnp.broadcast_to(stat_in[0:1], (rows, 128)), 0.0), axis=1, keepdims=True
    )
    row_scale[1] = jnp.broadcast_to(column, (rows, 128))

    mods.wait_recv()
    for i in range(tp):
        cols = slice(i * mod_cols, (i + 1) * mod_cols)
        shift_v[:, cols] = mod_all[i, :, 0:mod_cols]
        factor_v[:, cols] = gain_v[:, cols] * (1.0 + mod_all[i, :, mod_cols : 2 * mod_cols])
        gate_v[:, cols] = mod_all[i, :, 2 * mod_cols : 3 * mod_cols]

    def normalize(block, source, cols, lanes, target):
        scale = row_scale[block]
        for at in range(0, lanes, 128):
            here = pl.ds(pl.multiple_of(cols + at, 128), 128)
            values = source[:, here].astype(f32) * scale
            target[:, at : at + 128] = (values * factor_v[:, here] + shift_v[:, here]).astype(bf16)

    def project(j):
        normalize(1, lat_far, j * chunk, chunk, normed)
        cols = pl.ds(pl.multiple_of(j * chunk, 128), chunk)
        for slot in range(2):
            acc[slot] += jnp.dot(
                normed[:, 0:chunk], proj_w[slot, cols], preferred_element_type=f32
            )

    low = lane < HD

    def turned(block, values):
        swapped = jnp.where(
            first, pltpu.roll(values, 128 - quarter, 1), pltpu.roll(values, quarter, 1)
        )
        return values * turn_cos[block] + swapped * turn_sin[block]

    def finish_pairs(block, position):
        base = pl.ds(pl.multiple_of(position * rows, rows), rows)
        for slot in range(2):
            key_value[slot, base, 0:kw] = turned(block, acc[slot, :, qw : qw + kw]).astype(bf16)
            key_value[slot, base, kw : 2 * kw] = acc[slot, :, qw + kw : qw + 2 * kw].astype(bf16)

    def finish_queries(block, slot):
        factor = HD ** (-0.5)
        for u in range(heads // 2):
            lanes = turned(block, acc[slot, :, u * 128 : (u + 1) * 128]).astype(bf16)
            lanes = lanes.astype(f32) * factor
            swapped = pltpu.roll(lanes, HD, 1)
            keep = low if u == 0 else jnp.logical_not(low)
            for at in range(2):
                aligned = lanes if at == u else swapped
                queries[block, slot, u, at * rows : (at + 1) * rows] = jnp.where(
                    keep, aligned, 0.0
                ).astype(bf16)

    def kv_at(position):
        return key_value.at[:, pl.ds(pl.multiple_of(position * rows, rows), rows)]

    def kv_pair(block, position):
        return remote(
            kv_at(position), kv_at(position), kv_send, kv_recv.at[block], pair_dev
        )

    halo_down = remote(
        kv_at(1), kv_at(tp + 1), halo_sem.at[0], halo_sem.at[1], {**left_dev, "tp": pair}
    )
    halo_up = remote(kv_at(tp), kv_at(0), halo_sem.at[0], halo_sem.at[1], {**right_dev, "tp": pair})
    sends_down = jnp.logical_and(core == 0, has_left)
    sends_up = jnp.logical_and(core == 1, has_right)

    def send_halo(mine):
        @pl.when(jnp.logical_and(mine, sends_down))
        def _():
            halo_down.start()

        @pl.when(jnp.logical_and(mine, sends_up))
        def _():
            halo_up.start()

    def wait_halo(mine):
        @pl.when(jnp.logical_and(mine, sends_down))
        def _():
            halo_up.wait_recv()

        @pl.when(jnp.logical_and(mine, sends_up))
        def _():
            halo_down.wait_recv()

    def context_part(block, slot):
        units = range(pairs)
        scores = [
            lax.dot_general(
                ctx_kv[slot, :, 0:kw],
                queries[block, slot, u],
                contract,
                preferred_element_type=f32,
            )
            for u in units
        ]
        sinks = [
            jnp.concatenate(
                [sink_v[slot, u * group + h : u * group + h + 1] for h in range(group)], axis=1
            )
            for u in units
        ]
        tops = [
            jnp.maximum(jnp.max(scores[u], axis=0, keepdims=True), sinks[u]) for u in units
        ]
        exps = [jnp.exp(scores[u] - tops[u]) for u in units]
        for u in units:
            part_top[block, slot, u] = tops[u]
            part_sum[block, slot, u] = jnp.sum(exps[u], axis=0, keepdims=True) + jnp.exp(
                sinks[u] - tops[u]
            )
            part_out[block, slot, u] = jnp.dot(
                ctx_vt[slot, u * HD : (u + 1) * HD],
                exps[u].astype(bf16),
                preferred_element_type=f32,
            )

    def window_part(block, position, slot, skip, blocks):
        units = range(pairs)
        here = pl.ds(pl.multiple_of(skip * rows, rows), blocks * rows)
        window = pl.ds(pl.multiple_of((position - 1 + skip) * rows, rows), blocks * rows)
        mask = jnp.concatenate([bias[block, here]] * group, axis=1)
        scores = [
            lax.dot_general(
                key_value[slot, window, 0:kw],
                queries[block, slot, u],
                contract,
                preferred_element_type=f32,
            )
            + mask
            for u in units
        ]
        befores = [part_top[block, slot, u] for u in units]
        tops = [
            jnp.maximum(jnp.max(scores[u], axis=0, keepdims=True), befores[u]) for u in units
        ]
        exps = [jnp.exp(scores[u] - tops[u]) for u in units]
        keeps = [jnp.exp(befores[u] - tops[u]) for u in units]
        values = jnp.transpose(key_value[slot, window, kw : 2 * kw])
        bottoms = [
            jnp.sum(exps[u], axis=0, keepdims=True) + part_sum[block, slot, u] * keeps[u]
            for u in units
        ]
        results = [
            jnp.dot(
                values[u * HD : (u + 1) * HD], exps[u].astype(bf16), preferred_element_type=f32
            )
            + part_out[block, slot, u] * keeps[u]
            for u in units
        ]
        return tops, bottoms, results

    def window_early(block, position, slot, skip, blocks):
        tops, bottoms, results = window_part(block, position, slot, skip, blocks)
        for u in range(pairs):
            part_top[block, slot, u] = tops[u]
            part_sum[block, slot, u] = bottoms[u]
            part_out[block, slot, u] = results[u]

    def store_attended(results, bottoms, slot, target):
        for u in range(pairs):
            result = results[u] / bottoms[u]
            turned_back = jnp.concatenate(
                [result[:, h * rows : (h + 1) * rows] for h in range(group)], axis=0
            )
            target[slot, :, u * 128 : (u + 1) * 128] = jnp.transpose(turned_back).astype(bf16)

    def window_last(block, position, slot, skip, blocks, target):
        _, bottoms, results = window_part(block, position, slot, skip, blocks)
        store_attended(results, bottoms, slot, target)

    def attend_whole(block, position, slot, target):
        units = range(pairs)
        window = pl.ds(pl.multiple_of((position - 1) * rows, rows), band)
        mask = jnp.concatenate([bias[block]] * group, axis=1)
        wide = [
            lax.dot_general(
                ctx_kv[slot, :, 0:kw],
                queries[block, slot, u],
                contract,
                preferred_element_type=f32,
            )
            for u in units
        ]
        near = [
            lax.dot_general(
                key_value[slot, window, 0:kw],
                queries[block, slot, u],
                contract,
                preferred_element_type=f32,
            )
            + mask
            for u in units
        ]
        values = jnp.transpose(key_value[slot, window, kw : 2 * kw])
        sinks = [
            jnp.concatenate(
                [sink_v[slot, u * group + h : u * group + h + 1] for h in range(group)], axis=1
            )
            for u in units
        ]
        tops = [
            jnp.maximum(
                jnp.maximum(
                    jnp.max(wide[u], axis=0, keepdims=True),
                    jnp.max(near[u], axis=0, keepdims=True),
                ),
                sinks[u],
            )
            for u in units
        ]
        wide = [jnp.exp(wide[u] - tops[u]) for u in units]
        near = [jnp.exp(near[u] - tops[u]) for u in units]
        bottoms = [
            jnp.sum(wide[u], axis=0, keepdims=True)
            + jnp.sum(near[u], axis=0, keepdims=True)
            + jnp.exp(sinks[u] - tops[u])
            for u in units
        ]
        results = [
            jnp.dot(
                ctx_vt[slot, u * HD : (u + 1) * HD],
                wide[u].astype(bf16),
                preferred_element_type=f32,
            )
            + jnp.dot(
                values[u * HD : (u + 1) * HD], near[u].astype(bf16), preferred_element_type=f32
            )
            for u in units
        ]
        store_attended(results, bottoms, slot, target)

    edge = jnp.zeros((2, rows, 2 * kw), bf16)

    @pl.when(jnp.logical_and(core == 0, jnp.logical_not(has_left)))
    def _():
        key_value[:, 0:rows] = edge

    @pl.when(jnp.logical_and(core == 1, jnp.logical_not(has_right)))
    def _():
        key_value[:, (tp + 1) * rows : (tp + 2) * rows] = edge

    for i in range(10, 12):
        loads[i].wait()
    pair_copies[0].wait_recv()
    pair_weights = remote(
        proj_w.at[core], proj_w.at[core], pair_send.at[1], pair_recv.at[1], pair_dev
    )
    pair_weights.wait_recv()

    def far_step(j, carry):
        lat_copy(j).wait_recv()
        project(j)
        return carry

    normalize(0, lat_own, 0, width, normed)
    for slot in range(2):
        acc[slot] = jnp.dot(normed[...], proj_w[slot], preferred_element_type=f32)
    finish_pairs(0, t + 1)
    kv_pair(0, t + 1).start()
    send_halo(chip == core)
    for slot in range(2):
        finish_queries(0, slot)
    def wo_pair(gg):
        part = wo.at[far, pl.ds(pl.multiple_of(gg * sp * shard, 16), sp * shard)]
        return remote(part, part, wop_send.at[gg], wop_recv.at[gg], pair_dev)


    def wo_last(c):
        for k in range(3, sp):
            wo_relays(k * WEIGHT_CHUNKS + c, k * WEIGHT_CHUNKS + c + 1)

    wo_relays(2 * WEIGHT_CHUNKS, 2 * WEIGHT_CHUNKS + 1)
    for slot in range(2):
        acc[slot] = jnp.zeros(acc.shape[1:], f32)
    lax.fori_loop(0 * LATENT_CHUNKS // 8, 3 * LATENT_CHUNKS // 8, far_step, 0)
    for k in range(3, sp):
        line_relay(k, ctx_at, ctxz_send, ctxz_recv)
    ctx_pair = remote(ctx_kv.at[core], ctx_kv.at[core], ctxp_sem.at[0], ctxp_sem.at[1], pair_dev)
    ctx_pair.start()
    wo_relays(2 * WEIGHT_CHUNKS + 1, 2 * WEIGHT_CHUNKS + 2)
    lax.fori_loop(3 * LATENT_CHUNKS // 8, 5 * LATENT_CHUNKS // 8, far_step, 0)
    wo_relays(2 * WEIGHT_CHUNKS + 2, 2 * WEIGHT_CHUNKS + 3)
    ctx_pair.wait_recv()
    for slot in range(2):
        ctx_vt[slot] = jnp.transpose(ctx_kv[slot, :, kw : 2 * kw])
    context_part(0, 0)
    kv_pair(0, pair + 1).wait_recv()
    window_early(0, t + 1, 0, 1 - core, 2)
    wo_relays(2 * WEIGHT_CHUNKS + 3, 3 * WEIGHT_CHUNKS)
    context_part(0, 1)
    window_early(0, t + 1, 1, 1 - core, 2)
    start_held(1)
    wo_last(0)
    wo_share(s)
    wo_shares(1)
    lax.fori_loop(5 * LATENT_CHUNKS // 8, 6 * LATENT_CHUNKS // 8, far_step, 0)
    wo_last(1)
    lax.fori_loop(6 * LATENT_CHUNKS // 8, 7 * LATENT_CHUNKS // 8, far_step, 0)
    wo_last(2)
    lax.fori_loop(7 * LATENT_CHUNKS // 8, LATENT_CHUNKS, far_step, 0)
    finish_pairs(1, far + 1)
    kv_pair(1, far + 1).start()
    send_halo(chip != core)
    for c in range(3, WEIGHT_CHUNKS):
        wo_last(c)
    finish_queries(1, 0)

    context_part(1, 0)
    finish_queries(1, 1)

    def att_copy(slot):
        return remote(
            att_out.at[slot], att.at[chip, slot], att_send, att_recv.at[slot], far_dev
        )

    kv_pair(1, pair + 1).wait_recv()
    wait_halo(chip != core)
    window_last(1, far + 1, 0, 0, 3, att_out)
    att_copy(0).start()
    attend_whole(1, far + 1, 1, att_out)
    att_copy(1).start()
    wo_shares(2)
    wait_halo(chip == core)
    for slot in range(2):
        window_last(0, t + 1, slot, 2 * core, 1, att.at[chip])
    for k in range(3, sp):
        wo_shares(k)
    pair_copies[4].wait_recv()
    other = (1 - chip) * 2 + 1 - core
    order = (t, pair, far, other)

    def product(x, slot, i):
        part = pl.ds(pl.multiple_of((2 * x + slot) * qw, qw), qw)
        return jnp.dot(att[x, slot], wo[i, part], preferred_element_type=f32)

    def out_own(k):
        out_part[k] = product(chip, 0, order[k]) + product(chip, 1, order[k])

    def out_first(k):
        out_part[k] += product(1 - chip, 0, order[k])

    def out_last(k):
        cols = pl.ds(pl.multiple_of(order[k] * out_width, 128), out_width)
        sums = out_part[k] + product(1 - chip, 1, order[k])
        blended = sums.astype(bf16).astype(f32)
        mixed[:, cols] = (lat_own[:, cols].astype(f32) + gate_v[:, cols] * blended).astype(bf16)

    out_own(0)
    out_own(1)
    out_own(2)
    att_copy(0).wait_recv()
    for k in range(3):
        out_first(k)
    for gg in range(2):
        part = wo.at[other, pl.ds(gg * sp * shard, sp * shard)]
        remote(part, part, wop_send.at[gg], wop_recv.at[gg], pair_dev).wait_recv()
    out_part[3] = (
        product(chip, 0, other) + product(chip, 1, other) + product(1 - chip, 0, other)
    )
    att_copy(1).wait_recv()
    for k in range(4):
        out_last(k)

    stat_copy.wait_send()
    remote(wo_shard, wo_shard, wox_send, wo_recv.at[0, 0], far_dev).wait_send()
    remote(lat_own, lat_far, lat_send, lat_recv.at[0], far_dev).wait_send()
    pair_copies[0].wait_send()
    pair_weights.wait_send()
    pair_copies[4].wait_send()
    mods.wait_send()
    line_finish(lambda count: mod_part.at[0:count], modz_send)
    line_finish(lambda count: ctx_kv.at[core, 0 : count * ctx_rows], ctxz_send)
    ctx_pair.wait_send()
    def wo_total(count):
        return wo.at[far, 0 : count * shard]

    line_finish(wo_total, wo_send)
    wo_sent = wo.at[far, pl.ds(pl.multiple_of(g * sp * shard, 16), sp * shard)]
    remote(wo_sent, wo_sent, woy_send, woy_recv.at[0, 0], y_dev).wait_send()
    wo_pair(0).wait_send()
    wo_pair(1).wait_send()
    both = key_value.at[:, 0 : 2 * rows]
    remote(both, both, kv_send, kv_recv.at[0], pair_dev).wait_send()

    @pl.when(sends_down)
    def _():
        halo_down.wait_send()

    @pl.when(sends_up)
    def _():
        halo_up.wait_send()

    remote(att_out, att_out, att_send, att_recv.at[0], far_dev).wait_send()


def local(
    latent,
    context,
    conditioning,
    norm_gain,
    shift_weight,
    scale_weight,
    gate_weight,
    query_weight,
    key_weight,
    value_weight,
    out_weight,
    sink_logit,
):
    tp, sp, grp = lax.axis_size("tp"), lax.axis_size("sp"), lax.axis_size("grp")
    rows, width = latent.shape
    ctx_rows = context.shape[0]
    mod_rows, mod_cols = shift_weight.shape
    query_width, key_width = query_weight.shape[1], key_weight.shape[1]
    out_rows, out_width = out_weight.shape
    fits = (
        rows == WIN
        and rows == 128
        and key_width == 2 * HD
        and query_width == 4 * HD
        and tp == 4
        and grp == 2
        and sp >= 3
        and sp * ctx_rows % 128 == 0
        and ctx_rows % CONTEXT_ROWS == 0
        and width % 512 == 0
        and mod_cols % 128 == 0
        and width % (128 * LATENT_CHUNKS) == 0
        and out_width % 128 == 0
        and tp * out_width == width
        and out_rows == tp * query_width
        and out_rows % (2 * sp * WEIGHT_CHUNKS * 16) == 0
    )
    if not fits:
        return local_plain(
            latent,
            context,
            conditioning,
            norm_gain,
            shift_weight,
            scale_weight,
            gate_weight,
            query_weight,
            key_weight,
            value_weight,
            out_weight,
            sink_logit,
        )
    f32, bf16 = jnp.float32, jnp.bfloat16
    dma = pltpu.SemaphoreType.DMA
    anywhere = pl.BlockSpec(memory_space=pl.ANY)
    return pl.pallas_call(
        functools.partial(fused_kernel, sp),
        out_shape=pltpu.VMEM((rows, width), bf16),
        in_specs=[anywhere] * 11 + [pl.BlockSpec(memory_space=pltpu.SMEM)],
        out_specs=pl.BlockSpec(memory_space=pltpu.VMEM),
        scratch_shapes=[
            pltpu.VMEM((mod_rows,), bf16),
            pltpu.VMEM((1, width), f32),
            pltpu.VMEM((3, mod_rows, mod_cols), bf16),
            pltpu.VMEM((2, width, query_width + 2 * key_width), bf16),
            pltpu.VMEM((tp, out_rows, out_width), bf16),
            pltpu.VMEM((out_rows // (2 * sp), out_width), bf16),
            pltpu.VMEM(context.shape, bf16),
            pltpu.VMEM((rows, width), bf16),
            pltpu.VMEM((rows, width), bf16),
            pltpu.VMEM((rows, width), bf16),
            pltpu.VMEM((8, 128), f32),
            pltpu.VMEM((8, 128), f32),
            pltpu.VMEM((2, rows, 128), f32),
            pltpu.VMEM((2, 8, 128), f32),
            pltpu.VMEM((sp, 1, 3 * mod_cols), f32),
            pltpu.VMEM((tp, 1, 3 * mod_cols), f32),
            pltpu.VMEM((1, width), f32),
            pltpu.VMEM((1, width), f32),
            pltpu.VMEM((1, width), f32),
            pltpu.VMEM((2, rows, 128), f32),
            pltpu.VMEM((2, rows, 128), f32),
            pltpu.VMEM((2, rows, query_width + 2 * key_width), f32),
            pltpu.VMEM((2, 2, 2, 2 * rows, key_width), bf16),
            pltpu.VMEM((2, (tp + 2) * rows, 2 * key_width), bf16),
            pltpu.VMEM((2, sp * ctx_rows, 2 * key_width), bf16),
            pltpu.VMEM((2, 2, rows, query_width), bf16),
            pltpu.VMEM((2, rows, query_width), bf16),
            pltpu.VMEM((2, key_width, sp * ctx_rows), bf16),
            pltpu.VMEM((2, 3 * rows, rows), f32),
            pltpu.VMEM((2, 2, 2, HD, 2 * rows), f32),
            pltpu.VMEM((2, 2, 2, 1, 2 * rows), f32),
            pltpu.VMEM((2, 2, 2, 1, 2 * rows), f32),
            pltpu.VMEM((tp, rows, out_width), f32),
            dma((9,)),
            dma,
            dma((LATENT_CHUNKS,)),
            dma((2,)),
            dma((3,)),
            dma((3,)),
            dma,
            dma((2,)),
            dma((sp, WEIGHT_CHUNKS)),
            dma,
            dma((sp, 2)),
            dma((2,)),
            dma((2,)),
            dma((2,)),
            dma((sp,)),
            dma,
            dma,
            dma((2,)),
            dma((sp,)),
            dma((2,)),
            dma,
            dma((2,)),
            dma((2,)),
            dma,
            dma((2,)),
        ],
        compiler_params=pltpu.CompilerParams(
            collective_id=0,
            has_side_effects=True,
            vmem_limit_bytes=60 * 1024 * 1024,
        ),
        name="fused",
    )(
        latent,
        context,
        conditioning,
        norm_gain.reshape(1, width),
        shift_weight,
        scale_weight,
        gate_weight,
        query_weight,
        key_weight,
        value_weight,
        out_weight,
        sink_logit,
    )


def solution(mesh):
    in_specs = (
        P(("grp", "sp", "tp"), None),
        P(("grp", "sp"), None),
        P(("grp", "sp")),
        P(),
        P("sp", "tp"),
        P("sp", "tp"),
        P("sp", "tp"),
        P(None, "tp"),
        P(None, "tp"),
        P(None, "tp"),
        P(None, "tp"),
        P("tp"),
    )
    out_specs = P(("grp", "sp", "tp"), None)
    return jax.shard_map(local, mesh=mesh, in_specs=in_specs, out_specs=out_specs, check_vma=False)
```

```python
import functools

import jax
import jax.numpy as jnp
from jax import lax
from jax.experimental import pallas as pl
from jax.experimental.pallas import tpu as pltpu
from jax.sharding import PartitionSpec as P

HEADS = 16
KV_HEADS = 8
HD = 64
GRID_W = 64
WIN = 128


epsilon = 1e-06
rope_base = 10000.0
neg_large = -1e30


def with_halo(cells, sides, width):
    for axis, dim in sides:
        count = lax.axis_size(axis)
        ends = count - 1
        head = lax.slice_in_dim(cells, 0, width, axis=dim)
        tail = lax.slice_in_dim(cells, cells.shape[dim] - width, cells.shape[dim], axis=dim)
        cells = jnp.concatenate(
            [
                lax.ppermute(tail, axis, [(i, (i + 1) % count) for i in range(ends)]),
                cells,
                lax.ppermute(head, axis, [((i + 1) % count, i) for i in range(ends)]),
            ],
            axis=dim,
        )
    return cells


def row_norm(matrix, norm_gain):
    values = matrix.astype(jnp.float32)
    return (
        values * lax.rsqrt(jnp.mean(values * values, axis=-1, keepdims=True) + epsilon) * norm_gain
    )


def axial_turn(values, position):
    half_dim = values.shape[-1] // 2
    quarter = half_dim // 2
    inverse = rope_base ** (-jnp.arange(quarter, dtype=jnp.float32) / quarter)

    def turn(section, coordinate):
        angles = coordinate.astype(jnp.float32)[:, None] * inverse[None, :]
        cosine = jnp.cos(angles)[:, None, :]
        sine_part = jnp.sin(angles)[:, None, :]
        leading = section[..., :quarter]
        trailing = section[..., quarter:]
        return jnp.concatenate(
            [leading * cosine - trailing * sine_part, leading * sine_part + trailing * cosine],
            axis=-1,
        )

    return jnp.concatenate(
        [
            turn(values[..., :half_dim], position // GRID_W),
            turn(values[..., half_dim:], position % GRID_W),
        ],
        axis=-1,
    )


def context_pairs(context_rows, norm_gain, key_weight, value_weight):
    prepared = row_norm(context_rows, norm_gain).astype(jnp.bfloat16)
    return jnp.concatenate(
        [
            jnp.dot(prepared, key_weight, preferred_element_type=jnp.float32),
            jnp.dot(prepared, value_weight, preferred_element_type=jnp.float32),
        ],
        axis=1,
    ).astype(jnp.bfloat16)


def local_plain(
    latent,
    context,
    conditioning,
    norm_gain,
    shift_weight,
    scale_weight,
    gate_weight,
    query_weight,
    key_weight,
    value_weight,
    out_weight,
    sink_logit,
):
    lifted = jax.nn.silu(conditioning.astype(jnp.float32)).astype(jnp.bfloat16)[None, :]
    shift_part = jnp.dot(lifted, shift_weight, preferred_element_type=jnp.float32)[0]
    scale_part = jnp.dot(lifted, scale_weight, preferred_element_type=jnp.float32)[0]
    gate_part = jnp.dot(lifted, gate_weight, preferred_element_type=jnp.float32)[0]
    summed = lax.psum((shift_part, scale_part, gate_part), "sp")
    shift_vec, scale_vec, gate_vec = (
        lax.all_gather(summed[0], "tp", axis=0, tiled=True),
        lax.all_gather(summed[1], "tp", axis=0, tiled=True),
        lax.all_gather(summed[2], "tp", axis=0, tiled=True),
    )
    normed = (row_norm(latent, norm_gain) * (1.0 + scale_vec) + shift_vec).astype(jnp.bfloat16)
    segment = lax.all_gather(normed, "tp", axis=0, tiled=True)
    projected = jnp.concatenate(
        [
            jnp.dot(segment, query_weight, preferred_element_type=jnp.float32),
            jnp.dot(segment, key_weight, preferred_element_type=jnp.float32),
            jnp.dot(segment, value_weight, preferred_element_type=jnp.float32),
        ],
        axis=1,
    )
    row_count = projected.shape[0]
    query_width = query_weight.shape[1]
    key_width = key_weight.shape[1]
    query_heads = query_width // HD
    pair_heads = key_width // HD
    group_size = HEADS // KV_HEADS
    row_offset = lax.axis_index("sp") * row_count
    position = row_offset + jnp.arange(row_count, dtype=jnp.int32)
    queries = axial_turn(
        projected[:, :query_width].reshape(row_count, query_heads, HD), position
    ).astype(jnp.bfloat16)
    latent_keys = axial_turn(
        projected[:, query_width : query_width + key_width].reshape(row_count, pair_heads, HD),
        position,
    ).astype(jnp.bfloat16)
    latent_values = projected[:, query_width + key_width :].astype(jnp.bfloat16)
    key_value = jnp.concatenate([latent_keys.reshape(row_count, key_width), latent_values], axis=1)
    widened = with_halo(key_value, (("sp", 0),), WIN)
    context_all = lax.all_gather(
        context_pairs(context, norm_gain, key_weight, value_weight), "sp", axis=0, tiled=True
    )
    block_count = row_count // WIN
    context_count = context_all.shape[0]
    query_blocks = queries.reshape(block_count, WIN, pair_heads, group_size, HD)
    band_blocks = widened.reshape(block_count + 2, WIN, 2 * key_width)
    band_rows = jnp.concatenate(
        [band_blocks[:block_count], band_blocks[1 : block_count + 1], band_blocks[2:]], axis=1
    )
    band_keys = band_rows[..., :key_width].reshape(block_count, 3 * WIN, pair_heads, HD)
    band_values = band_rows[..., key_width:].reshape(block_count, 3 * WIN, pair_heads, HD)
    context_keys = context_all[:, :key_width].reshape(context_count, pair_heads, HD)
    context_values = context_all[:, key_width:].reshape(context_count, pair_heads, HD)
    factor = HD ** (-0.5)
    local_scores = (
        jnp.einsum("nqhgd,nkhd->nhgqk", query_blocks, band_keys, preferred_element_type=jnp.float32)
        * factor
    )
    query_pos = position.reshape(block_count, WIN)
    key_pos = (
        row_offset
        - WIN
        + jnp.arange(block_count, dtype=jnp.int32)[:, None] * WIN
        + jnp.arange(3 * WIN, dtype=jnp.int32)[None, :]
    )
    seq_total = row_count * lax.axis_size("sp")
    allowed = (
        (jnp.abs(key_pos[:, None, :] - query_pos[:, :, None]) <= WIN)
        & (key_pos[:, None, :] >= 0)
        & (key_pos[:, None, :] < seq_total)
    )
    local_scores = jnp.where(allowed[:, None, None], local_scores, neg_large)
    context_scores = (
        jnp.einsum(
            "nqhgd,thd->nhgqt", query_blocks, context_keys, preferred_element_type=jnp.float32
        )
        * factor
    )
    sink_values = sink_logit.reshape(pair_heads, group_size)[None, :, :, None, None]
    highest = jnp.maximum(
        jnp.maximum(
            jnp.max(local_scores, axis=-1, keepdims=True),
            jnp.max(context_scores, axis=-1, keepdims=True),
        ),
        sink_values,
    )
    local_exp = jnp.exp(local_scores - highest)
    context_exp = jnp.exp(context_scores - highest)
    denominator = (
        jnp.sum(local_exp, axis=-1, keepdims=True)
        + jnp.sum(context_exp, axis=-1, keepdims=True)
        + jnp.exp(sink_values - highest)
    )
    local_weights = (local_exp / denominator).astype(jnp.bfloat16)
    context_weights = (context_exp / denominator).astype(jnp.bfloat16)
    attended = jnp.einsum(
        "nhgqk,nkhd->nqhgd", local_weights, band_values, preferred_element_type=jnp.float32
    ) + jnp.einsum(
        "nhgqt,thd->nqhgd", context_weights, context_values, preferred_element_type=jnp.float32
    )
    attended = attended.reshape(row_count, query_width).astype(jnp.bfloat16)
    columns_part = jnp.dot(
        lax.all_gather(attended, "tp", axis=1, tiled=True),
        out_weight,
        preferred_element_type=jnp.float32,
    ).astype(jnp.bfloat16)
    blended = lax.all_to_all(columns_part, "tp", split_axis=0, concat_axis=1, tiled=True)
    return (latent.astype(jnp.float32) + gate_vec * blended.astype(jnp.float32)).astype(
        jnp.bfloat16
    )


LATENT_CHUNKS = 8
WEIGHT_CHUNKS = 4
HELD = 1
AHEAD = 3 * LATENT_CHUNKS // 8
NORM_ROWS = 16
CONTEXT_ROWS = 32


def remote(src, dst, send, recv, device):
    return pltpu.make_async_remote_copy(
        src_ref=src,
        dst_ref=dst,
        send_sem=send,
        recv_sem=recv,
        device_id=device,
        device_id_type=pl.DeviceIdType.MESH,
    )


def fused_kernel(
    sp,
    latent,
    context,
    conditioning,
    norm_gain,
    shift_weight,
    scale_weight,
    gate_weight,
    query_weight,
    key_weight,
    value_weight,
    out_weight,
    sink,
    mixed,
    cond_v,
    gain_v,
    mod_w,
    proj_w,
    wo,
    wo_shard,
    ctx_v,
    lat_own,
    lat_far,
    normed,
    stat_out,
    stat_in,
    row_scale,
    sink_v,
    mod_part,
    mod_all,
    factor_v,
    shift_v,
    gate_v,
    turn_cos,
    turn_sin,
    acc,
    queries,
    key_value,
    ctx_kv,
    att,
    att_out,
    ctx_vt,
    bias,
    part_out,
    part_top,
    part_sum,
    out_part,
    load_sem,
    lat_send,
    lat_recv,
    stat_sem,
    pair_send,
    pair_recv,
    wox_send,
    wo_send,
    wo_recv,
    woy_send,
    woy_recv,
    wop_send,
    wop_recv,
    modz_send,
    modz_recv,
    modt_send,
    modt_recv,
    ctxz_send,
    ctxz_recv,
    ctxp_sem,
    kv_send,
    kv_recv,
    halo_sem,
    att_send,
    att_recv,
):
    g = lax.axis_index("grp")
    s = lax.axis_index("sp")
    t = lax.axis_index("tp")
    chip = t // 2
    core = lax.rem(t, 2)
    pair = chip * 2 + 1 - core
    far = (1 - chip) * 2 + core
    pair_dev, far_dev, y_dev = {"tp": pair}, {"tp": far}, {"grp": 1 - g}
    right_dev = {"sp": lax.rem(s + 1, sp)}
    left_dev = {"sp": lax.rem(s + sp - 1, sp)}
    has_right, has_left = s < sp - 1, s > 0
    rows, width = latent.shape
    ctx_rows = context.shape[0]
    mod_cols = shift_weight.shape[1]
    qw = query_weight.shape[1]
    kw = key_weight.shape[1]
    heads = qw // HD
    group = heads // (kw // HD)
    tp = 4
    total = tp * rows
    out_rows, out_width = out_weight.shape
    half = rows // 2
    f32, bf16 = jnp.float32, jnp.bfloat16
    chunk = width // LATENT_CHUNKS
    shard = out_rows // (2 * sp)
    slab = shard // WEIGHT_CHUNKS
    MESH = pl.DeviceIdType.MESH

    loads = [
        (out_weight.at[pl.ds(pl.multiple_of((g * sp + s) * shard, 16), shard)], wo_shard),
        (latent, lat_own),
        (norm_gain, gain_v),
        (context, ctx_v),
        (key_weight, proj_w.at[core, :, qw : qw + kw]),
        (value_weight, proj_w.at[core, :, qw + kw : qw + 2 * kw]),
        (conditioning, cond_v),
        (shift_weight, mod_w.at[0]),
        (scale_weight, mod_w.at[1]),
        (gate_weight, mod_w.at[2]),
        (query_weight, proj_w.at[core, :, 0:qw]),
        (out_weight, wo.at[t]),
    ]
    slots = (0, 1, 2, 3, 4, 4, 5, 6, 6, 6, 7, 8)
    loads = [
        pltpu.make_async_copy(a, b, load_sem.at[i]) for i, (a, b) in zip(slots, loads, strict=True)
    ]
    for load in loads:
        load.start()

    barrier = pltpu.get_barrier_semaphore()
    for k in range(1, tp):
        pl.semaphore_signal(
            barrier, inc=1, device_id={"tp": lax.rem(t + k, tp)}, device_id_type=MESH
        )
    pl.semaphore_signal(barrier, inc=1, device_id=y_dev, device_id_type=MESH)
    for has, place in ((has_right, right_dev), (has_left, left_dev)):

        @pl.when(has)
        def _():
            for peer in (t, pair):
                pl.semaphore_signal(
                    barrier, inc=1, device_id={**place, "tp": peer}, device_id_type=MESH
                )

    def row_factor(source, part):
        squares = None
        for at in range(0, width, 512):
            values = source[part, at : at + 512].astype(f32)
            values = values * values
            squares = values if squares is None else squares + values
        return lax.rsqrt(jnp.sum(squares, axis=-1, keepdims=True) * (1.0 / width) + epsilon)

    lane = lax.broadcasted_iota(jnp.int32, (rows, 128), 1)
    row = lax.broadcasted_iota(jnp.int32, (rows, 128), 0)
    diagonal = lane == row

    pl.semaphore_wait(
        barrier, tp + jnp.where(has_right, 2, 0) + jnp.where(has_left, 2, 0)
    )

    def lat_copy(j):
        cols = pl.ds(pl.multiple_of(j * chunk, 128), chunk)
        return remote(
            lat_own.at[:, cols], lat_far.at[:, cols], lat_send, lat_recv.at[j], far_dev
        )

    def wo_rows(gg, j, c):
        return pl.ds(pl.multiple_of((gg * sp + j) * shard + c * slab, 16), slab)

    def wo_cross(c):
        part = wo_rows(g, s, c)
        return remote(
            wo_shard.at[pl.ds(c * slab, slab)],
            wo.at[t, part],
            wox_send,
            wo_recv.at[s, c],
            far_dev,
        )

    loads[0].wait()
    for c in range(WEIGHT_CHUNKS):
        wo_cross(c).start()
    loads[1].wait()

    def row_stat(i, carry):
        part = pl.ds(pl.multiple_of(i * CONTEXT_ROWS, 16), CONTEXT_ROWS)
        row_scale[0, part] = jnp.broadcast_to(row_factor(lat_own, part), (CONTEXT_ROWS, 128))
        return carry

    lax.fori_loop(0, rows // CONTEXT_ROWS, row_stat, 0)
    flat = jnp.sum(jnp.where(diagonal, row_scale[0], 0.0), axis=0, keepdims=True)
    stat_out[...] = jnp.broadcast_to(flat, (8, 128))
    sink_row = lax.broadcasted_iota(jnp.int32, (8, 128), 0)
    sink_all = jnp.full((8, 128), sink[0], f32)
    for h in range(1, heads):
        sink_all = jnp.where(sink_row == h, sink[h], sink_all)
    sink_v[core] = sink_all

    stat_copy = remote(stat_out, stat_in, stat_sem.at[0], stat_sem.at[1], far_dev)
    stat_copy.start()
    for j in range(LATENT_CHUNKS // 4):
        lat_copy(j).start()
    pair_copies = [
        (sink_v.at[core], sink_v.at[core]),
        (query_weight, proj_w.at[core, :, 0:qw]),
        (key_weight, proj_w.at[core, :, qw : qw + kw]),
        (value_weight, proj_w.at[core, :, qw + kw : qw + 2 * kw]),
        (out_weight, wo.at[t]),
    ]
    pair_copies = [
        remote(a, b, pair_send.at[i], pair_recv.at[i], pair_dev)
        for i, (a, b) in zip((0, 1, 1, 1, 2), pair_copies, strict=True)
    ]
    pair_copies[0].start()

    def line_copy(at, j, send, recv, toward):
        return remote(at(j), at(j), send.at[toward], recv.at[j], (left_dev, right_dev)[toward])

    def line_start(at, send, recv):
        for toward, has in ((0, has_left), (1, has_right)):

            @pl.when(has)
            def _():
                line_copy(at, s, send, recv, toward).start()

    def line_relay(k, at, send, recv):
        for toward, has, j, there in (
            (1, has_right, s - k, s >= k),
            (0, has_left, s + k, s + k < sp),
        ):

            @pl.when(there)
            def _():
                line_copy(at, j, send, recv, toward).wait_recv()

                @pl.when(has)
                def _():
                    line_copy(at, j, send, recv, toward).start()

    def line_finish(total_of, send):
        for toward, has, sent in ((1, has_right, s + 1), (0, has_left, sp - s)):
            for count in range(1, sp + 1):

                @pl.when(jnp.logical_and(has, sent == count))
                def _():
                    part = total_of(count)
                    remote(part, part, send.at[toward], stat_sem.at[1], right_dev).wait_send()

    def mod_at(j):
        return mod_part.at[j]

    def ctx_at(j):
        return ctx_kv.at[core, pl.ds(pl.multiple_of(j * ctx_rows, 16), ctx_rows)]

    loads[2].wait()
    loads[3].wait()
    kv_weights = proj_w.at[core, :, qw : qw + 2 * kw]
    pltpu.make_async_copy(kv_weights, kv_weights, load_sem.at[4]).wait()

    def norm_context(i, carry):
        part = pl.ds(pl.multiple_of(i * CONTEXT_ROWS, 16), CONTEXT_ROWS)
        scale = row_factor(ctx_v, part)
        for at in range(0, width, 512):
            here = slice(at, at + 512)
            values = ctx_v[part, here].astype(f32)
            ctx_v[part, here] = (values * scale * gain_v[:, here]).astype(bf16)
        return carry

    lax.fori_loop(0, ctx_rows // CONTEXT_ROWS, norm_context, 0)
    own_ctx = pl.ds(pl.multiple_of(s * ctx_rows, 16), ctx_rows)
    ctx_kv[core, own_ctx] = jnp.dot(
        ctx_v[...], proj_w[core, :, qw : qw + 2 * kw], preferred_element_type=f32
    ).astype(bf16)
    line_start(ctx_at, ctxz_send, ctxz_recv)
    loads[6].wait()
    pltpu.make_async_copy(mod_w, mod_w, load_sem.at[6]).wait()
    cond = cond_v[...].astype(f32).reshape(1, cond_v.shape[0])
    lifted = jnp.broadcast_to(cond / (1.0 + jnp.exp(-cond)), (16, cond.shape[1])).astype(bf16)
    for i in range(3):
        mod_part[s, :, i * mod_cols : (i + 1) * mod_cols] = jnp.dot(
            lifted, mod_w[i], preferred_element_type=f32
        )[0:1]
    line_start(mod_at, modz_send, modz_recv)
    for copy in pair_copies[1:4]:
        copy.start()

    def wo_line(j, c, toward):
        part = wo.at[far, wo_rows(g, j, c)]
        return remote(
            part, part, wo_send.at[toward], wo_recv.at[j, c], (left_dev, right_dev)[toward]
        )

    def wo_across(j, c):
        part = wo.at[far, wo_rows(g, j, c)]
        return remote(part, part, woy_send, woy_recv.at[j, c // (WEIGHT_CHUNKS - 1)], y_dev)

    def wo_pass(j, c):
        part = wo.at[far, wo_rows(g, j, c)]
        remote(part, part, wop_send.at[g], wop_recv.at[g], pair_dev).start()

    def wo_share(j):
        begin = ((1 - g) * sp + j) * shard
        for n, (low_row, size) in enumerate(((0, shard - slab), (shard - slab, slab))):
            part = wo.at[far, pl.ds(pl.multiple_of(begin + low_row, 16), size)]
            remote(part, part, woy_send, woy_recv.at[j, n], y_dev).wait_recv()
            remote(part, part, wop_send.at[1 - g], wop_recv.at[1 - g], pair_dev).start()

    def wo_shares(k):
        for j, there in ((s - k, s >= k), (s + k, s + k < sp)):

            @pl.when(there)
            def _():
                wo_share(j)

    def wo_own(c):
        wo_line(s, c, 0).wait_recv()
        wo_across(s, c).start()
        wo_pass(s, c)

    def wo_own_line(c):
        for toward, has in ((0, has_left), (1, has_right)):

            @pl.when(has)
            def _():
                wo_line(s, c, toward).start()

    def wo_relay(e):
        k, c = e // WEIGHT_CHUNKS, lax.rem(e, WEIGHT_CHUNKS)
        for toward, has, j, there in (
            (1, has_right, s - k, s >= k),
            (0, has_left, s + k, s + k < sp),
        ):

            @pl.when(there)
            def _():
                wo_line(j, c, toward).wait_recv()

                @pl.when(has)
                def _():
                    wo_line(j, c, toward).start()

                wo_across(j, c).start()
                wo_pass(j, c)

    def wo_relays(low, high):
        def step(e, carry):
            wo_relay(e)
            return carry

        lax.fori_loop(low, high, step, 0)

    quarter = HD // 4
    inverse = jnp.exp(
        lax.rem(lane, quarter).astype(f32) * (-jnp.log(jnp.float32(rope_base)) / quarter)
    )
    first = lax.rem(lane, 2 * quarter) < quarter
    by_row = lax.rem(lane, HD) < HD // 2

    def tables(b, carry):
        place = s * total + jnp.where(b == 0, t, far) * rows + row
        coordinate = jnp.where(by_row, place // GRID_W, lax.rem(place, GRID_W))
        angles = coordinate.astype(f32) * inverse
        turn_cos[b] = jnp.cos(angles)
        sines = jnp.sin(angles)
        turn_sin[b] = jnp.where(first, -sines, sines)
        return carry

    contract = (((1,), (1,)), ((), ()))
    band = 3 * rows
    pairs = kw // HD
    stack = group * rows

    def biases(block, carry):
        q_pos = lax.broadcasted_iota(jnp.int32, (band, rows), 1)
        k_pos = lax.broadcasted_iota(jnp.int32, (band, rows), 0)
        place = s * total + jnp.where(block == 0, t, far) * rows - WIN + k_pos
        allowed = jnp.logical_and(
            jnp.logical_and(k_pos >= q_pos, k_pos <= q_pos + 2 * WIN),
            jnp.logical_and(place >= 0, place < sp * total),
        )
        bias[block] = jnp.where(allowed, 0.0, neg_large)
        return carry

    for c in range(2):
        wo_own(c)
        wo_own_line(c)
    line_relay(1, mod_at, modz_send, modz_recv)
    line_relay(1, ctx_at, ctxz_send, ctxz_recv)
    wo_own(2)
    wo_own_line(2)
    lax.fori_loop(0, 2, tables, 0)
    lax.fori_loop(0, 2, biases, 0)
    line_relay(2, mod_at, modz_send, modz_recv)
    for j in range(LATENT_CHUNKS // 4, AHEAD):
        lat_copy(j).start()
    for c in range(3, WEIGHT_CHUNKS):
        wo_own(c)
        wo_own_line(c)
    wo_relays(WEIGHT_CHUNKS, WEIGHT_CHUNKS + 1)
    pair_copies[4].start()
    line_relay(2, ctx_at, ctxz_send, ctxz_recv)
    for k in range(3, sp):
        line_relay(k, mod_at, modz_send, modz_recv)
    summed = mod_part[0]
    for k in range(1, sp):
        summed = summed + mod_part[k]
    mod_all[t] = summed
    for k in range(1, tp):
        remote(
            mod_all.at[t], mod_all.at[t], modt_send, modt_recv, {"tp": lax.rem(t + k, tp)}
        ).start()
    mods = remote(
        mod_all.at[0 : tp - 1], mod_all.at[0 : tp - 1], modt_send, modt_recv, pair_dev
    )
    for j in range(AHEAD, LATENT_CHUNKS - HELD):
        lat_copy(j).start()

    def start_held(who):
        @pl.when(core == who)
        def _():
            for j in range(LATENT_CHUNKS - HELD, LATENT_CHUNKS):
                lat_copy(j).start()

    start_held(0)
    wo_relays(WEIGHT_CHUNKS + 1, 2 * WEIGHT_CHUNKS)
    stat_copy.wait_recv()
    column = jnp.sum(
        jnp.where(diagonal, jnp.broadcast_to(stat_in[0:1], (rows, 128)), 0.0), axis=1, keepdims=True
    )
    row_scale[1] = jnp.broadcast_to(column, (rows, 128))

    mods.wait_recv()
    for i in range(tp):
        cols = slice(i * mod_cols, (i + 1) * mod_cols)
        shift_v[:, cols] = mod_all[i, :, 0:mod_cols]
        factor_v[:, cols] = gain_v[:, cols] * (1.0 + mod_all[i, :, mod_cols : 2 * mod_cols])
        gate_v[:, cols] = mod_all[i, :, 2 * mod_cols : 3 * mod_cols]

    def normalize(block, source, cols, lanes, target):
        scale = row_scale[block]
        for at in range(0, lanes, 128):
            here = pl.ds(pl.multiple_of(cols + at, 128), 128)
            values = source[:, here].astype(f32) * scale
            target[:, at : at + 128] = (values * factor_v[:, here] + shift_v[:, here]).astype(bf16)

    def project(j):
        normalize(1, lat_far, j * chunk, chunk, normed)
        cols = pl.ds(pl.multiple_of(j * chunk, 128), chunk)
        for slot in range(2):
            acc[slot] += jnp.dot(
                normed[:, 0:chunk], proj_w[slot, cols], preferred_element_type=f32
            )

    low = lane < HD

    def turned(block, values):
        swapped = jnp.where(
            first, pltpu.roll(values, 128 - quarter, 1), pltpu.roll(values, quarter, 1)
        )
        return values * turn_cos[block] + swapped * turn_sin[block]

    def finish_pairs(block, position):
        base = pl.ds(pl.multiple_of(position * rows, rows), rows)
        for slot in range(2):
            key_value[slot, base, 0:kw] = turned(block, acc[slot, :, qw : qw + kw]).astype(bf16)
            key_value[slot, base, kw : 2 * kw] = acc[slot, :, qw + kw : qw + 2 * kw].astype(bf16)

    def finish_queries(block, slot):
        factor = HD ** (-0.5)
        for u in range(heads // 2):
            lanes = turned(block, acc[slot, :, u * 128 : (u + 1) * 128]).astype(bf16)
            lanes = lanes.astype(f32) * factor
            swapped = pltpu.roll(lanes, HD, 1)
            keep = low if u == 0 else jnp.logical_not(low)
            for at in range(2):
                aligned = lanes if at == u else swapped
                queries[block, slot, u, at * rows : (at + 1) * rows] = jnp.where(
                    keep, aligned, 0.0
                ).astype(bf16)

    def kv_at(position):
        return key_value.at[:, pl.ds(pl.multiple_of(position * rows, rows), rows)]

    def kv_pair(block, position):
        return remote(
            kv_at(position), kv_at(position), kv_send, kv_recv.at[block], pair_dev
        )

    halo_down = remote(
        kv_at(1), kv_at(tp + 1), halo_sem.at[0], halo_sem.at[1], {**left_dev, "tp": pair}
    )
    halo_up = remote(kv_at(tp), kv_at(0), halo_sem.at[0], halo_sem.at[1], {**right_dev, "tp": pair})
    sends_down = jnp.logical_and(core == 0, has_left)
    sends_up = jnp.logical_and(core == 1, has_right)

    def send_halo(mine):
        @pl.when(jnp.logical_and(mine, sends_down))
        def _():
            halo_down.start()

        @pl.when(jnp.logical_and(mine, sends_up))
        def _():
            halo_up.start()

    def wait_halo(mine):
        @pl.when(jnp.logical_and(mine, sends_down))
        def _():
            halo_up.wait_recv()

        @pl.when(jnp.logical_and(mine, sends_up))
        def _():
            halo_down.wait_recv()

    def context_part(block, slot):
        units = range(pairs)
        scores = [
            lax.dot_general(
                ctx_kv[slot, :, 0:kw],
                queries[block, slot, u],
                contract,
                preferred_element_type=f32,
            )
            for u in units
        ]
        sinks = [
            jnp.concatenate(
                [sink_v[slot, u * group + h : u * group + h + 1] for h in range(group)], axis=1
            )
            for u in units
        ]
        tops = [
            jnp.maximum(jnp.max(scores[u], axis=0, keepdims=True), sinks[u]) for u in units
        ]
        exps = [jnp.exp(scores[u] - tops[u]) for u in units]
        for u in units:
            part_top[block, slot, u] = tops[u]
            part_sum[block, slot, u] = jnp.sum(exps[u], axis=0, keepdims=True) + jnp.exp(
                sinks[u] - tops[u]
            )
            part_out[block, slot, u] = jnp.dot(
                ctx_vt[slot, u * HD : (u + 1) * HD],
                exps[u].astype(bf16),
                preferred_element_type=f32,
            )

    def window_part(block, position, slot, skip, blocks):
        units = range(pairs)
        here = pl.ds(pl.multiple_of(skip * rows, rows), blocks * rows)
        window = pl.ds(pl.multiple_of((position - 1 + skip) * rows, rows), blocks * rows)
        mask = jnp.concatenate([bias[block, here]] * group, axis=1)
        scores = [
            lax.dot_general(
                key_value[slot, window, 0:kw],
                queries[block, slot, u],
                contract,
                preferred_element_type=f32,
            )
            + mask
            for u in units
        ]
        befores = [part_top[block, slot, u] for u in units]
        tops = [
            jnp.maximum(jnp.max(scores[u], axis=0, keepdims=True), befores[u]) for u in units
        ]
        exps = [jnp.exp(scores[u] - tops[u]) for u in units]
        keeps = [jnp.exp(befores[u] - tops[u]) for u in units]
        values = jnp.transpose(key_value[slot, window, kw : 2 * kw])
        bottoms = [
            jnp.sum(exps[u], axis=0, keepdims=True) + part_sum[block, slot, u] * keeps[u]
            for u in units
        ]
        results = [
            jnp.dot(
                values[u * HD : (u + 1) * HD], exps[u].astype(bf16), preferred_element_type=f32
            )
            + part_out[block, slot, u] * keeps[u]
            for u in units
        ]
        return tops, bottoms, results

    def window_early(block, position, slot, skip, blocks):
        tops, bottoms, results = window_part(block, position, slot, skip, blocks)
        for u in range(pairs):
            part_top[block, slot, u] = tops[u]
            part_sum[block, slot, u] = bottoms[u]
            part_out[block, slot, u] = results[u]

    def store_attended(results, bottoms, slot, target):
        for u in range(pairs):
            result = results[u] / bottoms[u]
            turned_back = jnp.concatenate(
                [result[:, h * rows : (h + 1) * rows] for h in range(group)], axis=0
            )
            target[slot, :, u * 128 : (u + 1) * 128] = jnp.transpose(turned_back).astype(bf16)

    def window_last(block, position, slot, skip, blocks, target):
        _, bottoms, results = window_part(block, position, slot, skip, blocks)
        store_attended(results, bottoms, slot, target)

    def attend_whole(block, position, slot, target):
        units = range(pairs)
        window = pl.ds(pl.multiple_of((position - 1) * rows, rows), band)
        mask = jnp.concatenate([bias[block]] * group, axis=1)
        wide = [
            lax.dot_general(
                ctx_kv[slot, :, 0:kw],
                queries[block, slot, u],
                contract,
                preferred_element_type=f32,
            )
            for u in units
        ]
        near = [
            lax.dot_general(
                key_value[slot, window, 0:kw],
                queries[block, slot, u],
                contract,
                preferred_element_type=f32,
            )
            + mask
            for u in units
        ]
        values = jnp.transpose(key_value[slot, window, kw : 2 * kw])
        sinks = [
            jnp.concatenate(
                [sink_v[slot, u * group + h : u * group + h + 1] for h in range(group)], axis=1
            )
            for u in units
        ]
        tops = [
            jnp.maximum(
                jnp.maximum(
                    jnp.max(wide[u], axis=0, keepdims=True),
                    jnp.max(near[u], axis=0, keepdims=True),
                ),
                sinks[u],
            )
            for u in units
        ]
        wide = [jnp.exp(wide[u] - tops[u]) for u in units]
        near = [jnp.exp(near[u] - tops[u]) for u in units]
        bottoms = [
            jnp.sum(wide[u], axis=0, keepdims=True)
            + jnp.sum(near[u], axis=0, keepdims=True)
            + jnp.exp(sinks[u] - tops[u])
            for u in units
        ]
        results = [
            jnp.dot(
                ctx_vt[slot, u * HD : (u + 1) * HD],
                wide[u].astype(bf16),
                preferred_element_type=f32,
            )
            + jnp.dot(
                values[u * HD : (u + 1) * HD], near[u].astype(bf16), preferred_element_type=f32
            )
            for u in units
        ]
        store_attended(results, bottoms, slot, target)

    edge = jnp.zeros((2, rows, 2 * kw), bf16)

    @pl.when(jnp.logical_and(core == 0, jnp.logical_not(has_left)))
    def _():
        key_value[:, 0:rows] = edge

    @pl.when(jnp.logical_and(core == 1, jnp.logical_not(has_right)))
    def _():
        key_value[:, (tp + 1) * rows : (tp + 2) * rows] = edge

    for i in range(10, 12):
        loads[i].wait()
    pair_copies[0].wait_recv()
    pair_weights = remote(
        proj_w.at[core], proj_w.at[core], pair_send.at[1], pair_recv.at[1], pair_dev
    )
    pair_weights.wait_recv()

    def far_step(j, carry):
        lat_copy(j).wait_recv()
        project(j)
        return carry

    normalize(0, lat_own, 0, width, normed)
    for slot in range(2):
        acc[slot] = jnp.dot(normed[...], proj_w[slot], preferred_element_type=f32)
    finish_pairs(0, t + 1)
    kv_pair(0, t + 1).start()
    send_halo(chip == core)
    for slot in range(2):
        finish_queries(0, slot)
    def wo_pair(gg):
        part = wo.at[far, pl.ds(pl.multiple_of(gg * sp * shard, 16), sp * shard)]
        return remote(part, part, wop_send.at[gg], wop_recv.at[gg], pair_dev)


    def wo_last(c):
        for k in range(3, sp):
            wo_relays(k * WEIGHT_CHUNKS + c, k * WEIGHT_CHUNKS + c + 1)

    wo_relays(2 * WEIGHT_CHUNKS, 2 * WEIGHT_CHUNKS + 1)
    for slot in range(2):
        acc[slot] = jnp.zeros(acc.shape[1:], f32)
    lax.fori_loop(0 * LATENT_CHUNKS // 8, 3 * LATENT_CHUNKS // 8, far_step, 0)
    for k in range(3, sp):
        line_relay(k, ctx_at, ctxz_send, ctxz_recv)
    ctx_pair = remote(ctx_kv.at[core], ctx_kv.at[core], ctxp_sem.at[0], ctxp_sem.at[1], pair_dev)
    ctx_pair.start()
    wo_relays(2 * WEIGHT_CHUNKS + 1, 2 * WEIGHT_CHUNKS + 2)
    lax.fori_loop(3 * LATENT_CHUNKS // 8, 5 * LATENT_CHUNKS // 8, far_step, 0)
    wo_relays(2 * WEIGHT_CHUNKS + 2, 2 * WEIGHT_CHUNKS + 3)
    ctx_pair.wait_recv()
    for slot in range(2):
        ctx_vt[slot] = jnp.transpose(ctx_kv[slot, :, kw : 2 * kw])
    context_part(0, 0)
    kv_pair(0, pair + 1).wait_recv()
    window_early(0, t + 1, 0, 1 - core, 2)
    wo_relays(2 * WEIGHT_CHUNKS + 3, 3 * WEIGHT_CHUNKS)
    context_part(0, 1)
    window_early(0, t + 1, 1, 1 - core, 2)
    start_held(1)
    wo_last(0)
    wo_share(s)
    wo_shares(1)
    lax.fori_loop(5 * LATENT_CHUNKS // 8, 6 * LATENT_CHUNKS // 8, far_step, 0)
    wo_last(1)
    lax.fori_loop(6 * LATENT_CHUNKS // 8, 7 * LATENT_CHUNKS // 8, far_step, 0)
    wo_last(2)
    lax.fori_loop(7 * LATENT_CHUNKS // 8, LATENT_CHUNKS, far_step, 0)
    finish_pairs(1, far + 1)
    kv_pair(1, far + 1).start()
    send_halo(chip != core)
    for c in range(3, WEIGHT_CHUNKS):
        wo_last(c)
    finish_queries(1, 0)

    context_part(1, 0)
    finish_queries(1, 1)

    def att_copy(slot):
        return remote(
            att_out.at[slot], att.at[chip, slot], att_send, att_recv.at[slot], far_dev
        )

    kv_pair(1, pair + 1).wait_recv()
    wait_halo(chip != core)
    window_last(1, far + 1, 0, 0, 3, att_out)
    att_copy(0).start()
    attend_whole(1, far + 1, 1, att_out)
    att_copy(1).start()
    wo_shares(2)
    wait_halo(chip == core)
    for slot in range(2):
        window_last(0, t + 1, slot, 2 * core, 1, att.at[chip])
    for k in range(3, sp):
        wo_shares(k)
    pair_copies[4].wait_recv()
    other = (1 - chip) * 2 + 1 - core
    order = (t, pair, far, other)

    def product(x, slot, i):
        part = pl.ds(pl.multiple_of((2 * x + slot) * qw, qw), qw)
        return jnp.dot(att[x, slot], wo[i, part], preferred_element_type=f32)

    def out_own(k):
        out_part[k] = product(chip, 0, order[k]) + product(chip, 1, order[k])

    def out_first(k):
        out_part[k] += product(1 - chip, 0, order[k])

    def out_last(k):
        cols = pl.ds(pl.multiple_of(order[k] * out_width, 128), out_width)
        sums = out_part[k] + product(1 - chip, 1, order[k])
        blended = sums.astype(bf16).astype(f32)
        mixed[:, cols] = (lat_own[:, cols].astype(f32) + gate_v[:, cols] * blended).astype(bf16)

    out_own(0)
    out_own(1)
    out_own(2)
    att_copy(0).wait_recv()
    for k in range(3):
        out_first(k)
    for gg in range(2):
        part = wo.at[other, pl.ds(gg * sp * shard, sp * shard)]
        remote(part, part, wop_send.at[gg], wop_recv.at[gg], pair_dev).wait_recv()
    out_part[3] = (
        product(chip, 0, other) + product(chip, 1, other) + product(1 - chip, 0, other)
    )
    att_copy(1).wait_recv()
    for k in range(4):
        out_last(k)

    stat_copy.wait_send()
    remote(wo_shard, wo_shard, wox_send, wo_recv.at[0, 0], far_dev).wait_send()
    remote(lat_own, lat_far, lat_send, lat_recv.at[0], far_dev).wait_send()
    pair_copies[0].wait_send()
    pair_weights.wait_send()
    pair_copies[4].wait_send()
    mods.wait_send()
    line_finish(lambda count: mod_part.at[0:count], modz_send)
    line_finish(lambda count: ctx_kv.at[core, 0 : count * ctx_rows], ctxz_send)
    ctx_pair.wait_send()
    def wo_total(count):
        return wo.at[far, 0 : count * shard]

    line_finish(wo_total, wo_send)
    wo_sent = wo.at[far, pl.ds(pl.multiple_of(g * sp * shard, 16), sp * shard)]
    remote(wo_sent, wo_sent, woy_send, woy_recv.at[0, 0], y_dev).wait_send()
    wo_pair(0).wait_send()
    wo_pair(1).wait_send()
    both = key_value.at[:, 0 : 2 * rows]
    remote(both, both, kv_send, kv_recv.at[0], pair_dev).wait_send()

    @pl.when(sends_down)
    def _():
        halo_down.wait_send()

    @pl.when(sends_up)
    def _():
        halo_up.wait_send()

    remote(att_out, att_out, att_send, att_recv.at[0], far_dev).wait_send()


def local(
    latent,
    context,
    conditioning,
    norm_gain,
    shift_weight,
    scale_weight,
    gate_weight,
    query_weight,
    key_weight,
    value_weight,
    out_weight,
    sink_logit,
):
    tp, sp, grp = lax.axis_size("tp"), lax.axis_size("sp"), lax.axis_size("grp")
    rows, width = latent.shape
    ctx_rows = context.shape[0]
    mod_rows, mod_cols = shift_weight.shape
    query_width, key_width = query_weight.shape[1], key_weight.shape[1]
    out_rows, out_width = out_weight.shape
    fits = (
        rows == WIN
        and rows == 128
        and key_width == 2 * HD
        and query_width == 4 * HD
        and tp == 4
        and grp == 2
        and sp >= 3
        and sp * ctx_rows % 128 == 0
        and ctx_rows % CONTEXT_ROWS == 0
        and width % 512 == 0
        and mod_cols % 128 == 0
        and width % (128 * LATENT_CHUNKS) == 0
        and out_width % 128 == 0
        and tp * out_width == width
        and out_rows == tp * query_width
        and out_rows % (2 * sp * WEIGHT_CHUNKS * 16) == 0
    )
    if not fits:
        return local_plain(
            latent,
            context,
            conditioning,
            norm_gain,
            shift_weight,
            scale_weight,
            gate_weight,
            query_weight,
            key_weight,
            value_weight,
            out_weight,
            sink_logit,
        )
    f32, bf16 = jnp.float32, jnp.bfloat16
    dma = pltpu.SemaphoreType.DMA
    anywhere = pl.BlockSpec(memory_space=pl.ANY)
    return pl.pallas_call(
        functools.partial(fused_kernel, sp),
        out_shape=pltpu.VMEM((rows, width), bf16),
        in_specs=[anywhere] * 11 + [pl.BlockSpec(memory_space=pltpu.SMEM)],
        out_specs=pl.BlockSpec(memory_space=pltpu.VMEM),
        scratch_shapes=[
            pltpu.VMEM((mod_rows,), bf16),
            pltpu.VMEM((1, width), f32),
            pltpu.VMEM((3, mod_rows, mod_cols), bf16),
            pltpu.VMEM((2, width, query_width + 2 * key_width), bf16),
            pltpu.VMEM((tp, out_rows, out_width), bf16),
            pltpu.VMEM((out_rows // (2 * sp), out_width), bf16),
            pltpu.VMEM(context.shape, bf16),
            pltpu.VMEM((rows, width), bf16),
            pltpu.VMEM((rows, width), bf16),
            pltpu.VMEM((rows, width), bf16),
            pltpu.VMEM((8, 128), f32),
            pltpu.VMEM((8, 128), f32),
            pltpu.VMEM((2, rows, 128), f32),
            pltpu.VMEM((2, 8, 128), f32),
            pltpu.VMEM((sp, 1, 3 * mod_cols), f32),
            pltpu.VMEM((tp, 1, 3 * mod_cols), f32),
            pltpu.VMEM((1, width), f32),
            pltpu.VMEM((1, width), f32),
            pltpu.VMEM((1, width), f32),
            pltpu.VMEM((2, rows, 128), f32),
            pltpu.VMEM((2, rows, 128), f32),
            pltpu.VMEM((2, rows, query_width + 2 * key_width), f32),
            pltpu.VMEM((2, 2, 2, 2 * rows, key_width), bf16),
            pltpu.VMEM((2, (tp + 2) * rows, 2 * key_width), bf16),
            pltpu.VMEM((2, sp * ctx_rows, 2 * key_width), bf16),
            pltpu.VMEM((2, 2, rows, query_width), bf16),
            pltpu.VMEM((2, rows, query_width), bf16),
            pltpu.VMEM((2, key_width, sp * ctx_rows), bf16),
            pltpu.VMEM((2, 3 * rows, rows), f32),
            pltpu.VMEM((2, 2, 2, HD, 2 * rows), f32),
            pltpu.VMEM((2, 2, 2, 1, 2 * rows), f32),
            pltpu.VMEM((2, 2, 2, 1, 2 * rows), f32),
            pltpu.VMEM((tp, rows, out_width), f32),
            dma((9,)),
            dma,
            dma((LATENT_CHUNKS,)),
            dma((2,)),
            dma((3,)),
            dma((3,)),
            dma,
            dma((2,)),
            dma((sp, WEIGHT_CHUNKS)),
            dma,
            dma((sp, 2)),
            dma((2,)),
            dma((2,)),
            dma((2,)),
            dma((sp,)),
            dma,
            dma,
            dma((2,)),
            dma((sp,)),
            dma((2,)),
            dma,
            dma((2,)),
            dma((2,)),
            dma,
            dma((2,)),
        ],
        compiler_params=pltpu.CompilerParams(
            collective_id=0,
            has_side_effects=True,
            vmem_limit_bytes=60 * 1024 * 1024,
        ),
        name="fused",
    )(
        latent,
        context,
        conditioning,
        norm_gain.reshape(1, width),
        shift_weight,
        scale_weight,
        gate_weight,
        query_weight,
        key_weight,
        value_weight,
        out_weight,
        sink_logit,
    )


def solution(mesh):
    in_specs = (
        P(("grp", "sp", "tp"), None),
        P(("grp", "sp"), None),
        P(("grp", "sp")),
        P(),
        P("sp", "tp"),
        P("sp", "tp"),
        P("sp", "tp"),
        P(None, "tp"),
        P(None, "tp"),
        P(None, "tp"),
        P(None, "tp"),
        P("tp"),
    )
    out_specs = P(("grp", "sp", "tp"), None)
    return jax.shard_map(local, mesh=mesh, in_specs=in_specs, out_specs=out_specs, check_vma=False)
```
